128 devices in a mesh: sp: 32 (over z, y, core), tp: 4 (over x).
Axes of the slice: x: 4, y: 4, z: 4, core: 2. Of those that a mesh axis runs over, the one named last changes fastest.
Arguments:
- query_rows: bfloat16 [16384, 1024], P('sp', 'tp'), may hold values from -6 to 6
- key_rows: bfloat16 [16384, 512], P('sp', 'tp'), may hold values from -6 to 6
- value_rows: bfloat16 [16384, 512], P('sp', 'tp'), may hold values from -12 to 12
- query_gain: float32 [128], replicated, may hold values from 0.2 to 6.5
- key_gain: float32 [128], replicated, may hold values from 0.2 to 6.5
- residual: bfloat16 [16384, 2048], P(('sp', 'tp')), may hold values from -6 to 6
- out_weight: bfloat16 [1024, 2048], P('tp'), may hold values from -3 to 3
- mix_gain: float32 [2048], replicated, may hold values from 0.1 to 1.9
- gate_weight: bfloat16 [2048, 5632], P('sp', 'tp'), may hold values from -0.125 to 0.125
- up_weight: bfloat16 [2048, 5632], P('sp', 'tp'), may hold values from -0.125 to 0.125
- down_weight: bfloat16 [5632, 2048], P('tp', 'sp'), may hold values from -0.15625 to 0.15625
Outputs:
- layer_out: bfloat16 [16384, 2048], P(('sp', 'tp'))
The draws below stay inside these ranges and needn't reach their ends.
All inputs are finite; a program needn't handle non-finite values.
Results may differ from the reference program's by a relative error of at most 0.015.
The reference program's roundings to bfloat16 on the way count: a program that leaves them out, or rounds other values in their place, can miss the bound.
Values may be sent and summed in bfloat16 or wider, within the bound.
No kernel may reach another device: no remote copies, remote signals or barrier semaphores. Data moves between devices by JAX's collectives and lax.ppermute only.
A program may use at most 128 MiB of HBM per device.

```python
import jax
import jax.numpy as jnp
from jax import lax

D = 2048
HD = 128
QHEADS = 8
KVHEADS = 4
FF = 5632
GRID = 64
TOK_DEV = 512
TOKENS = 16384
N_TP = 4


def drawn_keys(key):
    base_keys = jnp.clip(jax.random.normal(jax.random.fold_in(key, 11), (TOKENS, KVHEADS * HD), jnp.float32), -6.0, 6.0)
    return base_keys


def draw_key_rows(key, part):
    return drawn_keys(key).astype(jnp.bfloat16)


def draw_query_rows(key, part):
    fresh = jnp.clip(jax.random.normal(jax.random.fold_in(key, 23), (TOKENS, QHEADS * HD), jnp.float32), -6.0, 6.0)
    return fresh.astype(jnp.bfloat16)


def gain_values(key):
    return 1.0 + 0.18 * jnp.clip(jax.random.normal(key, (HD,), jnp.float32), -4.4, 4.4)


def draw_query_gain(key, part):
    return gain_values(jax.random.fold_in(key, 31))


def draw_key_gain(key, part):
    return gain_values(jax.random.fold_in(key, 37))


def draw_out_weight(key, part):
    fresh = jnp.clip(jax.random.normal(jax.random.fold_in(key, 41), (QHEADS * HD, D), jnp.float32), -6.0, 6.0)
    spread = 0.5
    return (fresh * spread).astype(jnp.bfloat16)


def level_of(own_key, extent, pieces, least, largest):
    factor_of, own = 1.0, jax.random.fold_in(own_key, 6)
    for dim, shards_of in pieces:
        heights = jnp.exp(jax.random.uniform(jax.random.fold_in(own, dim), (shards_of,), jnp.float32, least / len(pieces), largest / len(pieces)))
        factor_of = factor_of * jnp.repeat(heights, extent[dim] // shards_of).reshape([-1 if axis == dim else 1 for axis in range(len(extent))])
    return factor_of


def bell_draw(own_key, dims, deviation, limit, cuts=(), kind=jnp.bfloat16):
    result = deviation * jax.random.normal(own_key, dims, jnp.float32)
    if cuts:
        result = result * level_of(own_key, dims, cuts, -0.22, 0.18)
    return jnp.clip(result, -limit, limit).astype(kind)


def setup_inputs(seed: int = 0) -> dict:
    keys = jax.random.split(jax.random.key(seed), 12)
    return {
        "query_rows": draw_query_rows(jax.random.fold_in(keys[11], 71), 0),
        "key_rows": draw_key_rows(jax.random.fold_in(keys[11], 71), 0),
        "value_rows": bell_draw(keys[2], (TOKENS, KVHEADS * HD), 2.0, 12.0, ((0, 32), (1, 4))),
        "query_gain": draw_query_gain(jax.random.fold_in(keys[11], 71), 0),
        "key_gain": draw_key_gain(jax.random.fold_in(keys[11], 71), 0),
        "residual": bell_draw(keys[5], (TOKENS, D), 1.0, 6.0, ((0, 128),)),
        "out_weight": draw_out_weight(jax.random.fold_in(keys[11], 71), 0),
        "mix_gain": jnp.clip(1.0 + 0.18 * jax.random.normal(keys[7], (D,), jnp.float32), 0.1, 1.9),
        "gate_weight": bell_draw(keys[8], (D, FF), D ** -0.5, 0.125, ((0, 32), (1, 4))),
        "up_weight": bell_draw(keys[9], (D, FF), D ** -0.5, 0.125, ((0, 32), (1, 4))),
        "down_weight": bell_draw(keys[10], (FF, D), (FF // 4) ** -0.5, 0.15625, ((0, 4), (1, 32))),
    }


norm_eps = 1e-06
theta_base = 10000.0

def spin(halfway, angles):
    cosine = jnp.cos(angles)[:, None, :]
    sine_val = jnp.sin(angles)[:, None, :]
    quarter = halfway.shape[-1] // 2
    leading = halfway[..., :quarter]
    trailing = halfway[..., quarter:]
    return [leading * cosine - trailing * sine_val, trailing * cosine + leading * sine_val]

def rotate_grid(vectors, positions):
    head_dim = vectors.shape[-1]
    quarter = head_dim // 4
    frequency = jnp.power(theta_base, -2.0 * jnp.arange(quarter, dtype=jnp.float32) / (head_dim // 2))
    row_angle = (positions // GRID).astype(jnp.float32)[:, None] * frequency
    col_angle = (positions % GRID).astype(jnp.float32)[:, None] * frequency
    lower_half = vectors[..., :2 * quarter]
    upper_half = vectors[..., 2 * quarter:]
    return jnp.concatenate(spin(lower_half, row_angle) + spin(upper_half, col_angle), axis=-1)

def prepare_heads(raw_heads, head_gain, positions):
    floated = raw_heads.astype(jnp.float32)
    scaled = floated * lax.rsqrt(lax.optimization_barrier(jnp.mean(floated * floated, axis=-1, keepdims=True)) + norm_eps)
    return rotate_grid(scaled * head_gain, positions).astype(jnp.bfloat16)

def row_norm(row_data, row_gain):
    floated = row_data.astype(jnp.float32)
    scaled = floated * lax.rsqrt(lax.optimization_barrier(jnp.mean(floated * floated, axis=-1, keepdims=True)) + norm_eps)
    return (scaled * row_gain).astype(jnp.bfloat16)

def to_wire(partial_value):
    return lax.optimization_barrier(partial_value.astype(jnp.bfloat16)).astype(jnp.float32)

def reference(query_rows, key_rows, value_rows, query_gain, key_gain, residual, out_weight, mix_gain, gate_weight, up_weight, down_weight):
    positions = jnp.arange(TOKENS, dtype=jnp.int32)
    group_size = QHEADS // KVHEADS
    q_heads = prepare_heads(query_rows.reshape(TOKENS, QHEADS, HD), query_gain, positions)
    k_heads = prepare_heads(key_rows.reshape(TOKENS, KVHEADS, HD), key_gain, positions).astype(jnp.float32)
    v_heads = value_rows.reshape(TOKENS, KVHEADS, HD).astype(jnp.float32)
    score_scale = HD ** (-0.5)
    q_blocks = q_heads.reshape(TOKENS // TOK_DEV, TOK_DEV, KVHEADS, group_size, HD)

    def attend(query_block):
        scores = jnp.einsum('qkgd,skd->kgqs', query_block.astype(jnp.float32), k_heads) * score_scale
        row_max = lax.optimization_barrier(jnp.max(scores, axis=-1, keepdims=True))
        weights = jnp.exp(scores - row_max)
        row_sum = lax.optimization_barrier(jnp.sum(weights, axis=-1))
        narrow = lax.optimization_barrier(weights.astype(jnp.bfloat16)).astype(jnp.float32)
        combined = jnp.einsum('kgqs,skd->qkgd', narrow, v_heads)
        return (combined / jnp.transpose(row_sum, (2, 0, 1))[..., None]).astype(jnp.bfloat16)
    attended = lax.map(attend, q_blocks).reshape(TOKENS, QHEADS * HD)
    head_cols = QHEADS * HD // N_TP
    attn_sum = jnp.zeros((TOKENS, D), jnp.float32)
    for member in range(N_TP):
        partial_value = jnp.dot(attended[:, member * head_cols:(member + 1) * head_cols], out_weight[member * head_cols:(member + 1) * head_cols], preferred_element_type=jnp.float32)
        attn_sum = attn_sum + to_wire(partial_value)
    updated = (residual.astype(jnp.float32) + attn_sum).astype(jnp.bfloat16)
    normed = row_norm(updated, mix_gain)
    unit_cols = FF // N_TP
    unit_sum = jnp.zeros((TOKENS, D), jnp.float32)
    for member in range(N_TP):
        gate_act = jnp.dot(normed, gate_weight[:, member * unit_cols:(member + 1) * unit_cols], preferred_element_type=jnp.float32)
        up_act = jnp.dot(normed, up_weight[:, member * unit_cols:(member + 1) * unit_cols], preferred_element_type=jnp.float32)
        hidden = (jax.nn.silu(gate_act) * up_act).astype(jnp.bfloat16)
        partial_value = jnp.dot(hidden, down_weight[member * unit_cols:(member + 1) * unit_cols], preferred_element_type=jnp.float32)
        unit_sum = unit_sum + to_wire(partial_value)
    return (updated.astype(jnp.float32) + 0.5 * unit_sum).astype(jnp.bfloat16)
```

```python
import functools

import jax
import jax.numpy as jnp
from jax import lax
from jax.experimental import pallas as pl
from jax.experimental.pallas import tpu as pltpu
from jax.sharding import PartitionSpec as P

GRID = 64
norm_eps = 1e-06
theta_base = 10000.0
LOG2E = 1.4426950408889634
f32 = jnp.float32
bf16 = jnp.bfloat16


def angle_tables(first_row, rows, head_dim):
    quarter = head_dim // 4
    frequency = jnp.power(theta_base, -2.0 * jnp.arange(quarter, dtype=f32) / (head_dim // 2))
    places = jnp.concatenate([first_row + jnp.arange(rows, dtype=jnp.int32), jnp.arange(GRID, dtype=jnp.int32)])
    angles = places.astype(f32)[:, None] * frequency
    cosine, sine = lax.optimization_barrier((jnp.cos(angles), jnp.sin(angles)))
    is_row = (jnp.arange(rows + GRID) < rows)[:, None]
    zero = jnp.zeros_like(cosine)

    def placed(lead, trail):
        return jnp.concatenate(
            [
                jnp.where(is_row, lead, zero),
                jnp.where(is_row, trail, zero),
                jnp.where(is_row, zero, lead),
                jnp.where(is_row, zero, trail),
            ],
            axis=1,
        )

    return placed(cosine, cosine), placed(-sine, sine)


def prepare_kernel(q_ref, k_ref, v_ref, qg_ref, kg_ref, cos_ref, sin_ref, q_out, kv_out, *, rows, head_dim, heads):
    tok = rows * GRID

    def spread(ref):
        both = ref[0:rows, :][:, None, :] + ref[rows : rows + GRID, :][None, :, :]
        return both.reshape(tok, head_dim)

    cosine = spread(cos_ref)
    sine = spread(sin_ref)
    lane = lax.broadcasted_iota(jnp.int32, (tok, head_dim), 1)
    first = (lane % (head_dim // 2)) < head_dim // 4
    quarter = head_dim // 4

    def prepared(raw, gain):
        x = raw.astype(f32)
        x = x * lax.rsqrt(jnp.mean(x * x, axis=-1, keepdims=True) + norm_eps) * gain
        partner = jnp.where(first, pltpu.roll(x, head_dim - quarter, 1), pltpu.roll(x, quarter, 1))
        return (x * cosine + partner * sine).astype(bf16)

    for h in range(heads):
        q_out[h * tok : (h + 1) * tok, :] = prepared(q_ref[:, h * head_dim : (h + 1) * head_dim], qg_ref[...])
    kv_out[:, 0:head_dim] = prepared(k_ref[...], kg_ref[...])
    kv_out[:, head_dim:] = v_ref[...]


def prepare(query_rows, key_rows, value_rows, query_gain, key_gain):
    tok, width = query_rows.shape
    head_dim = query_gain.shape[0]
    rows = tok // GRID
    cosine, sine = angle_tables(lax.axis_index("sp") * rows, rows, head_dim)
    return pl.pallas_call(
        functools.partial(prepare_kernel, rows=rows, head_dim=head_dim, heads=width // head_dim),
        out_shape=(
            jax.ShapeDtypeStruct((tok * (width // head_dim), head_dim), bf16),
            jax.ShapeDtypeStruct((tok, 2 * head_dim), bf16),
        ),
        name="prepare",
    )(query_rows, key_rows, value_rows, query_gain[None, :], key_gain[None, :], cosine, sine)


def flash_kernel(q_ref, kv_ref, o_ref, m_ref, acc_ref, *, tile, scale):
    step = pl.program_id(0)
    head_dim = q_ref.shape[1]

    @pl.when(step == 0)
    def _():
        m_ref[...] = jnp.full_like(m_ref, -jnp.inf)
        acc_ref[...] = jnp.zeros_like(acc_ref)

    keys = kv_ref[:, 0:head_dim]
    values = kv_ref[:, head_dim:]
    values = jnp.concatenate([values, jnp.ones_like(values)], axis=1)
    for t in range(q_ref.shape[0] // tile):
        part = slice(t * tile, (t + 1) * tile)
        s = lax.dot_general(q_ref[part, :], keys, (((1,), (1,)), ((), ())), preferred_element_type=f32) * scale
        old = m_ref[part, :]
        new = jnp.maximum(old, jnp.max(s, axis=1, keepdims=True))
        w = jnp.exp2(s - new[:, 0:1]).astype(bf16)
        factor = jnp.exp2(old - new)
        m_ref[part, :] = new
        acc_ref[part, :] = acc_ref[part, :] * factor[:, 0:1] + jnp.dot(w, values, preferred_element_type=f32)

    @pl.when(step == pl.num_programs(0) - 1)
    def _():
        tok = o_ref.shape[0]
        for h in range(q_ref.shape[0] // tok):
            a = acc_ref[h * tok : (h + 1) * tok, :]
            o_ref[:, h * head_dim : (h + 1) * head_dim] = (a[:, 0:head_dim] / a[:, head_dim:]).astype(bf16)


def flash(q, kv, tok, tile=256, block=1024):
    rows, head_dim = q.shape
    heads = rows // tok
    keys = kv.shape[0]
    return pl.pallas_call(
        functools.partial(flash_kernel, tile=tile, scale=head_dim**-0.5 * LOG2E),
        grid=(keys // block,),
        in_specs=[
            pl.BlockSpec((rows, head_dim), lambda i: (0, 0)),
            pl.BlockSpec((block, 2 * head_dim), lambda i: (i, 0)),
        ],
        out_specs=pl.BlockSpec((tok, heads * head_dim), lambda i: (0, 0)),
        out_shape=jax.ShapeDtypeStruct((tok, heads * head_dim), bf16),
        scratch_shapes=[pltpu.VMEM((rows, 128), f32), pltpu.VMEM((rows, 2 * head_dim), f32)],
        compiler_params=pltpu.CompilerParams(dimension_semantics=("arbitrary",)),
        cost_estimate=pl.CostEstimate(
            flops=4 * rows * keys * head_dim, bytes_accessed=4 * keys * head_dim, transcendentals=rows * keys
        ),
        name="flash",
    )(q, kv)


def project_kernel(place, *refs, parts, tile):
    att = refs[0:parts]
    weight = refs[parts : 2 * parts]
    res = refs[2 * parts : 3 * parts]
    gain_ref, own_ref, norm_ref, up_ref = refs[3 * parts :]
    step = pl.program_id(0)
    sub = res[0].shape[0]
    cols = pl.ds(pl.multiple_of(step * tile, tile), tile)
    total = None
    for a, w in zip(att, weight):
        rolled = jnp.concatenate(
            [a[pl.ds(pl.multiple_of(((place[0] + r) % parts) * sub, sub), sub), :] for r in range(parts)], axis=0
        )
        part = jnp.dot(rolled, w[...], preferred_element_type=f32).astype(bf16).astype(f32)
        total = part if total is None else total + part
    for r in range(parts):
        updated = (res[r][...].astype(f32) + total[r * sub : (r + 1) * sub, :]).astype(bf16)
        up_ref[r * sub : (r + 1) * sub, cols] = updated

    @pl.when(step == pl.num_programs(0) - 1)
    def _():
        own_ref[...] = up_ref[0:sub, :]
        for r in range(2 * parts):
            some = slice(r * sub // 2, (r + 1) * sub // 2)
            x = up_ref[some, :].astype(f32)
            x = x * lax.rsqrt(jnp.mean(x * x, axis=-1, keepdims=True) + norm_eps)
            norm_ref[some, :] = (x * gain_ref[...]).astype(bf16)


def project(place, att, weight, res, gain, tile=512):
    parts = len(att)
    tok, part_width = att[0].shape
    sub, width = res[0].shape
    return pl.pallas_call(
        functools.partial(project_kernel, parts=parts, tile=tile),
        grid_spec=pltpu.PrefetchScalarGridSpec(
            num_scalar_prefetch=1,
            grid=(width // tile,),
            in_specs=[pl.BlockSpec((tok, part_width), lambda i, p: (0, 0))] * parts
            + [pl.BlockSpec((part_width, tile), lambda i, p: (0, i))] * parts
            + [pl.BlockSpec((sub, tile), lambda i, p: (0, i))] * parts
            + [pl.BlockSpec((1, width), lambda i, p: (0, 0))],
            out_specs=(
                pl.BlockSpec((sub, width), lambda i, p: (0, 0)),
                pl.BlockSpec((tok, width), lambda i, p: (0, 0)),
            ),
            scratch_shapes=[pltpu.VMEM((tok, width), bf16)],
        ),
        out_shape=(jax.ShapeDtypeStruct((sub, width), bf16), jax.ShapeDtypeStruct((tok, width), bf16)),
        compiler_params=pltpu.CompilerParams(dimension_semantics=("arbitrary",)),
        name="project",
    )(place, *att, *weight, *res, gain[None, :])


def hidden_kernel(x_ref, g_ref, u_ref, h_ref):
    both = jnp.concatenate([g_ref[...], u_ref[...]], axis=1)
    r = jnp.dot(x_ref[...], both, preferred_element_type=f32)
    tile = g_ref.shape[1]
    gate = r[:, 0:tile]
    h_ref[...] = (gate / (1.0 + jnp.exp(-gate)) * r[:, tile:]).astype(bf16)


def down_kernel(h_ref, d_ref, o_ref):
    o_ref[...] = lax.dot_general(
        h_ref[...], d_ref[...], (((1,), (1,)), ((), ())), preferred_element_type=f32
    ).astype(bf16)


def feed_forward(x, weights, units, tile=128, out_tile=256):
    tok, width = x.shape
    count = units // tile
    hidden = pl.pallas_call(
        hidden_kernel,
        grid=(count,),
        in_specs=[
            pl.BlockSpec((tok, width), lambda i: (0, 0)),
            pl.BlockSpec((width, tile), lambda i: (0, i)),
            pl.BlockSpec((width, tile), lambda i: (0, i + count)),
        ],
        out_specs=pl.BlockSpec((tok, tile), lambda i: (0, i)),
        out_shape=jax.ShapeDtypeStruct((tok, units), bf16),
        compiler_params=pltpu.CompilerParams(dimension_semantics=("arbitrary",)),
        name="hidden",
    )(x, weights, weights)
    return pl.pallas_call(
        down_kernel,
        grid=(width // out_tile,),
        in_specs=[
            pl.BlockSpec((tok, units), lambda i: (0, 0)),
            pl.BlockSpec((out_tile, units), lambda i: (i, 2)),
        ],
        out_specs=pl.BlockSpec((tok, out_tile), lambda i: (0, i)),
        out_shape=jax.ShapeDtypeStruct((tok, width), bf16),
        compiler_params=pltpu.CompilerParams(dimension_semantics=("arbitrary",)),
        name="down",
    )(hidden, weights)


def shifted(value, by):
    count = lax.axis_size("tp")
    return lax.ppermute(value, "tp", [(i, (i + by) % count) for i in range(count)])


def on_device(
    query_rows,
    key_rows,
    value_rows,
    query_gain,
    key_gain,
    residual,
    out_weight,
    mix_gain,
    gate_weight,
    up_weight,
    down_weight,
):
    tok = query_rows.shape[0]
    parts = lax.axis_size("tp")
    units = gate_weight.shape[1]
    place = lax.axis_index("tp")[None]
    q, kv = prepare(query_rows, key_rows, value_rows, query_gain, key_gain)
    kv_all = lax.all_gather(kv, "sp", axis=0, tiled=True)
    own_weights = jnp.concatenate([gate_weight, up_weight, down_weight.T], axis=1)
    own_weights, _ = lax.optimization_barrier((own_weights, kv))
    weights = lax.all_gather(own_weights, "sp", axis=0, tiled=True)
    out_parts = [out_weight] + [shifted(out_weight, -r) for r in range(1, parts)]
    res_parts = [residual] + [shifted(residual, -r) for r in range(1, parts)]
    attended = flash(q, kv_all, tok)
    att_parts = [attended] + [shifted(attended, -r) for r in range(1, parts)]
    own_rows, normed = project(place, att_parts, out_parts, res_parts, mix_gain)
    unit_part = feed_forward(normed, weights, units)
    sub = tok // parts
    unit_sum = unit_part[0:sub].astype(f32)
    for r in range(1, parts):
        unit_sum = unit_sum + shifted(unit_part[r * sub : (r + 1) * sub], r).astype(f32)
    return (own_rows.astype(f32) + 0.5 * unit_sum).astype(bf16)


def solution(mesh):
    placed = (
        P("sp", "tp"),
        P("sp", "tp"),
        P("sp", "tp"),
        P(),
        P(),
        P(("sp", "tp"), None),
        P("tp", None),
        P(),
        P("sp", "tp"),
        P("sp", "tp"),
        P("tp", "sp"),
    )
    return jax.shard_map(
        on_device, mesh=mesh, in_specs=placed, out_specs=P(("sp", "tp"), None), check_vma=False
    )
```

```python
import functools

import jax
import jax.numpy as jnp
from jax import lax
from jax.experimental import pallas as pl
from jax.experimental.pallas import tpu as pltpu
from jax.sharding import PartitionSpec as P

GRID = 64
norm_eps = 1e-06
theta_base = 10000.0
LOG2E = 1.4426950408889634
f32 = jnp.float32
bf16 = jnp.bfloat16


def angle_tables(first_row, rows, head_dim):
    quarter = head_dim // 4
    frequency = jnp.power(theta_base, -2.0 * jnp.arange(quarter, dtype=f32) / (head_dim // 2))
    places = jnp.concatenate([first_row + jnp.arange(rows, dtype=jnp.int32), jnp.arange(GRID, dtype=jnp.int32)])
    angles = places.astype(f32)[:, None] * frequency
    cosine, sine = lax.optimization_barrier((jnp.cos(angles), jnp.sin(angles)))
    is_row = (jnp.arange(rows + GRID) < rows)[:, None]
    zero = jnp.zeros_like(cosine)

    def placed(lead, trail):
        return jnp.concatenate(
            [
                jnp.where(is_row, lead, zero),
                jnp.where(is_row, trail, zero),
                jnp.where(is_row, zero, lead),
                jnp.where(is_row, zero, trail),
            ],
            axis=1,
        )

    return placed(cosine, cosine), placed(-sine, sine)


def prepare_kernel(
    core, q_hbm, k_hbm, v_hbm, g_hbm, u_hbm, d_hbm, w_hbm, r_hbm, qg_ref, kg_ref, cos_ref, sin_ref,
    q_out, a_out, b_out, woven, sent, kept,
    q_ref, k_ref, v_ref, g_ref, u_ref, d_ref, sems, *, rows, head_dim, heads, tile,
):
    tok = rows * GRID
    half = kept.shape[0]
    first_half = pl.ds(pl.multiple_of(core[0] * half, half), half)
    other_half = pl.ds(pl.multiple_of((1 - core[0]) * half, half), half)
    moves = [
        (k_hbm, k_ref),
        (v_hbm, v_ref),
        (q_hbm, q_ref),
        (g_hbm, g_ref),
        (u_hbm, u_ref),
        (d_hbm, d_ref),
        (w_hbm.at[first_half, :], sent.at[pl.ds(0, half), :]),
        (r_hbm, sent.at[pl.ds(half, r_hbm.shape[0]), :]),
        (w_hbm.at[other_half, :], kept),
    ]
    copies = [pltpu.make_async_copy(x, y, sems.at[n]) for n, (x, y) in enumerate(moves)]
    for c in copies:
        c.start()

    def spread(ref):
        both = ref[0:rows, :][:, None, :] + ref[rows : rows + GRID, :][None, :, :]
        return both.reshape(tok, head_dim)

    cosine = spread(cos_ref)
    sine = spread(sin_ref)
    lane = lax.broadcasted_iota(jnp.int32, (tok, head_dim), 1)
    first = (lane % (head_dim // 2)) < head_dim // 4
    quarter = head_dim // 4

    def prepared(raw, gain):
        x = raw.astype(f32)
        x = x * lax.rsqrt(jnp.mean(x * x, axis=-1, keepdims=True) + norm_eps) * gain
        partner = jnp.where(first, pltpu.roll(x, head_dim - quarter, 1), pltpu.roll(x, quarter, 1))
        return (x * cosine + partner * sine).astype(bf16)

    copies[0].wait()
    copies[1].wait()
    keys = prepared(k_ref[...], kg_ref[...])
    for n, out in enumerate((a_out, b_out)):
        part = slice(n * tok // 2, (n + 1) * tok // 2)
        out[:, 0:head_dim] = keys[part, :]
        out[:, head_dim:] = v_ref[part, :]
    copies[2].wait()
    for h in range(heads):
        q_out[h * tok : (h + 1) * tok, :] = prepared(q_ref[:, h * head_dim : (h + 1) * head_dim], qg_ref[...])
    for n in (3, 4, 5):
        copies[n].wait()
    units = g_ref.shape[1]
    for n in range(units // tile):
        part = slice(n * tile, (n + 1) * tile)
        woven[:, 2 * n * tile : (2 * n + 1) * tile] = g_ref[:, part]
        woven[:, (2 * n + 1) * tile : (2 * n + 2) * tile] = u_ref[:, part]
    woven[:, 2 * units :] = d_ref[...]
    for n in (6, 7, 8):
        copies[n].wait()


def prepare(query_rows, key_rows, value_rows, query_gain, key_gain, gate, up, down, out_weight, residual, tile=128):
    tok, width = query_rows.shape
    head_dim = query_gain.shape[0]
    rows = tok // GRID
    cosine, sine = angle_tables(lax.axis_index("sp") * rows, rows, head_dim)
    hbm = pl.BlockSpec(memory_space=pltpu.HBM)
    vmem = pl.BlockSpec(memory_space=pltpu.VMEM)
    big = (query_rows, key_rows, value_rows, gate, up, down.T)
    half = out_weight.shape[0] // 2
    return pl.pallas_call(
        functools.partial(prepare_kernel, rows=rows, head_dim=head_dim, heads=width // head_dim, tile=tile),
        in_specs=[pl.BlockSpec(memory_space=pltpu.SMEM)] + [hbm] * 8 + [vmem] * 4,
        out_specs=[vmem] * 4 + [hbm] * 2,
        out_shape=(
            jax.ShapeDtypeStruct((tok * (width // head_dim), head_dim), bf16),
            jax.ShapeDtypeStruct((tok // 2, 2 * head_dim), bf16),
            jax.ShapeDtypeStruct((tok // 2, 2 * head_dim), bf16),
            jax.ShapeDtypeStruct((gate.shape[0], 3 * gate.shape[1]), bf16),
            jax.ShapeDtypeStruct((half + residual.shape[0], residual.shape[1]), bf16),
            jax.ShapeDtypeStruct((half, residual.shape[1]), bf16),
        ),
        scratch_shapes=[pltpu.VMEM(x.shape, bf16) for x in big] + [pltpu.SemaphoreType.DMA((9,))],
        compiler_params=pltpu.CompilerParams(vmem_limit_bytes=60 * 1024 * 1024),
        name="prepare",
    )(
        (lax.axis_index("sp") % 2)[None], *big, out_weight, residual, query_gain[None, :], key_gain[None, :], cosine, sine
    )


def flash_kernel(*refs, pieces, scale, first, last):
    q_ref = refs[0]
    kv_refs = refs[1 : 1 + pieces]
    refs = refs[1 + pieces :]
    if not first:
        m_in, acc_in = refs[0:2]
        refs = refs[2:]
    if last:
        o_ref = refs[0]
        refs = refs[1:]
    else:
        m_out, acc_out = refs[0:2]
        refs = refs[2:]
    head_dim = q_ref.shape[1]
    q = q_ref[...]
    if first:
        m = jnp.full((q.shape[0], 128), -jnp.inf, f32)
        acc = jnp.zeros((q.shape[0], 2 * head_dim), f32)
    else:
        m = m_in[...]
        acc = acc_in[...]
    for n in range(pieces):
        keys = kv_refs[n][:, 0:head_dim]
        values = kv_refs[n][:, head_dim:]
        values = jnp.concatenate([values, jnp.ones_like(values)], axis=1)
        s = lax.dot_general(q, keys, (((1,), (1,)), ((), ())), preferred_element_type=f32) * scale
        new = jnp.maximum(m, jnp.max(s, axis=1, keepdims=True))
        w = jnp.exp2(s - new[:, 0:1]).astype(bf16)
        factor = jnp.exp2(m - new)
        acc = acc * factor[:, 0:1] + jnp.dot(w, values, preferred_element_type=f32)
        m = new
    if last:
        o_ref[...] = (acc[:, 0:head_dim] / acc[:, head_dim:]).astype(bf16)
    else:
        m_out[...] = m
        acc_out[...] = acc


def flash(q, kv, state, tok, last, tile=256):
    rows, head_dim = q.shape
    heads = rows // tok
    pieces = len(kv)
    piece = kv[0].shape
    tiles = tok // tile
    held = [pl.BlockSpec((tile, 128), lambda i: (i, 0)), pl.BlockSpec((tile, 2 * head_dim), lambda i: (i, 0))]
    held_shape = (jax.ShapeDtypeStruct((rows, 128), f32), jax.ShapeDtypeStruct((rows, 2 * head_dim), f32))
    first = state is None
    return pl.pallas_call(
        functools.partial(flash_kernel, pieces=pieces, scale=head_dim**-0.5 * LOG2E, first=first, last=last),
        grid=(rows // tile,),
        in_specs=[pl.BlockSpec((tile, head_dim), lambda i: (i, 0))]
        + [pl.BlockSpec(piece, lambda i: (0, 0))] * pieces
        + ([] if first else held),
        out_specs=pl.BlockSpec((tile, head_dim), lambda i: (i % tiles, i // tiles)) if last else tuple(held),
        out_shape=jax.ShapeDtypeStruct((tok, heads * head_dim), bf16) if last else held_shape,
        compiler_params=pltpu.CompilerParams(dimension_semantics=("arbitrary",), vmem_limit_bytes=12 << 20),
        cost_estimate=pl.CostEstimate(
            flops=4 * rows * piece[0] * pieces * head_dim,
            bytes_accessed=4 * piece[0] * pieces * head_dim,
            transcendentals=rows * piece[0] * pieces,
        ),
        name="flash_last" if last else "flash_first" if first else "flash_more",
    )(q, *kv, *([] if first else state))


def project_kernel(place, *refs, parts, tile):
    att = refs[0:parts]
    sent = refs[parts : 2 * parts]
    swapped = refs[2 * parts : 3 * parts]
    gain_ref, own_ref, norm_ref, up_ref = refs[3 * parts :]
    step = pl.program_id(0)
    half = swapped[0].shape[0]
    sub = sent[0].shape[0] - half
    cols = pl.ds(pl.multiple_of(step * tile, tile), tile)
    total = None
    for a, w, o in zip(att, sent, swapped):
        rolled = []
        for r in range(parts):
            rows = pl.ds(pl.multiple_of(((place[0] + r) % parts) * sub, sub), sub)
            halves = [a[rows, pl.ds(pl.multiple_of(c * half, half), half)] for c in (place[1], 1 - place[1])]
            rolled.append(jnp.concatenate(halves, axis=1))
        weight = jnp.concatenate([w[0:half, :], o[...]], axis=0)
        part = jnp.dot(jnp.concatenate(rolled, axis=0), weight, preferred_element_type=f32).astype(bf16).astype(f32)
        total = part if total is None else total + part
    for r in range(parts):
        updated = (sent[r][half:, :].astype(f32) + total[r * sub : (r + 1) * sub, :]).astype(bf16)
        up_ref[r * sub : (r + 1) * sub, cols] = updated

    @pl.when(step == pl.num_programs(0) - 1)
    def _():
        own_ref[...] = up_ref[0:sub, :]
        for r in range(2 * parts):
            some = slice(r * sub // 2, (r + 1) * sub // 2)
            x = up_ref[some, :].astype(f32)
            x = x * lax.rsqrt(jnp.mean(x * x, axis=-1, keepdims=True) + norm_eps)
            norm_ref[some, :] = (x * gain_ref[...]).astype(bf16)


def project(place, att, sent, swapped, gain, tile=512):
    parts = len(att)
    tok, part_width = att[0].shape
    both, width = sent[0].shape
    half = swapped[0].shape[0]
    sub = both - half
    return pl.pallas_call(
        functools.partial(project_kernel, parts=parts, tile=tile),
        grid_spec=pltpu.PrefetchScalarGridSpec(
            num_scalar_prefetch=1,
            grid=(width // tile,),
            in_specs=[pl.BlockSpec((tok, part_width), lambda i, p: (0, 0))] * parts
            + [pl.BlockSpec((both, tile), lambda i, p: (0, i))] * parts
            + [pl.BlockSpec((half, tile), lambda i, p: (0, i))] * parts
            + [pl.BlockSpec((1, width), lambda i, p: (0, 0))],
            out_specs=(
                pl.BlockSpec((sub, width), lambda i, p: (0, 0)),
                pl.BlockSpec((tok, width), lambda i, p: (0, 0)),
            ),
            scratch_shapes=[pltpu.VMEM((tok, width), bf16)],
        ),
        out_shape=(jax.ShapeDtypeStruct((sub, width), bf16), jax.ShapeDtypeStruct((tok, width), bf16)),
        compiler_params=pltpu.CompilerParams(dimension_semantics=("arbitrary",), vmem_limit_bytes=16 << 20),
        name="project",
    )(place, *att, *sent, *swapped, gain[None, :])


def unit_kernel(x_ref, w_hbm, *refs, units, tile, rows):
    outs = refs[:-4]
    pair_ref, down_ref, h_ref, sems = refs[-4:]
    count = units // tile
    blocks = down_ref.shape[0]

    def gate_copy(n):
        return pltpu.make_async_copy(w_hbm.at[:, pl.ds(2 * n * tile, 2 * tile)], pair_ref.at[n], sems.at[n])

    def down_copy(n):
        source = w_hbm.at[pl.ds(n * rows, rows), pl.ds(2 * units, units)]
        return pltpu.make_async_copy(source, down_ref.at[n], sems.at[count + n])

    for n in range(count):
        gate_copy(n).start()
    for n in range(blocks):
        down_copy(n).start()
    for n in range(count):
        gate_copy(n).wait()
        r = jnp.dot(x_ref[...], pair_ref[n], preferred_element_type=f32)
        gate = r[:, 0:tile]
        h_ref[:, n * tile : (n + 1) * tile] = (gate / (1.0 + jnp.exp(-gate)) * r[:, tile:]).astype(bf16)
    sub = outs[0].shape[0]
    for n in range(blocks):
        down_copy(n).wait()
        y = lax.dot_general(h_ref[...], down_ref[n], (((1,), (1,)), ((), ())), preferred_element_type=f32).astype(bf16)
        for p, out in enumerate(outs):
            out[:, n * rows : (n + 1) * rows] = y[p * sub : (p + 1) * sub, :]


def feed_forward(x, weights, units, parts, tile=128, rows=512):
    tok, width = x.shape
    count = units // tile
    blocks = width // rows
    sub = tok // parts
    return pl.pallas_call(
        functools.partial(unit_kernel, units=units, tile=tile, rows=rows),
        in_specs=[pl.BlockSpec(memory_space=pltpu.VMEM), pl.BlockSpec(memory_space=pltpu.HBM)],
        out_specs=[pl.BlockSpec(memory_space=pltpu.VMEM)] * parts,
        out_shape=[jax.ShapeDtypeStruct((sub, width), bf16)] * parts,
        scratch_shapes=[
            pltpu.VMEM((count, width, 2 * tile), bf16),
            pltpu.VMEM((blocks, rows, units), bf16),
            pltpu.VMEM((tok, units), bf16),
            pltpu.SemaphoreType.DMA((count + blocks,)),
        ],
        compiler_params=pltpu.CompilerParams(vmem_limit_bytes=50 << 20),
        name="units",
    )(x, weights)


def line_kernel(*refs, lines):
    each = (len(refs) - lines) // lines
    for n in range(lines):
        for m in range(each):
            piece = refs[n * each + m]
            rows = piece.shape[0]
            refs[lines * each + n][m * rows : (m + 1) * rows, :] = piece[...]


def lined_up(*lines):
    rows, width = lines[0][0].shape
    shape = jax.ShapeDtypeStruct((rows * len(lines[0]), width), bf16)
    return pl.pallas_call(
        functools.partial(line_kernel, lines=len(lines)),
        out_shape=[shape] * len(lines),
        compiler_params=pltpu.CompilerParams(vmem_limit_bytes=8 << 20),
        name="lines",
    )(*[piece for line in lines for piece in line])


def shifted(value, by):
    count = lax.axis_size("tp")
    return lax.ppermute(value, "tp", [(i, (i + by) % count) for i in range(count)])


SIDE = 4


def moved(value, z=0, y=0, other=False):
    pairs = []
    for a in range(SIDE):
        for b in range(SIDE):
            for c in range(2):
                goal = ((a + z) % SIDE * SIDE + (b + y) % SIDE) * 2 + (1 - c if other else c)
                pairs.append(((a * SIDE + b) * 2 + c, goal))
    return lax.ppermute(value, "sp", pairs)


def on_device(
    query_rows,
    key_rows,
    value_rows,
    query_gain,
    key_gain,
    residual,
    out_weight,
    mix_gain,
    gate_weight,
    up_weight,
    down_weight,
):
    tok = query_rows.shape[0]
    parts = lax.axis_size("tp")
    units = gate_weight.shape[1]
    core = lax.axis_index("sp") % 2
    place = jnp.stack([lax.axis_index("tp"), core])
    q, kv_a, kv_b, woven, payload, kept = prepare(
        query_rows, key_rows, value_rows, query_gain, key_gain, gate_weight, up_weight, down_weight, out_weight, residual
    )
    weights = lax.all_gather(woven, "sp", axis=0, tiled=True)

    a_line, b_line = lined_up(
        [kv_a] + [moved(kv_a, y=d) for d in (1, -1, 2)], [kv_b] + [moved(kv_b, z=d) for d in (1, -1, 2)]
    )
    near = [moved(a_line, z=1), moved(a_line, z=-1), moved(b_line, y=1), moved(b_line, y=-1)]
    far = [moved(a_line, z=2), moved(b_line, y=2)]
    lines = [a_line, b_line, moved(a_line, other=True), moved(b_line, other=True)]

    payload, lines = lax.optimization_barrier((payload, lines))
    sent = [payload] + [shifted(payload, -r) for r in range(1, parts)]

    state = flash(q, lines, None, tok, False)
    state, near = lax.optimization_barrier((state, near))
    near_swapped = [moved(v, other=True) for v in near]
    state = flash(q, near, state, tok, False)
    state, far = lax.optimization_barrier((state, far))
    far_swapped = [moved(v, other=True) for v in far]
    state = flash(q, near_swapped, state, tok, False)
    state, sent = lax.optimization_barrier((state, sent))
    swapped = [kept] + [moved(s[: kept.shape[0]], other=True) for s in sent[1:]]
    attended = flash(q, far + far_swapped, state, tok, True)

    att_parts = [attended] + [shifted(attended, -r) for r in range(1, parts)]
    own_rows, normed = project(place, att_parts, sent, swapped, mix_gain)
    unit_parts = feed_forward(normed, weights, units, parts)
    unit_sum = unit_parts[0].astype(f32)
    for r in range(1, parts):
        unit_sum = unit_sum + shifted(unit_parts[r], r).astype(f32)
    return (own_rows.astype(f32) + 0.5 * unit_sum).astype(bf16)


def solution(mesh):
    placed = (
        P("sp", "tp"),
        P("sp", "tp"),
        P("sp", "tp"),
        P(),
        P(),
        P(("sp", "tp"), None),
        P("tp", None),
        P(),
        P("sp", "tp"),
        P("sp", "tp"),
        P("tp", "sp"),
    )
    return jax.shard_map(
        on_device, mesh=mesh, in_specs=placed, out_specs=P(("sp", "tp"), None), check_vma=False
    )
```

```python
import functools

import jax
import jax.numpy as jnp
from jax import lax
from jax.experimental import pallas as pl
from jax.experimental.pallas import tpu as pltpu
from jax.sharding import PartitionSpec as P

GRID = 64
norm_eps = 1e-06
theta_base = 10000.0
LOG2E = 1.4426950408889634
f32 = jnp.float32
bf16 = jnp.bfloat16


def angle_tables(first_row, rows, head_dim):
    quarter = head_dim // 4
    frequency = jnp.power(theta_base, -2.0 * jnp.arange(quarter, dtype=f32) / (head_dim // 2))
    places = jnp.concatenate([first_row + jnp.arange(rows, dtype=jnp.int32), jnp.arange(GRID, dtype=jnp.int32)])
    angles = places.astype(f32)[:, None] * frequency
    cosine, sine = lax.optimization_barrier((jnp.cos(angles), jnp.sin(angles)))
    is_row = (jnp.arange(rows + GRID) < rows)[:, None]
    zero = jnp.zeros_like(cosine)

    def placed(lead, trail):
        return jnp.concatenate(
            [
                jnp.where(is_row, lead, zero),
                jnp.where(is_row, trail, zero),
                jnp.where(is_row, zero, lead),
                jnp.where(is_row, zero, trail),
            ],
            axis=1,
        )

    return placed(cosine, cosine), placed(-sine, sine)


def prepare_kernel(
    core, q_hbm, k_hbm, v_hbm, g_hbm, u_hbm, d_hbm, w_hbm, r_hbm, qg_ref, kg_ref, cos_ref, sin_ref,
    q_out, a_out, b_out, woven, sent, kept,
    q_ref, k_ref, v_ref, g_ref, u_ref, d_ref, w_ref, r_ref, sems, *, rows, head_dim, heads, tile,
):
    tok = rows * GRID
    half = kept.shape[0]
    first_half = pl.ds(pl.multiple_of(core[0] * half, half), half)
    other_half = pl.ds(pl.multiple_of((1 - core[0]) * half, half), half)
    moves = [
        (k_hbm, k_ref),
        (v_hbm, v_ref),
        (q_hbm, q_ref),
        (g_hbm, g_ref),
        (u_hbm, u_ref),
        (d_hbm, d_ref),
        (w_hbm.at[first_half, :], w_ref.at[pl.ds(0, half), :]),
        (w_hbm.at[other_half, :], w_ref.at[pl.ds(half, half), :]),
        (r_hbm, r_ref),
        (w_ref.at[pl.ds(0, half), :], sent.at[pl.ds(0, half), :]),
        (w_ref.at[pl.ds(half, half), :], kept),
        (r_ref, sent.at[pl.ds(half, r_hbm.shape[0]), :]),
    ]
    copies = [pltpu.make_async_copy(x, y, sems.at[n]) for n, (x, y) in enumerate(moves)]
    for c in copies[:9]:
        c.start()

    def spread(ref):
        both = ref[0:rows, :][:, None, :] + ref[rows : rows + GRID, :][None, :, :]
        return both.reshape(tok, head_dim)

    cosine = spread(cos_ref)
    sine = spread(sin_ref)
    lane = lax.broadcasted_iota(jnp.int32, (tok, head_dim), 1)
    first = (lane % (head_dim // 2)) < head_dim // 4
    quarter = head_dim // 4

    def prepared(raw, gain):
        x = raw.astype(f32)
        x = x * lax.rsqrt(jnp.mean(x * x, axis=-1, keepdims=True) + norm_eps) * gain
        partner = jnp.where(first, pltpu.roll(x, head_dim - quarter, 1), pltpu.roll(x, quarter, 1))
        return (x * cosine + partner * sine).astype(bf16)

    copies[0].wait()
    copies[1].wait()
    keys = prepared(k_ref[...], kg_ref[...])
    for n, out in enumerate((a_out, b_out)):
        part = slice(n * tok // 2, (n + 1) * tok // 2)
        out[:, 0:head_dim] = keys[part, :]
        out[:, head_dim:] = v_ref[part, :]
    for n in (6, 7, 8):
        copies[n].wait()
        copies[n + 3].start()
    copies[2].wait()
    for h in range(heads):
        q_out[h * tok : (h + 1) * tok, :] = prepared(q_ref[:, h * head_dim : (h + 1) * head_dim], qg_ref[...])
    for n in (3, 4, 5):
        copies[n].wait()
    units = g_ref.shape[1]
    for n in range(units // tile):
        part = slice(n * tile, (n + 1) * tile)
        woven[:, 2 * n * tile : (2 * n + 1) * tile] = g_ref[:, part]
        woven[:, (2 * n + 1) * tile : (2 * n + 2) * tile] = u_ref[:, part]
    woven[:, 2 * units :] = d_ref[...]
    for n in (9, 10, 11):
        copies[n].wait()


def prepare(query_rows, key_rows, value_rows, query_gain, key_gain, gate, up, down, out_weight, residual, tile=128):
    tok, width = query_rows.shape
    head_dim = query_gain.shape[0]
    rows = tok // GRID
    cosine, sine = angle_tables(lax.axis_index("sp") * rows, rows, head_dim)
    hbm = pl.BlockSpec(memory_space=pltpu.HBM)
    vmem = pl.BlockSpec(memory_space=pltpu.VMEM)
    big = (query_rows, key_rows, value_rows, gate, up, down.T)
    half = out_weight.shape[0] // 2
    return pl.pallas_call(
        functools.partial(prepare_kernel, rows=rows, head_dim=head_dim, heads=width // head_dim, tile=tile),
        in_specs=[pl.BlockSpec(memory_space=pltpu.SMEM)] + [hbm] * 8 + [vmem] * 4,
        out_specs=[vmem] * 4 + [hbm] * 2,
        out_shape=(
            jax.ShapeDtypeStruct((tok * (width // head_dim), head_dim), bf16),
            jax.ShapeDtypeStruct((tok // 2, 2 * head_dim), bf16),
            jax.ShapeDtypeStruct((tok // 2, 2 * head_dim), bf16),
            jax.ShapeDtypeStruct((gate.shape[0], 3 * gate.shape[1]), bf16),
            jax.ShapeDtypeStruct((half + residual.shape[0], residual.shape[1]), bf16),
            jax.ShapeDtypeStruct((half, residual.shape[1]), bf16),
        ),
        scratch_shapes=[pltpu.VMEM(x.shape, bf16) for x in (*big, out_weight, residual)] + [pltpu.SemaphoreType.DMA((12,))],
        compiler_params=pltpu.CompilerParams(vmem_limit_bytes=60 * 1024 * 1024),
        name="prepare",
    )(
        (lax.axis_index("sp") % 2)[None], *big, out_weight, residual, query_gain[None, :], key_gain[None, :], cosine, sine
    )


def flash_kernel(*refs, pieces, scale, first, last):
    q_ref = refs[0]
    kv_refs = refs[1 : 1 + pieces]
    refs = refs[1 + pieces :]
    if not first:
        m_in, acc_in = refs[0:2]
        refs = refs[2:]
    if last:
        o_ref = refs[0]
        refs = refs[1:]
    else:
        m_out, acc_out = refs[0:2]
        refs = refs[2:]
    head_dim = q_ref.shape[1]
    q = q_ref[...]
    if first:
        m = jnp.full((q.shape[0], 128), -jnp.inf, f32)
        acc = jnp.zeros((q.shape[0], 2 * head_dim), f32)
    else:
        m = m_in[...]
        acc = acc_in[...]

    def scores(n):
        return lax.dot_general(q, kv_refs[n][:, 0:head_dim], (((1,), (1,)), ((), ())), preferred_element_type=f32)

    following = scores(0)
    for n in range(pieces):
        values = kv_refs[n][:, head_dim:]
        values = jnp.concatenate([values, jnp.ones_like(values)], axis=1)
        s = following * scale
        if n + 1 < pieces:
            following = scores(n + 1)
        new = jnp.maximum(m, jnp.max(s, axis=1, keepdims=True))
        w = jnp.exp2(s - new[:, 0:1]).astype(bf16)
        factor = jnp.exp2(m - new)
        acc = acc * factor[:, 0:1] + jnp.dot(w, values, preferred_element_type=f32)
        m = new
    if last:
        o_ref[...] = (acc[:, 0:head_dim] / acc[:, head_dim:]).astype(bf16)
    else:
        m_out[...] = m
        acc_out[...] = acc


def flash(q, kv, state, tok, last, tile=256):
    rows, head_dim = q.shape
    heads = rows // tok
    pieces = len(kv)
    piece = kv[0].shape
    tiles = tok // tile
    held = [pl.BlockSpec((tile, 128), lambda i: (i, 0)), pl.BlockSpec((tile, 2 * head_dim), lambda i: (i, 0))]
    held_shape = (jax.ShapeDtypeStruct((rows, 128), f32), jax.ShapeDtypeStruct((rows, 2 * head_dim), f32))
    first = state is None
    return pl.pallas_call(
        functools.partial(flash_kernel, pieces=pieces, scale=head_dim**-0.5 * LOG2E, first=first, last=last),
        grid=(rows // tile,),
        in_specs=[pl.BlockSpec((tile, head_dim), lambda i: (i, 0))]
        + [pl.BlockSpec(piece, lambda i: (0, 0))] * pieces
        + ([] if first else held),
        out_specs=pl.BlockSpec((tile, head_dim), lambda i: (i % tiles, i // tiles)) if last else tuple(held),
        out_shape=jax.ShapeDtypeStruct((tok, heads * head_dim), bf16) if last else held_shape,
        compiler_params=pltpu.CompilerParams(dimension_semantics=("arbitrary",), vmem_limit_bytes=12 << 20),
        cost_estimate=pl.CostEstimate(
            flops=4 * rows * piece[0] * pieces * head_dim,
            bytes_accessed=4 * piece[0] * pieces * head_dim,
            transcendentals=rows * piece[0] * pieces,
        ),
        name="flash_last" if last else "flash_first" if first else "flash_more",
    )(q, *kv, *([] if first else state))


def project_kernel(place, *refs, parts, tile):
    att = refs[0:parts]
    sent = refs[parts : 2 * parts]
    swapped = refs[2 * parts : 3 * parts]
    gain_ref, own_ref, norm_ref, up_ref = refs[3 * parts :]
    step = pl.program_id(0)
    half = swapped[0].shape[0]
    sub = sent[0].shape[0] - half
    cols = pl.ds(pl.multiple_of(step * tile, tile), tile)
    total = None
    for a, w, o in zip(att, sent, swapped):
        rolled = []
        for r in range(parts):
            rows = pl.ds(pl.multiple_of(((place[0] + r) % parts) * sub, sub), sub)
            halves = [a[rows, pl.ds(pl.multiple_of(c * half, half), half)] for c in (place[1], 1 - place[1])]
            rolled.append(jnp.concatenate(halves, axis=1))
        weight = jnp.concatenate([w[0:half, :], o[...]], axis=0)
        part = jnp.dot(jnp.concatenate(rolled, axis=0), weight, preferred_element_type=f32).astype(bf16).astype(f32)
        total = part if total is None else total + part
    for r in range(parts):
        updated = (sent[r][half:, :].astype(f32) + total[r * sub : (r + 1) * sub, :]).astype(bf16)
        up_ref[r * sub : (r + 1) * sub, cols] = updated

    @pl.when(step == pl.num_programs(0) - 1)
    def _():
        own_ref[...] = up_ref[0:sub, :]
        for r in range(2 * parts):
            some = slice(r * sub // 2, (r + 1) * sub // 2)
            x = up_ref[some, :].astype(f32)
            x = x * lax.rsqrt(jnp.mean(x * x, axis=-1, keepdims=True) + norm_eps)
            norm_ref[some, :] = (x * gain_ref[...]).astype(bf16)


def project(place, att, sent, swapped, gain, tile=512):
    parts = len(att)
    tok, part_width = att[0].shape
    both, width = sent[0].shape
    half = swapped[0].shape[0]
    sub = both - half
    return pl.pallas_call(
        functools.partial(project_kernel, parts=parts, tile=tile),
        grid_spec=pltpu.PrefetchScalarGridSpec(
            num_scalar_prefetch=1,
            grid=(width // tile,),
            in_specs=[pl.BlockSpec((tok, part_width), lambda i, p: (0, 0))] * parts
            + [pl.BlockSpec((both, tile), lambda i, p: (0, i))] * parts
            + [pl.BlockSpec((half, tile), lambda i, p: (0, i))] * parts
            + [pl.BlockSpec((1, width), lambda i, p: (0, 0))],
            out_specs=(
                pl.BlockSpec((sub, width), lambda i, p: (0, 0)),
                pl.BlockSpec((tok, width), lambda i, p: (0, 0)),
            ),
            scratch_shapes=[pltpu.VMEM((tok, width), bf16)],
        ),
        out_shape=(jax.ShapeDtypeStruct((sub, width), bf16), jax.ShapeDtypeStruct((tok, width), bf16)),
        compiler_params=pltpu.CompilerParams(dimension_semantics=("arbitrary",), vmem_limit_bytes=16 << 20),
        name="project",
    )(place, *att, *sent, *swapped, gain[None, :])


def unit_kernel(x_ref, w_hbm, *refs, units, tile, rows, ahead=3):
    outs = refs[:-4]
    pair_ref, down_ref, h_ref, sems = refs[-4:]
    count = units // tile
    blocks = down_ref.shape[0]

    def gate_copy(n):
        return pltpu.make_async_copy(w_hbm.at[:, pl.ds(2 * n * tile, 2 * tile)], pair_ref.at[n], sems.at[n])

    def down_copy(n):
        source = w_hbm.at[pl.ds(n * rows, rows), pl.ds(2 * units, units)]
        return pltpu.make_async_copy(source, down_ref.at[n], sems.at[count + n])

    copies = [gate_copy(n) for n in range(count)] + [down_copy(n) for n in range(blocks)]

    def arrive(n):
        copies[n].wait()
        if n + ahead < len(copies):
            copies[n + ahead].start()

    for n in range(ahead):
        copies[n].start()
    for n in range(count):
        arrive(n)
        r = jnp.dot(x_ref[...], pair_ref[n], preferred_element_type=f32)
        gate = r[:, 0:tile]
        h_ref[:, n * tile : (n + 1) * tile] = (gate / (1.0 + jnp.exp(-gate)) * r[:, tile:]).astype(bf16)
    sub = outs[0].shape[0]
    for n in range(blocks):
        arrive(count + n)
        y = lax.dot_general(h_ref[...], down_ref[n], (((1,), (1,)), ((), ())), preferred_element_type=f32).astype(bf16)
        for p, out in enumerate(outs):
            out[:, n * rows : (n + 1) * rows] = y[p * sub : (p + 1) * sub, :]


def feed_forward(x, weights, units, parts, tile=128, rows=512):
    tok, width = x.shape
    count = units // tile
    blocks = width // rows
    sub = tok // parts
    return pl.pallas_call(
        functools.partial(unit_kernel, units=units, tile=tile, rows=rows),
        in_specs=[pl.BlockSpec(memory_space=pltpu.VMEM), pl.BlockSpec(memory_space=pltpu.HBM)],
        out_specs=[pl.BlockSpec(memory_space=pltpu.VMEM)] * parts,
        out_shape=[jax.ShapeDtypeStruct((sub, width), bf16)] * parts,
        scratch_shapes=[
            pltpu.VMEM((count, width, 2 * tile), bf16),
            pltpu.VMEM((blocks, rows, units), bf16),
            pltpu.VMEM((tok, units), bf16),
            pltpu.SemaphoreType.DMA((count + blocks,)),
        ],
        compiler_params=pltpu.CompilerParams(vmem_limit_bytes=50 << 20),
        name="units",
    )(x, weights)


def line_kernel(*refs, lines):
    each = (len(refs) - lines) // lines
    for n in range(lines):
        for m in range(each):
            piece = refs[n * each + m]
            rows = piece.shape[0]
            refs[lines * each + n][m * rows : (m + 1) * rows, :] = piece[...]


def lined_up(*lines):
    rows, width = lines[0][0].shape
    shape = jax.ShapeDtypeStruct((rows * len(lines[0]), width), bf16)
    return pl.pallas_call(
        functools.partial(line_kernel, lines=len(lines)),
        out_shape=[shape] * len(lines),
        compiler_params=pltpu.CompilerParams(vmem_limit_bytes=8 << 20),
        name="lines",
    )(*[piece for line in lines for piece in line])


def shifted(value, by):
    count = lax.axis_size("tp")
    return lax.ppermute(value, "tp", [(i, (i + by) % count) for i in range(count)])


SIDE = 4


def moved(value, z=0, y=0, other=False):
    pairs = []
    for a in range(SIDE):
        for b in range(SIDE):
            for c in range(2):
                goal = ((a + z) % SIDE * SIDE + (b + y) % SIDE) * 2 + (1 - c if other else c)
                pairs.append(((a * SIDE + b) * 2 + c, goal))
    return lax.ppermute(value, "sp", pairs)


def on_device(
    query_rows,
    key_rows,
    value_rows,
    query_gain,
    key_gain,
    residual,
    out_weight,
    mix_gain,
    gate_weight,
    up_weight,
    down_weight,
):
    tok = query_rows.shape[0]
    parts = lax.axis_size("tp")
    units = gate_weight.shape[1]
    core = lax.axis_index("sp") % 2
    place = jnp.stack([lax.axis_index("tp"), core])
    q, kv_a, kv_b, woven, payload, kept = prepare(
        query_rows, key_rows, value_rows, query_gain, key_gain, gate_weight, up_weight, down_weight, out_weight, residual
    )
    weights = lax.all_gather(woven, "sp", axis=0, tiled=True)

    a_line, b_line = lined_up(
        [kv_a] + [moved(kv_a, y=d) for d in (1, -1, 2)], [kv_b] + [moved(kv_b, z=d) for d in (1, -1, 2)]
    )
    near = [moved(a_line, z=1), moved(a_line, z=-1), moved(b_line, y=1), moved(b_line, y=-1)]
    far = [moved(a_line, z=2), moved(b_line, y=2)]
    lines = [a_line, b_line, moved(a_line, other=True), moved(b_line, other=True)]

    sent = [payload] + [shifted(payload, -r) for r in range(1, parts)]

    state = flash(q, lines, None, tok, False)
    state, near = lax.optimization_barrier((state, near))
    near_swapped = [moved(v, other=True) for v in near]
    state = flash(q, near, state, tok, False)
    state, far = lax.optimization_barrier((state, far))
    far_swapped = [moved(v, other=True) for v in far]
    state = flash(q, near_swapped, state, tok, False)
    attended = flash(q, far + far_swapped, state, tok, True)
    attended, sent = lax.optimization_barrier((attended, sent))
    swapped = [kept] + [moved(s[: kept.shape[0]], other=True) for s in sent[1:]]

    att_parts = [attended] + [shifted(attended, -r) for r in range(1, parts)]
    own_rows, normed = project(place, att_parts, sent, swapped, mix_gain)
    unit_parts = feed_forward(normed, weights, units, parts)
    unit_sum = unit_parts[0].astype(f32)
    for r in range(1, parts):
        unit_sum = unit_sum + shifted(unit_parts[r], r).astype(f32)
    return (own_rows.astype(f32) + 0.5 * unit_sum).astype(bf16)


def solution(mesh):
    placed = (
        P("sp", "tp"),
        P("sp", "tp"),
        P("sp", "tp"),
        P(),
        P(),
        P(("sp", "tp"), None),
        P("tp", None),
        P(),
        P("sp", "tp"),
        P("sp", "tp"),
        P("tp", "sp"),
    )
    return jax.shard_map(
        on_device, mesh=mesh, in_specs=placed, out_specs=P(("sp", "tp"), None), check_vma=False
    )
```

```python
import functools

import jax
import jax.numpy as jnp
from jax import lax
from jax.experimental import pallas as pl
from jax.experimental.pallas import tpu as pltpu
from jax.sharding import PartitionSpec as P

GRID = 64
norm_eps = 1e-06
theta_base = 10000.0
LOG2E = 1.4426950408889634
f32 = jnp.float32
bf16 = jnp.bfloat16


def angle_tables(first_row, rows, head_dim):
    quarter = head_dim // 4
    frequency = jnp.power(theta_base, -2.0 * jnp.arange(quarter, dtype=f32) / (head_dim // 2))
    places = jnp.concatenate([first_row + jnp.arange(rows, dtype=jnp.int32), jnp.arange(GRID, dtype=jnp.int32)])
    angles = places.astype(f32)[:, None] * frequency
    cosine, sine = lax.optimization_barrier((jnp.cos(angles), jnp.sin(angles)))
    is_row = (jnp.arange(rows + GRID) < rows)[:, None]
    zero = jnp.zeros_like(cosine)

    def placed(lead, trail):
        return jnp.concatenate(
            [
                jnp.where(is_row, lead, zero),
                jnp.where(is_row, trail, zero),
                jnp.where(is_row, zero, lead),
                jnp.where(is_row, zero, trail),
            ],
            axis=1,
        )

    return placed(cosine, cosine), placed(-sine, sine)


def prepare_kernel(
    core, q_hbm, k_hbm, v_hbm, g_hbm, u_hbm, d_hbm, w_hbm, r_hbm, qg_ref, kg_ref, cos_ref, sin_ref,
    q_out, a_out, b_out, woven, sent, kept,
    q_ref, k_ref, v_ref, g_ref, u_ref, d_ref, w_ref, r_ref, sems, *, rows, head_dim, heads, tile,
):
    tok = rows * GRID
    half = kept.shape[0]
    first_half = pl.ds(pl.multiple_of(core[0] * half, half), half)
    other_half = pl.ds(pl.multiple_of((1 - core[0]) * half, half), half)
    moves = [
        (k_hbm, k_ref),
        (v_hbm, v_ref),
        (q_hbm, q_ref),
        (g_hbm, g_ref),
        (u_hbm, u_ref),
        (d_hbm, d_ref),
        (w_hbm.at[first_half, :], w_ref.at[pl.ds(0, half), :]),
        (w_hbm.at[other_half, :], w_ref.at[pl.ds(half, half), :]),
        (r_hbm, r_ref),
        (w_ref.at[pl.ds(0, half), :], sent.at[pl.ds(0, half), :]),
        (w_ref.at[pl.ds(half, half), :], kept),
        (r_ref, sent.at[pl.ds(half, r_hbm.shape[0]), :]),
    ]
    copies = [pltpu.make_async_copy(x, y, sems.at[n]) for n, (x, y) in enumerate(moves)]
    for c in copies[:9]:
        c.start()

    def spread(ref):
        both = ref[0:rows, :][:, None, :] + ref[rows : rows + GRID, :][None, :, :]
        return both.reshape(tok, head_dim)

    cosine = spread(cos_ref)
    sine = spread(sin_ref)
    lane = lax.broadcasted_iota(jnp.int32, (tok, head_dim), 1)
    first = (lane % (head_dim // 2)) < head_dim // 4
    quarter = head_dim // 4

    def prepared(raw, gain):
        x = raw.astype(f32)
        x = x * lax.rsqrt(jnp.mean(x * x, axis=-1, keepdims=True) + norm_eps) * gain
        partner = jnp.where(first, pltpu.roll(x, head_dim - quarter, 1), pltpu.roll(x, quarter, 1))
        return (x * cosine + partner * sine).astype(bf16)

    copies[0].wait()
    copies[1].wait()
    keys = prepared(k_ref[...], kg_ref[...])
    for n, out in enumerate((a_out, b_out)):
        part = slice(n * tok // 2, (n + 1) * tok // 2)
        out[:, 0:head_dim] = keys[part, :]
        out[:, head_dim:] = v_ref[part, :]
    for n in (6, 7, 8):
        copies[n].wait()
        copies[n + 3].start()
    copies[2].wait()
    for h in range(heads):
        q_out[h * tok : (h + 1) * tok, :] = prepared(q_ref[:, h * head_dim : (h + 1) * head_dim], qg_ref[...])
    for n in (3, 4, 5):
        copies[n].wait()
    units = g_ref.shape[1]
    for n in range(units // tile):
        part = slice(n * tile, (n + 1) * tile)
        woven[:, 2 * n * tile : (2 * n + 1) * tile] = g_ref[:, part]
        woven[:, (2 * n + 1) * tile : (2 * n + 2) * tile] = u_ref[:, part]
    woven[:, 2 * units :] = d_ref[...]
    for n in (9, 10, 11):
        copies[n].wait()


def prepare(query_rows, key_rows, value_rows, query_gain, key_gain, gate, up, down, out_weight, residual, tile=128):
    tok, width = query_rows.shape
    head_dim = query_gain.shape[0]
    rows = tok // GRID
    cosine, sine = angle_tables(lax.axis_index("sp") * rows, rows, head_dim)
    hbm = pl.BlockSpec(memory_space=pltpu.HBM)
    vmem = pl.BlockSpec(memory_space=pltpu.VMEM)
    big = (query_rows, key_rows, value_rows, gate, up, down.T)
    half = out_weight.shape[0] // 2
    return pl.pallas_call(
        functools.partial(prepare_kernel, rows=rows, head_dim=head_dim, heads=width // head_dim, tile=tile),
        in_specs=[pl.BlockSpec(memory_space=pltpu.SMEM)] + [hbm] * 8 + [vmem] * 4,
        out_specs=[vmem] * 4 + [hbm] * 2,
        out_shape=(
            jax.ShapeDtypeStruct((tok * (width // head_dim), head_dim), bf16),
            jax.ShapeDtypeStruct((tok // 2, 2 * head_dim), bf16),
            jax.ShapeDtypeStruct((tok // 2, 2 * head_dim), bf16),
            jax.ShapeDtypeStruct((gate.shape[0], 3 * gate.shape[1]), bf16),
            jax.ShapeDtypeStruct((half + residual.shape[0], residual.shape[1]), bf16),
            jax.ShapeDtypeStruct((half, residual.shape[1]), bf16),
        ),
        scratch_shapes=[pltpu.VMEM(x.shape, bf16) for x in (*big, out_weight, residual)] + [pltpu.SemaphoreType.DMA((12,))],
        compiler_params=pltpu.CompilerParams(vmem_limit_bytes=60 * 1024 * 1024),
        name="prepare",
    )(
        (lax.axis_index("sp") % 2)[None], *big, out_weight, residual, query_gain[None, :], key_gain[None, :], cosine, sine
    )


def flash_kernel(*refs, pieces, scale, first, last):
    q_ref = refs[0]
    kv_refs = refs[1 : 1 + pieces]
    refs = refs[1 + pieces :]
    if not first:
        m_in, acc_in = refs[0:2]
        refs = refs[2:]
    if last:
        o_ref = refs[0]
        refs = refs[1:]
    else:
        m_out, acc_out = refs[0:2]
        refs = refs[2:]
    head_dim = q_ref.shape[1]
    q = q_ref[...]
    if first:
        m = jnp.full((q.shape[0], 128), -jnp.inf, f32)
        acc = jnp.zeros((q.shape[0], 2 * head_dim), f32)
    else:
        m = m_in[...]
        acc = acc_in[...]

    def scores(n):
        return lax.dot_general(q, kv_refs[n][:, 0:head_dim], (((1,), (1,)), ((), ())), preferred_element_type=f32)

    following = scores(0)
    for n in range(pieces):
        values = kv_refs[n][:, head_dim:]
        values = jnp.concatenate([values, jnp.ones_like(values)], axis=1)
        s = following * scale
        if n + 1 < pieces:
            following = scores(n + 1)
        new = jnp.maximum(m, jnp.max(s, axis=1, keepdims=True))
        w = jnp.exp2(s - new[:, 0:1]).astype(bf16)
        factor = jnp.exp2(m - new)
        acc = acc * factor[:, 0:1] + jnp.dot(w, values, preferred_element_type=f32)
        m = new
    if last:
        o_ref[...] = (acc[:, 0:head_dim] / acc[:, head_dim:]).astype(bf16)
    else:
        m_out[...] = m
        acc_out[...] = acc


def flash(q, kv, state, tok, last, tile=256):
    rows, head_dim = q.shape
    heads = rows // tok
    pieces = len(kv)
    piece = kv[0].shape
    tiles = tok // tile
    held = [pl.BlockSpec((tile, 128), lambda i: (i, 0)), pl.BlockSpec((tile, 2 * head_dim), lambda i: (i, 0))]
    held_shape = (jax.ShapeDtypeStruct((rows, 128), f32), jax.ShapeDtypeStruct((rows, 2 * head_dim), f32))
    first = state is None
    return pl.pallas_call(
        functools.partial(flash_kernel, pieces=pieces, scale=head_dim**-0.5 * LOG2E, first=first, last=last),
        grid=(rows // tile,),
        in_specs=[pl.BlockSpec((tile, head_dim), lambda i: (i, 0))]
        + [pl.BlockSpec(piece, lambda i: (0, 0))] * pieces
        + ([] if first else held),
        out_specs=pl.BlockSpec((tile, head_dim), lambda i: (i % tiles, i // tiles)) if last else tuple(held),
        out_shape=jax.ShapeDtypeStruct((tok, heads * head_dim), bf16) if last else held_shape,
        compiler_params=pltpu.CompilerParams(dimension_semantics=("arbitrary",), vmem_limit_bytes=12 << 20),
        cost_estimate=pl.CostEstimate(
            flops=4 * rows * piece[0] * pieces * head_dim,
            bytes_accessed=4 * piece[0] * pieces * head_dim,
            transcendentals=rows * piece[0] * pieces,
        ),
        name="flash_last" if last else "flash_first" if first else "flash_more",
    )(q, *kv, *([] if first else state))


def project_kernel(place, *refs, parts, tile, res_rows):
    att = refs[0:parts]
    sent = refs[parts : 2 * parts]
    swapped = refs[2 * parts : 3 * parts]
    gain_ref, own_ref, norm_ref, up_ref = refs[3 * parts :]
    step = pl.program_id(0)
    sub = res_rows
    half = sent[0].shape[0] - sub
    cols = pl.ds(pl.multiple_of(step * tile, tile), tile)
    total = None
    for a, w, o in zip(att, sent, swapped):
        rolled = []
        for r in range(parts):
            rows = pl.ds(pl.multiple_of(((place[0] + r) % parts) * sub, sub), sub)
            halves = [a[rows, pl.ds(pl.multiple_of(c * half, half), half)] for c in (place[1], 1 - place[1])]
            rolled.append(jnp.concatenate(halves, axis=1))
        weight = jnp.concatenate([w[0:half, :], o[0:half, :]], axis=0)
        part = jnp.dot(jnp.concatenate(rolled, axis=0), weight, preferred_element_type=f32).astype(bf16).astype(f32)
        total = part if total is None else total + part
    for r in range(parts):
        updated = (sent[r][half:, :].astype(f32) + total[r * sub : (r + 1) * sub, :]).astype(bf16)
        up_ref[r * sub : (r + 1) * sub, cols] = updated

    @pl.when(step == pl.num_programs(0) - 1)
    def _():
        own_ref[...] = up_ref[0:sub, :]
        for r in range(2 * parts):
            some = slice(r * sub // 2, (r + 1) * sub // 2)
            x = up_ref[some, :].astype(f32)
            x = x * lax.rsqrt(jnp.mean(x * x, axis=-1, keepdims=True) + norm_eps)
            norm_ref[some, :] = (x * gain_ref[...]).astype(bf16)


def project(place, att, sent, swapped, gain, tile=512):
    parts = len(att)
    tok, part_width = att[0].shape
    both, width = sent[0].shape
    half = swapped[0].shape[0]
    sub = both - half
    return pl.pallas_call(
        functools.partial(project_kernel, parts=parts, tile=tile, res_rows=sub),
        grid_spec=pltpu.PrefetchScalarGridSpec(
            num_scalar_prefetch=1,
            grid=(width // tile,),
            in_specs=[pl.BlockSpec((tok, part_width), lambda i, p: (0, 0))] * parts
            + [pl.BlockSpec((both, tile), lambda i, p: (0, i))] * parts
            + [pl.BlockSpec((half, tile), lambda i, p: (0, i))] * parts
            + [pl.BlockSpec((1, width), lambda i, p: (0, 0))],
            out_specs=(
                pl.BlockSpec((sub, width), lambda i, p: (0, 0)),
                pl.BlockSpec((tok, width), lambda i, p: (0, 0)),
            ),
            scratch_shapes=[pltpu.VMEM((tok, width), bf16)],
        ),
        out_shape=(jax.ShapeDtypeStruct((sub, width), bf16), jax.ShapeDtypeStruct((tok, width), bf16)),
        compiler_params=pltpu.CompilerParams(dimension_semantics=("arbitrary",), vmem_limit_bytes=16 << 20),
        name="project",
    )(place, *att, *sent, *swapped, gain[None, :])


def unit_kernel(x_ref, w_hbm, *refs, units, tile, rows, split, ahead):
    outs = refs[:-4]
    pair_ref, down_ref, h_ref, sems = refs[-4:]
    count = units // tile
    blocks = down_ref.shape[0]
    width = x_ref.shape[1]

    def tile_copies(n):
        found = []
        for m in range(split):
            if n < count:
                part = pl.ds(m * width // split, width // split)
                source = w_hbm.at[part, pl.ds(2 * n * tile, 2 * tile)]
                target = pair_ref.at[n, part, :]
            else:
                b = n - count
                source = w_hbm.at[pl.ds(b * rows + m * rows // split, rows // split), pl.ds(2 * units, units)]
                target = down_ref.at[b, pl.ds(m * rows // split, rows // split), :]
            found.append(pltpu.make_async_copy(source, target, sems.at[n * split + m]))
        return found

    copies = [tile_copies(n) for n in range(count + blocks)]

    def begin(n):
        if n < count + blocks:
            for c in copies[n]:
                c.start()

    def arrive(n):
        for c in copies[n]:
            c.wait()
        begin(n + ahead)

    def product(n):
        return jnp.dot(x_ref[...], pair_ref[n], preferred_element_type=f32)

    for n in range(ahead):
        begin(n)
    arrive(0)
    following = product(0)
    for n in range(count):
        arrive(n + 1)
        r = following
        if n + 1 < count:
            following = product(n + 1)
        gate = r[:, 0:tile]
        h_ref[:, n * tile : (n + 1) * tile] = (gate / (1.0 + jnp.exp(-gate)) * r[:, tile:]).astype(bf16)
    sub = outs[0].shape[0]
    for n in range(blocks):
        if n > 0:
            arrive(count + n)
        y = lax.dot_general(h_ref[...], down_ref[n], (((1,), (1,)), ((), ())), preferred_element_type=f32).astype(bf16)
        for p, out in enumerate(outs):
            out[:, n * rows : (n + 1) * rows] = y[p * sub : (p + 1) * sub, :]


def feed_forward(x, weights, units, parts, tile=128, rows=512, split=4, ahead=4):
    tok, width = x.shape
    count = units // tile
    blocks = width // rows
    sub = tok // parts
    return pl.pallas_call(
        functools.partial(unit_kernel, units=units, tile=tile, rows=rows, split=split, ahead=ahead),
        in_specs=[pl.BlockSpec(memory_space=pltpu.VMEM), pl.BlockSpec(memory_space=pltpu.HBM)],
        out_specs=[pl.BlockSpec(memory_space=pltpu.VMEM)] * parts,
        out_shape=[jax.ShapeDtypeStruct((sub, width), bf16)] * parts,
        scratch_shapes=[
            pltpu.VMEM((count, width, 2 * tile), bf16),
            pltpu.VMEM((blocks, rows, units), bf16),
            pltpu.VMEM((tok, units), bf16),
            pltpu.SemaphoreType.DMA(((count + blocks) * split,)),
        ],
        compiler_params=pltpu.CompilerParams(vmem_limit_bytes=50 << 20),
        name="units",
    )(x, weights)


def line_kernel(*refs, lines):
    each = (len(refs) - lines) // lines
    for n in range(lines):
        for m in range(each):
            piece = refs[n * each + m]
            rows = piece.shape[0]
            refs[lines * each + n][m * rows : (m + 1) * rows, :] = piece[...]


def lined_up(*lines):
    rows, width = lines[0][0].shape
    shape = jax.ShapeDtypeStruct((rows * len(lines[0]), width), bf16)
    return pl.pallas_call(
        functools.partial(line_kernel, lines=len(lines)),
        out_shape=[shape] * len(lines),
        compiler_params=pltpu.CompilerParams(vmem_limit_bytes=8 << 20),
        name="lines",
    )(*[piece for line in lines for piece in line])


def shifted(value, by):
    count = lax.axis_size("tp")
    return lax.ppermute(value, "tp", [(i, (i + by) % count) for i in range(count)])


SIDE = 4


def moved(value, z=0, y=0, other=False):
    pairs = []
    for a in range(SIDE):
        for b in range(SIDE):
            for c in range(2):
                goal = ((a + z) % SIDE * SIDE + (b + y) % SIDE) * 2 + (1 - c if other else c)
                pairs.append(((a * SIDE + b) * 2 + c, goal))
    return lax.ppermute(value, "sp", pairs)


def on_device(
    query_rows,
    key_rows,
    value_rows,
    query_gain,
    key_gain,
    residual,
    out_weight,
    mix_gain,
    gate_weight,
    up_weight,
    down_weight,
):
    tok = query_rows.shape[0]
    parts = lax.axis_size("tp")
    units = gate_weight.shape[1]
    core = lax.axis_index("sp") % 2
    place = jnp.stack([lax.axis_index("tp"), core])
    q, kv_a, kv_b, woven, payload, kept = prepare(
        query_rows, key_rows, value_rows, query_gain, key_gain, gate_weight, up_weight, down_weight, out_weight, residual
    )
    weights = lax.all_gather(woven, "sp", axis=0, tiled=True)

    a_parts = [kv_a]
    b_parts = [kv_b]
    for d in (1, -1, 2):
        a_parts.append(moved(kv_a, y=d))
    for d in (1, -1, 2):
        b_parts.append(moved(kv_b, z=d))
    a_line, b_line = lined_up(a_parts, b_parts)
    near = [moved(a_line, z=1), moved(a_line, z=-1), moved(b_line, y=1), moved(b_line, y=-1)]
    far = [moved(a_line, z=2), moved(b_line, y=2)]
    lines = [a_line, b_line, moved(a_line, other=True), moved(b_line, other=True)]

    sent = [payload]
    for r in range(1, parts):
        sent.append(shifted(payload, -r))

    state = flash(q, lines, None, tok, False)
    state, near = lax.optimization_barrier((state, near))
    near_swapped = [moved(v, other=True) for v in near]
    state = flash(q, near, state, tok, False)
    state, far = lax.optimization_barrier((state, far))
    far_swapped = [moved(v, other=True) for v in far]
    state = flash(q, near_swapped, state, tok, False)
    state, sent = lax.optimization_barrier((state, sent))
    swapped = [kept] + [moved(s, other=True) for s in sent[1:]]
    attended = flash(q, far + far_swapped, state, tok, True)

    att_parts = [attended] + [shifted(attended, -r) for r in range(1, parts)]
    own_rows, normed = project(place, att_parts, sent, swapped, mix_gain)
    unit_parts = feed_forward(normed, weights, units, parts)
    unit_sum = unit_parts[0].astype(f32)
    for r in range(1, parts):
        unit_sum = unit_sum + shifted(unit_parts[r], r).astype(f32)
    return (own_rows.astype(f32) + 0.5 * unit_sum).astype(bf16)


def solution(mesh):
    placed = (
        P("sp", "tp"),
        P("sp", "tp"),
        P("sp", "tp"),
        P(),
        P(),
        P(("sp", "tp"), None),
        P("tp", None),
        P(),
        P("sp", "tp"),
        P("sp", "tp"),
        P("tp", "sp"),
    )
    return jax.shard_map(on_device, mesh=mesh, in_specs=placed, out_specs=P(("sp", "tp"), None), check_vma=False)
```

```python
import functools

import jax
import jax.numpy as jnp
from jax import lax
from jax.experimental import pallas as pl
from jax.experimental.pallas import tpu as pltpu
from jax.sharding import PartitionSpec as P

GRID = 64
norm_eps = 1e-06
theta_base = 10000.0
LOG2E = 1.4426950408889634
f32 = jnp.float32
bf16 = jnp.bfloat16


def angle_tables(first_row, rows, head_dim):
    quarter = head_dim // 4
    frequency = jnp.power(theta_base, -2.0 * jnp.arange(quarter, dtype=f32) / (head_dim // 2))
    places = jnp.concatenate([first_row + jnp.arange(rows, dtype=jnp.int32), jnp.arange(GRID, dtype=jnp.int32)])
    angles = places.astype(f32)[:, None] * frequency
    cosine, sine = lax.optimization_barrier((jnp.cos(angles), jnp.sin(angles)))
    is_row = (jnp.arange(rows + GRID) < rows)[:, None]
    zero = jnp.zeros_like(cosine)

    def placed(lead, trail):
        return jnp.concatenate(
            [
                jnp.where(is_row, lead, zero),
                jnp.where(is_row, trail, zero),
                jnp.where(is_row, zero, lead),
                jnp.where(is_row, zero, trail),
            ],
            axis=1,
        )

    return placed(cosine, cosine), placed(-sine, sine)


def prepare_kernel(
    core, q_hbm, k_hbm, v_hbm, g_hbm, u_hbm, d_hbm, w_hbm, r_hbm, qg_ref, kg_ref, cos_ref, sin_ref,
    q_out, kv_out, woven, sent, kept,
    q_ref, k_ref, v_ref, g_ref, u_ref, d_ref, w_ref, r_ref, sems, *, rows, head_dim, heads, tile,
):
    tok = rows * GRID
    half = kept.shape[0]
    first_half = pl.ds(pl.multiple_of(core[0] * half, half), half)
    other_half = pl.ds(pl.multiple_of((1 - core[0]) * half, half), half)
    moves = [
        (k_hbm, k_ref),
        (v_hbm, v_ref),
        (q_hbm, q_ref),
        (g_hbm, g_ref),
        (u_hbm, u_ref),
        (d_hbm, d_ref),
        (w_hbm.at[first_half, :], w_ref.at[pl.ds(0, half), :]),
        (w_hbm.at[other_half, :], w_ref.at[pl.ds(half, half), :]),
        (r_hbm, r_ref),
        (w_ref.at[pl.ds(0, half), :], sent.at[pl.ds(0, half), :]),
        (w_ref.at[pl.ds(half, half), :], kept),
        (r_ref, sent.at[pl.ds(half, r_hbm.shape[0]), :]),
    ]
    copies = [pltpu.make_async_copy(x, y, sems.at[n]) for n, (x, y) in enumerate(moves)]
    for c in copies[:9]:
        c.start()

    def spread(ref):
        both = ref[0:rows, :][:, None, :] + ref[rows : rows + GRID, :][None, :, :]
        return both.reshape(tok, head_dim)

    cosine = spread(cos_ref)
    sine = spread(sin_ref)
    lane = lax.broadcasted_iota(jnp.int32, (tok, head_dim), 1)
    first = (lane % (head_dim // 2)) < head_dim // 4
    quarter = head_dim // 4

    def prepared(raw, gain):
        x = raw.astype(f32)
        x = x * lax.rsqrt(jnp.mean(x * x, axis=-1, keepdims=True) + norm_eps) * gain
        partner = jnp.where(first, pltpu.roll(x, head_dim - quarter, 1), pltpu.roll(x, quarter, 1))
        return (x * cosine + partner * sine).astype(bf16)

    copies[0].wait()
    copies[1].wait()
    kv_out[:, 0:head_dim] = prepared(k_ref[...], kg_ref[...])
    kv_out[:, head_dim:] = v_ref[...]
    for n in (6, 7, 8):
        copies[n].wait()
        copies[n + 3].start()
    copies[2].wait()
    for h in range(heads):
        q_out[h * tok : (h + 1) * tok, :] = prepared(q_ref[:, h * head_dim : (h + 1) * head_dim], qg_ref[...])
    for n in (3, 4, 5):
        copies[n].wait()
    units = g_ref.shape[1]
    for n in range(units // tile):
        part = slice(n * tile, (n + 1) * tile)
        woven[:, 2 * n * tile : (2 * n + 1) * tile] = g_ref[:, part]
        woven[:, (2 * n + 1) * tile : (2 * n + 2) * tile] = u_ref[:, part]
    woven[:, 2 * units :] = d_ref[...]
    for n in (9, 10, 11):
        copies[n].wait()


def prepare(query_rows, key_rows, value_rows, query_gain, key_gain, gate, up, down, out_weight, residual, tile=128):
    tok, width = query_rows.shape
    head_dim = query_gain.shape[0]
    rows = tok // GRID
    cosine, sine = angle_tables(lax.axis_index("sp") * rows, rows, head_dim)
    hbm = pl.BlockSpec(memory_space=pltpu.HBM)
    vmem = pl.BlockSpec(memory_space=pltpu.VMEM)
    big = (query_rows, key_rows, value_rows, gate, up, down.T)
    half = out_weight.shape[0] // 2
    return pl.pallas_call(
        functools.partial(prepare_kernel, rows=rows, head_dim=head_dim, heads=width // head_dim, tile=tile),
        in_specs=[pl.BlockSpec(memory_space=pltpu.SMEM)] + [hbm] * 8 + [vmem] * 4,
        out_specs=[vmem] * 3 + [hbm] * 2,
        out_shape=(
            jax.ShapeDtypeStruct((tok * (width // head_dim), head_dim), bf16),
            jax.ShapeDtypeStruct((tok, 2 * head_dim), bf16),
            jax.ShapeDtypeStruct((gate.shape[0], 3 * gate.shape[1]), bf16),
            jax.ShapeDtypeStruct((half + residual.shape[0], residual.shape[1]), bf16),
            jax.ShapeDtypeStruct((half, residual.shape[1]), bf16),
        ),
        scratch_shapes=[pltpu.VMEM(x.shape, bf16) for x in (*big, out_weight, residual)] + [pltpu.SemaphoreType.DMA((12,))],
        compiler_params=pltpu.CompilerParams(vmem_limit_bytes=60 * 1024 * 1024),
        name="prepare",
    )(
        (lax.axis_index("sp") % 2)[None], *big, out_weight, residual, query_gain[None, :], key_gain[None, :], cosine, sine
    )


def flash_kernel(*refs, pieces, scale, first, last, block=1024):
    q_ref = refs[0]
    kv_refs = refs[1 : 1 + pieces]
    refs = refs[1 + pieces :]
    if not first:
        m_in, acc_in = refs[0:2]
        refs = refs[2:]
    if last:
        o_ref = refs[0]
        refs = refs[1:]
    else:
        m_out, acc_out = refs[0:2]
        refs = refs[2:]
    head_dim = q_ref.shape[1]
    q = q_ref[...]
    if first:
        m = jnp.full((q.shape[0], 128), -jnp.inf, f32)
        acc = jnp.zeros((q.shape[0], 2 * head_dim), f32)
    else:
        m = m_in[...]
        acc = acc_in[...]

    parts = [(ref, slice(r, r + block)) for ref in kv_refs for r in range(0, ref.shape[0], block)]

    def scores(n):
        ref, rows = parts[n]
        return lax.dot_general(q, ref[rows, 0:head_dim], (((1,), (1,)), ((), ())), preferred_element_type=f32)

    following = scores(0)
    for n, (ref, rows) in enumerate(parts):
        values = ref[rows, head_dim:]
        values = jnp.concatenate([values, jnp.ones_like(values)], axis=1)
        s = following * scale
        if n + 1 < len(parts):
            following = scores(n + 1)
        new = jnp.maximum(m, jnp.max(s, axis=1, keepdims=True))
        w = jnp.exp2(s - new[:, 0:1]).astype(bf16)
        factor = jnp.exp2(m - new)
        acc = acc * factor[:, 0:1] + jnp.dot(w, values, preferred_element_type=f32)
        m = new
    if last:
        o_ref[...] = (acc[:, 0:head_dim] / acc[:, head_dim:]).astype(bf16)
    else:
        m_out[...] = m
        acc_out[...] = acc


def flash(q, kv, state, tok, last, tile=256):
    rows, head_dim = q.shape
    heads = rows // tok
    pieces = len(kv)
    piece = kv[0].shape
    tiles = tok // tile
    held = [pl.BlockSpec((tile, 128), lambda i: (i, 0)), pl.BlockSpec((tile, 2 * head_dim), lambda i: (i, 0))]
    held_shape = (jax.ShapeDtypeStruct((rows, 128), f32), jax.ShapeDtypeStruct((rows, 2 * head_dim), f32))
    first = state is None
    return pl.pallas_call(
        functools.partial(flash_kernel, pieces=pieces, scale=head_dim**-0.5 * LOG2E, first=first, last=last),
        grid=(rows // tile,),
        in_specs=[pl.BlockSpec((tile, head_dim), lambda i: (i, 0))]
        + [pl.BlockSpec(piece, lambda i: (0, 0))] * pieces
        + ([] if first else held),
        out_specs=pl.BlockSpec((tile, head_dim), lambda i: (i % tiles, i // tiles)) if last else tuple(held),
        out_shape=jax.ShapeDtypeStruct((tok, heads * head_dim), bf16) if last else held_shape,
        compiler_params=pltpu.CompilerParams(dimension_semantics=("arbitrary",), vmem_limit_bytes=12 << 20),
        cost_estimate=pl.CostEstimate(
            flops=4 * rows * piece[0] * pieces * head_dim,
            bytes_accessed=4 * piece[0] * pieces * head_dim,
            transcendentals=rows * piece[0] * pieces,
        ),
        name="flash_last" if last else "flash_first" if first else "flash_more",
    )(q, *kv, *([] if first else state))


def layer_kernel(place, *refs, parts, tile, sub, units, unit_tile):
    att = refs[0:parts]
    sent = refs[parts : 2 * parts]
    swapped = refs[2 * parts : 3 * parts]
    gain_ref, w_hbm, own_ref = refs[3 * parts : 3 * parts + 3]
    outs = refs[3 * parts + 3 : -5]
    x_ref, pair_ref, down_ref, h_ref, sems = refs[-5:]
    step = pl.program_id(0)
    half = sent[0].shape[0] - sub
    count = units // unit_tile
    blocks, rows, _ = down_ref.shape

    def copies():
        found = []
        for n in range(count):
            source = w_hbm.at[:, pl.ds(2 * n * unit_tile, 2 * unit_tile)]
            found.append(pltpu.make_async_copy(source, pair_ref.at[n], sems.at[n]))
        for n in range(blocks):
            source = w_hbm.at[pl.ds(n * rows, rows), pl.ds(2 * units, units)]
            found.append(pltpu.make_async_copy(source, down_ref.at[n], sems.at[count + n]))
        return found

    @pl.when(step == 0)
    def _():
        for c in copies():
            c.start()

    cols = pl.ds(pl.multiple_of(step * tile, tile), tile)
    total = None
    for a, w, o in zip(att, sent, swapped):
        rolled = []
        for r in range(parts):
            some = pl.ds(pl.multiple_of(((place[0] + r) % parts) * sub, sub), sub)
            halves = [a[some, pl.ds(pl.multiple_of(c * half, half), half)] for c in (place[1], 1 - place[1])]
            rolled.append(jnp.concatenate(halves, axis=1))
        weight = jnp.concatenate([w[0:half, :], o[0:half, :]], axis=0)
        part = jnp.dot(jnp.concatenate(rolled, axis=0), weight, preferred_element_type=f32).astype(bf16).astype(f32)
        total = part if total is None else total + part
    for r in range(parts):
        updated = (sent[r][half:, :].astype(f32) + total[r * sub : (r + 1) * sub, :]).astype(bf16)
        x_ref[r * sub : (r + 1) * sub, cols] = updated

    @pl.when(step == pl.num_programs(0) - 1)
    def _():
        own_ref[...] = x_ref[0:sub, :]
        for r in range(2 * parts):
            some = slice(r * sub // 2, (r + 1) * sub // 2)
            x = x_ref[some, :].astype(f32)
            x = x * lax.rsqrt(jnp.mean(x * x, axis=-1, keepdims=True) + norm_eps)
            x_ref[some, :] = (x * gain_ref[...]).astype(bf16)
        for c in copies():
            c.wait()

        def product(n):
            return jnp.dot(x_ref[...], pair_ref[n], preferred_element_type=f32)

        following = product(0)
        for n in range(count):
            r = following
            if n + 1 < count:
                following = product(n + 1)
            gate = r[:, 0:unit_tile]
            hidden = gate / (1.0 + jnp.exp(-gate)) * r[:, unit_tile:]
            h_ref[:, n * unit_tile : (n + 1) * unit_tile] = hidden.astype(bf16)
        for n in range(blocks):
            y = lax.dot_general(h_ref[...], down_ref[n], (((1,), (1,)), ((), ())), preferred_element_type=f32).astype(bf16)
            for p, out in enumerate(outs):
                out[:, n * rows : (n + 1) * rows] = y[p * sub : (p + 1) * sub, :]


def layer(place, att, sent, swapped, gain, weights, units, tile=512, unit_tile=128, rows=512):
    parts = len(att)
    tok, part_width = att[0].shape
    both, width = sent[0].shape
    sub = tok // parts
    count = units // unit_tile
    blocks = width // rows
    return pl.pallas_call(
        functools.partial(layer_kernel, parts=parts, tile=tile, sub=sub, units=units, unit_tile=unit_tile),
        grid_spec=pltpu.PrefetchScalarGridSpec(
            num_scalar_prefetch=1,
            grid=(width // tile,),
            in_specs=[pl.BlockSpec((tok, part_width), lambda i, p: (0, 0))] * parts
            + [pl.BlockSpec((both, tile), lambda i, p: (0, i))] * parts
            + [pl.BlockSpec((s.shape[0], tile), lambda i, p: (0, i)) for s in swapped]
            + [pl.BlockSpec((1, width), lambda i, p: (0, 0)), pl.BlockSpec(memory_space=pltpu.HBM)],
            out_specs=[pl.BlockSpec((sub, width), lambda i, p: (0, 0))] * (1 + parts),
            scratch_shapes=[
                pltpu.VMEM((tok, width), bf16),
                pltpu.VMEM((count, width, 2 * unit_tile), bf16),
                pltpu.VMEM((blocks, rows, units), bf16),
                pltpu.VMEM((tok, units), bf16),
                pltpu.SemaphoreType.DMA((count + blocks,)),
            ],
        ),
        out_shape=[jax.ShapeDtypeStruct((sub, width), bf16)] * (1 + parts),
        compiler_params=pltpu.CompilerParams(dimension_semantics=("arbitrary",), vmem_limit_bytes=50 << 20),
        name="layer",
    )(place, *att, *sent, *swapped, gain[None, :], weights)


def line_kernel(*refs):
    rows = refs[0].shape[0]
    for n, piece in enumerate(refs[:-1]):
        refs[-1][n * rows : (n + 1) * rows, :] = piece[...]


def lined_up(*pieces):
    rows, width = pieces[0].shape
    return pl.pallas_call(
        line_kernel,
        out_shape=jax.ShapeDtypeStruct((rows * len(pieces), width), bf16),
        compiler_params=pltpu.CompilerParams(vmem_limit_bytes=8 << 20),
        name="lines",
    )(*pieces)


def shifted(value, by):
    count = lax.axis_size("tp")
    return lax.ppermute(value, "tp", [(i, (i + by) % count) for i in range(count)])


SIDE = 4


def sp_index(z, y, core):
    return (z % SIDE * SIDE + y % SIDE) * 2 + core


def crossed(value, by, turned):
    pairs = []
    for z in range(SIDE):
        for y in range(SIDE):
            for core in range(2):
                along_y = (core == 0) != turned
                goal = sp_index(z, y + by, core) if along_y else sp_index(z + by, y, core)
                pairs.append((sp_index(z, y, core), goal))
    return lax.ppermute(value, "sp", pairs)


def other_core(value):
    count = 2 * SIDE * SIDE
    return lax.ppermute(value, "sp", [(n, n ^ 1) for n in range(count)])


def on_device(
    query_rows,
    key_rows,
    value_rows,
    query_gain,
    key_gain,
    residual,
    out_weight,
    mix_gain,
    gate_weight,
    up_weight,
    down_weight,
):
    tok = query_rows.shape[0]
    parts = lax.axis_size("tp")
    units = gate_weight.shape[1]
    core = lax.axis_index("sp") % 2
    place = jnp.stack([lax.axis_index("tp"), core])
    q, kv, woven, payload, kept = prepare(
        query_rows, key_rows, value_rows, query_gain, key_gain, gate_weight, up_weight, down_weight, out_weight, residual
    )
    weights = lax.all_gather(woven, "sp", axis=0, tiled=True)

    steps = (2, 1, -1)
    line = [kv]
    for d in steps:
        line.append(crossed(kv, d, False))
    line = lined_up(*line)
    turned = []
    for d in steps:
        turned.append(crossed(line, d, True))
    far, *near = turned

    sent = [payload]
    for r in range(1, parts):
        sent.append(shifted(payload, -r))

    state = flash(q, [line, other_core(line)], None, tok, False)
    state, near = lax.optimization_barrier((state, near))
    near_swapped = [other_core(v) for v in near]
    state = flash(q, near, state, tok, False)
    state = flash(q, near_swapped, state, tok, False)
    state, far, sent = lax.optimization_barrier((state, far, sent))
    far_swapped = other_core(far)
    swapped = [kept]
    for r in range(1, parts):
        swapped.append(other_core(sent[r]))
    state = flash(q, [far], state, tok, False)
    attended = flash(q, [far_swapped], state, tok, True)

    att_parts = [attended] + [shifted(attended, -r) for r in range(1, parts)]
    own_rows, *unit_parts = layer(place, att_parts, sent, swapped, mix_gain, weights, units)
    unit_sum = unit_parts[0].astype(f32)
    for r in range(1, parts):
        unit_sum = unit_sum + shifted(unit_parts[r], r).astype(f32)
    return (own_rows.astype(f32) + 0.5 * unit_sum).astype(bf16)


def solution(mesh):
    placed = (
        P("sp", "tp"),
        P("sp", "tp"),
        P("sp", "tp"),
        P(),
        P(),
        P(("sp", "tp"), None),
        P("tp", None),
        P(),
        P("sp", "tp"),
        P("sp", "tp"),
        P("tp", "sp"),
    )
    return jax.shard_map(on_device, mesh=mesh, in_specs=placed, out_specs=P(("sp", "tp"), None), check_vma=False)
```

```python
import functools

import jax
import jax.numpy as jnp
from jax import lax
from jax.experimental import pallas as pl
from jax.experimental.pallas import tpu as pltpu
from jax.sharding import PartitionSpec as P

GRID = 64
norm_eps = 1e-06
theta_base = 10000.0
LOG2E = 1.4426950408889634
f32 = jnp.float32
bf16 = jnp.bfloat16


def angle_tables(first_row, rows, head_dim):
    quarter = head_dim // 4
    frequency = jnp.power(theta_base, -2.0 * jnp.arange(quarter, dtype=f32) / (head_dim // 2))
    places = jnp.concatenate([first_row + jnp.arange(rows, dtype=jnp.int32), jnp.arange(GRID, dtype=jnp.int32)])
    angles = places.astype(f32)[:, None] * frequency
    cosine, sine = lax.optimization_barrier((jnp.cos(angles), jnp.sin(angles)))
    is_row = (jnp.arange(rows + GRID) < rows)[:, None]
    zero = jnp.zeros_like(cosine)

    def placed(lead, trail):
        return jnp.concatenate(
            [
                jnp.where(is_row, lead, zero),
                jnp.where(is_row, trail, zero),
                jnp.where(is_row, zero, lead),
                jnp.where(is_row, zero, trail),
            ],
            axis=1,
        )

    return placed(cosine, cosine), placed(-sine, sine)


def prepare_kernel(
    core, q_hbm, k_hbm, v_hbm, g_hbm, u_hbm, d_hbm, w_hbm, r_hbm, qg_ref, kg_ref, cos_ref, sin_ref,
    q_out, kv_out, woven, sent, kept,
    q_ref, k_ref, v_ref, g_ref, u_ref, d_ref, w_ref, r_ref, sems, *, rows, head_dim, heads, tile,
):
    tok = rows * GRID
    half = kept.shape[0]
    first_half = pl.ds(pl.multiple_of(core[0] * half, half), half)
    other_half = pl.ds(pl.multiple_of((1 - core[0]) * half, half), half)
    moves = [
        (k_hbm, k_ref),
        (v_hbm, v_ref),
        (q_hbm, q_ref),
        (g_hbm, g_ref),
        (u_hbm, u_ref),
        (d_hbm, d_ref),
        (w_hbm.at[first_half, :], w_ref.at[pl.ds(0, half), :]),
        (w_hbm.at[other_half, :], w_ref.at[pl.ds(half, half), :]),
        (r_hbm, r_ref),
        (w_ref.at[pl.ds(0, half), :], sent.at[pl.ds(0, half), :]),
        (w_ref.at[pl.ds(half, half), :], kept),
        (r_ref, sent.at[pl.ds(half, r_hbm.shape[0]), :]),
    ]
    copies = [pltpu.make_async_copy(x, y, sems.at[n]) for n, (x, y) in enumerate(moves)]
    for c in copies[:9]:
        c.start()

    def spread(ref):
        both = ref[0:rows, :][:, None, :] + ref[rows : rows + GRID, :][None, :, :]
        return both.reshape(tok, head_dim)

    cosine = spread(cos_ref)
    sine = spread(sin_ref)
    lane = lax.broadcasted_iota(jnp.int32, (tok, head_dim), 1)
    first = (lane % (head_dim // 2)) < head_dim // 4
    quarter = head_dim // 4

    def prepared(raw, gain):
        x = raw.astype(f32)
        x = x * lax.rsqrt(jnp.mean(x * x, axis=-1, keepdims=True) + norm_eps) * gain
        partner = jnp.where(first, pltpu.roll(x, head_dim - quarter, 1), pltpu.roll(x, quarter, 1))
        return (x * cosine + partner * sine).astype(bf16)

    copies[0].wait()
    copies[1].wait()
    kv_out[:, 0:head_dim] = prepared(k_ref[...], kg_ref[...])
    kv_out[:, head_dim:] = v_ref[...]
    for n in (6, 7, 8):
        copies[n].wait()
        copies[n + 3].start()
    copies[2].wait()
    for h in range(heads):
        q_out[h * tok : (h + 1) * tok, :] = prepared(q_ref[:, h * head_dim : (h + 1) * head_dim], qg_ref[...])
    for n in (3, 4, 5):
        copies[n].wait()
    units = g_ref.shape[1]
    for n in range(units // tile):
        part = slice(n * tile, (n + 1) * tile)
        woven[:, 2 * n * tile : (2 * n + 1) * tile] = g_ref[:, part]
        woven[:, (2 * n + 1) * tile : (2 * n + 2) * tile] = u_ref[:, part]
    woven[:, 2 * units :] = d_ref[...]
    for n in (9, 10, 11):
        copies[n].wait()


def prepare(query_rows, key_rows, value_rows, query_gain, key_gain, gate, up, down, out_weight, residual, tile=128):
    tok, width = query_rows.shape
    head_dim = query_gain.shape[0]
    rows = tok // GRID
    cosine, sine = angle_tables(lax.axis_index("sp") * rows, rows, head_dim)
    hbm = pl.BlockSpec(memory_space=pltpu.HBM)
    vmem = pl.BlockSpec(memory_space=pltpu.VMEM)
    big = (query_rows, key_rows, value_rows, gate, up, down.T)
    half = out_weight.shape[0] // 2
    return pl.pallas_call(
        functools.partial(prepare_kernel, rows=rows, head_dim=head_dim, heads=width // head_dim, tile=tile),
        in_specs=[pl.BlockSpec(memory_space=pltpu.SMEM)] + [hbm] * 8 + [vmem] * 4,
        out_specs=[vmem] * 3 + [hbm] * 2,
        out_shape=(
            jax.ShapeDtypeStruct((tok * (width // head_dim), head_dim), bf16),
            jax.ShapeDtypeStruct((tok, 2 * head_dim), bf16),
            jax.ShapeDtypeStruct((gate.shape[0], 3 * gate.shape[1]), bf16),
            jax.ShapeDtypeStruct((half + residual.shape[0], residual.shape[1]), bf16),
            jax.ShapeDtypeStruct((half, residual.shape[1]), bf16),
        ),
        scratch_shapes=[pltpu.VMEM(x.shape, bf16) for x in (*big, out_weight, residual)] + [pltpu.SemaphoreType.DMA((12,))],
        compiler_params=pltpu.CompilerParams(vmem_limit_bytes=60 * 1024 * 1024),
        name="prepare",
    )(
        (lax.axis_index("sp") % 2)[None], *big, out_weight, residual, query_gain[None, :], key_gain[None, :], cosine, sine
    )


def flash_kernel(*refs, pieces, scale, first, last, block=1024):
    q_ref = refs[0]
    kv_refs = refs[1 : 1 + pieces]
    refs = refs[1 + pieces :]
    if not first:
        m_in, acc_in = refs[0:2]
        refs = refs[2:]
    if last:
        o_ref = refs[0]
        refs = refs[1:]
    else:
        m_out, acc_out = refs[0:2]
        refs = refs[2:]
    head_dim = q_ref.shape[1]
    q = q_ref[...]
    if first:
        m = jnp.full((q.shape[0], 128), -jnp.inf, f32)
        acc = jnp.zeros((q.shape[0], 2 * head_dim), f32)
    else:
        m = m_in[...]
        acc = acc_in[...]

    parts = [(ref, slice(r, r + block)) for ref in kv_refs for r in range(0, ref.shape[0], block)]

    def scores(n):
        ref, rows = parts[n]
        return lax.dot_general(q, ref[rows, 0:head_dim], (((1,), (1,)), ((), ())), preferred_element_type=f32)

    following = scores(0)
    for n, (ref, rows) in enumerate(parts):
        values = ref[rows, head_dim:]
        values = jnp.concatenate([values, jnp.ones_like(values)], axis=1)
        s = following * scale
        if n + 1 < len(parts):
            following = scores(n + 1)
        new = jnp.maximum(m, jnp.max(s, axis=1, keepdims=True))
        w = jnp.exp2(s - new[:, 0:1]).astype(bf16)
        factor = jnp.exp2(m - new)
        acc = acc * factor[:, 0:1] + jnp.dot(w, values, preferred_element_type=f32)
        m = new
    if last:
        o_ref[...] = (acc[:, 0:head_dim] / acc[:, head_dim:]).astype(bf16)
    else:
        m_out[...] = m
        acc_out[...] = acc


def flash(q, kv, state, tok, last, tile=256):
    rows, head_dim = q.shape
    heads = rows // tok
    pieces = len(kv)
    piece = kv[0].shape
    tiles = tok // tile
    held = [pl.BlockSpec((tile, 128), lambda i: (i, 0)), pl.BlockSpec((tile, 2 * head_dim), lambda i: (i, 0))]
    held_shape = (jax.ShapeDtypeStruct((rows, 128), f32), jax.ShapeDtypeStruct((rows, 2 * head_dim), f32))
    first = state is None
    return pl.pallas_call(
        functools.partial(flash_kernel, pieces=pieces, scale=head_dim**-0.5 * LOG2E, first=first, last=last),
        grid=(rows // tile,),
        in_specs=[pl.BlockSpec((tile, head_dim), lambda i: (i, 0))]
        + [pl.BlockSpec(piece, lambda i: (0, 0))] * pieces
        + ([] if first else held),
        out_specs=pl.BlockSpec((tile, head_dim), lambda i: (i % tiles, i // tiles)) if last else tuple(held),
        out_shape=jax.ShapeDtypeStruct((tok, heads * head_dim), bf16) if last else held_shape,
        compiler_params=pltpu.CompilerParams(dimension_semantics=("arbitrary",), vmem_limit_bytes=12 << 20),
        cost_estimate=pl.CostEstimate(
            flops=4 * rows * piece[0] * pieces * head_dim,
            bytes_accessed=4 * piece[0] * pieces * head_dim,
            transcendentals=rows * piece[0] * pieces,
        ),
        name="flash_last" if last else "flash_first" if first else "flash_more",
    )(q, *kv, *([] if first else state))


def layer_kernel(place, *refs, parts, tile, sub, units, unit_tile):
    att = refs[0:parts]
    sent = refs[parts : 2 * parts]
    swapped = refs[2 * parts : 3 * parts]
    gain_ref, w_hbm, own_ref = refs[3 * parts : 3 * parts + 3]
    out_1, out_2, rest_ref = refs[3 * parts + 3 : -5]
    x_ref, pair_ref, down_ref, h_ref, sems = refs[-5:]
    step = pl.program_id(0)
    half = sent[0].shape[0] - sub
    count = units // unit_tile
    blocks, rows, _ = down_ref.shape

    def copies():
        found = []
        for n in range(count):
            source = w_hbm.at[:, pl.ds(2 * n * unit_tile, 2 * unit_tile)]
            found.append(pltpu.make_async_copy(source, pair_ref.at[n], sems.at[n]))
        for n in range(blocks):
            source = w_hbm.at[pl.ds(n * rows, rows), pl.ds(2 * units, units)]
            found.append(pltpu.make_async_copy(source, down_ref.at[n], sems.at[count + n]))
        return found

    @pl.when(step == 0)
    def _():
        for c in copies():
            c.start()

    cols = pl.ds(pl.multiple_of(step * tile, tile), tile)
    total = None
    for a, w, o in zip(att, sent, swapped):
        rolled = []
        for r in range(parts):
            some = pl.ds(pl.multiple_of(((place[0] + r) % parts) * sub, sub), sub)
            halves = [a[some, pl.ds(pl.multiple_of(c * half, half), half)] for c in (place[1], 1 - place[1])]
            rolled.append(jnp.concatenate(halves, axis=1))
        weight = jnp.concatenate([w[0:half, :], o[0:half, :]], axis=0)
        part = jnp.dot(jnp.concatenate(rolled, axis=0), weight, preferred_element_type=f32).astype(bf16).astype(f32)
        total = part if total is None else total + part
    for r in range(parts):
        updated = (sent[r][half:, :].astype(f32) + total[r * sub : (r + 1) * sub, :]).astype(bf16)
        x_ref[r * sub : (r + 1) * sub, cols] = updated

    @pl.when(step == pl.num_programs(0) - 1)
    def _():
        own_ref[...] = x_ref[0:sub, :]
        for r in range(2 * parts):
            some = slice(r * sub // 2, (r + 1) * sub // 2)
            x = x_ref[some, :].astype(f32)
            x = x * lax.rsqrt(jnp.mean(x * x, axis=-1, keepdims=True) + norm_eps)
            x_ref[some, :] = (x * gain_ref[...]).astype(bf16)
        for c in copies():
            c.wait()

        def product(n):
            return jnp.dot(x_ref[...], pair_ref[n], preferred_element_type=f32)

        following = product(0)
        for n in range(count):
            r = following
            if n + 1 < count:
                following = product(n + 1)
            gate = r[:, 0:unit_tile]
            hidden = gate / (1.0 + jnp.exp(-gate)) * r[:, unit_tile:]
            h_ref[:, n * unit_tile : (n + 1) * unit_tile] = hidden.astype(bf16)
        rest_ref[0:sub, :] = h_ref[0:sub, :]
        rest_ref[sub:, :] = h_ref[3 * sub :, :]
        down_products(h_ref[sub : 3 * sub, :], down_ref, (out_1, out_2))


def down_products(hidden, down_ref, outs):
    blocks, rows, _ = down_ref.shape
    sub = outs[0].shape[0]
    for n in range(blocks):
        y = lax.dot_general(hidden, down_ref[n], (((1,), (1,)), ((), ())), preferred_element_type=f32).astype(bf16)
        for p, out in enumerate(outs):
            out[:, n * rows : (n + 1) * rows] = y[p * sub : (p + 1) * sub, :]


def rest_kernel(h_ref, w_hbm, out_0, out_3, down_ref, sems):
    blocks, rows, units = down_ref.shape
    copies = []
    for n in range(blocks):
        source = w_hbm.at[pl.ds(n * rows, rows), pl.ds(2 * units, units)]
        copies.append(pltpu.make_async_copy(source, down_ref.at[n], sems.at[n]))
    for c in copies:
        c.start()
    for c in copies:
        c.wait()
    down_products(h_ref[...], down_ref, (out_0, out_3))


def rest(hidden, weights, rows=512):
    tok, units = hidden.shape
    width = weights.shape[0]
    return pl.pallas_call(
        rest_kernel,
        in_specs=[pl.BlockSpec(memory_space=pltpu.VMEM), pl.BlockSpec(memory_space=pltpu.HBM)],
        out_shape=[jax.ShapeDtypeStruct((tok // 2, width), bf16)] * 2,
        scratch_shapes=[pltpu.VMEM((width // rows, rows, units), bf16), pltpu.SemaphoreType.DMA((width // rows,))],
        compiler_params=pltpu.CompilerParams(vmem_limit_bytes=50 << 20),
        name="rest",
    )(hidden, weights)


def layer(place, att, sent, swapped, gain, weights, units, tile=512, unit_tile=128, rows=512):
    parts = len(att)
    tok, part_width = att[0].shape
    both, width = sent[0].shape
    sub = tok // parts
    count = units // unit_tile
    blocks = width // rows
    return pl.pallas_call(
        functools.partial(layer_kernel, parts=parts, tile=tile, sub=sub, units=units, unit_tile=unit_tile),
        grid_spec=pltpu.PrefetchScalarGridSpec(
            num_scalar_prefetch=1,
            grid=(width // tile,),
            in_specs=[pl.BlockSpec((tok, part_width), lambda i, p: (0, 0))] * parts
            + [pl.BlockSpec((both, tile), lambda i, p: (0, i))] * parts
            + [pl.BlockSpec((s.shape[0], tile), lambda i, p: (0, i)) for s in swapped]
            + [pl.BlockSpec((1, width), lambda i, p: (0, 0)), pl.BlockSpec(memory_space=pltpu.HBM)],
            out_specs=[pl.BlockSpec((sub, width), lambda i, p: (0, 0))] * 3
            + [pl.BlockSpec((2 * sub, units), lambda i, p: (0, 0))],
            scratch_shapes=[
                pltpu.VMEM((tok, width), bf16),
                pltpu.VMEM((count, width, 2 * unit_tile), bf16),
                pltpu.VMEM((blocks, rows, units), bf16),
                pltpu.VMEM((tok, units), bf16),
                pltpu.SemaphoreType.DMA((count + blocks,)),
            ],
        ),
        out_shape=[jax.ShapeDtypeStruct((sub, width), bf16)] * 3 + [jax.ShapeDtypeStruct((2 * sub, units), bf16)],
        compiler_params=pltpu.CompilerParams(dimension_semantics=("arbitrary",), vmem_limit_bytes=50 << 20),
        name="layer",
    )(place, *att, *sent, *swapped, gain[None, :], weights)


def line_kernel(*refs):
    pieces, (whole, *halves) = refs[:-3], refs[-3:]
    rows = pieces[0].shape[0]
    each = len(pieces) // 2
    for n, piece in enumerate(pieces):
        whole[n * rows : (n + 1) * rows, :] = piece[...]
        halves[n // each][n % each * rows : (n % each + 1) * rows, :] = piece[...]


def lined_up(*pieces):
    rows, width = pieces[0].shape
    count = rows * len(pieces)
    return pl.pallas_call(
        line_kernel,
        out_shape=[jax.ShapeDtypeStruct((n, width), bf16) for n in (count, count // 2, count // 2)],
        compiler_params=pltpu.CompilerParams(vmem_limit_bytes=10 << 20),
        name="lines",
    )(*pieces)


def shifted(value, by):
    count = lax.axis_size("tp")
    return lax.ppermute(value, "tp", [(i, (i + by) % count) for i in range(count)])


SIDE = 4


def sp_index(z, y, core):
    return (z % SIDE * SIDE + y % SIDE) * 2 + core


def crossed(value, by, turned):
    pairs = []
    for z in range(SIDE):
        for y in range(SIDE):
            for core in range(2):
                along_y = (core == 0) != turned
                goal = sp_index(z, y + by, core) if along_y else sp_index(z + by, y, core)
                pairs.append((sp_index(z, y, core), goal))
    return lax.ppermute(value, "sp", pairs)


def other_core(value):
    count = 2 * SIDE * SIDE
    return lax.ppermute(value, "sp", [(n, n ^ 1) for n in range(count)])


def on_device(
    query_rows,
    key_rows,
    value_rows,
    query_gain,
    key_gain,
    residual,
    out_weight,
    mix_gain,
    gate_weight,
    up_weight,
    down_weight,
):
    tok = query_rows.shape[0]
    parts = lax.axis_size("tp")
    units = gate_weight.shape[1]
    core = lax.axis_index("sp") % 2
    place = jnp.stack([lax.axis_index("tp"), core])
    q, kv, woven, payload, kept = prepare(
        query_rows, key_rows, value_rows, query_gain, key_gain, gate_weight, up_weight, down_weight, out_weight, residual
    )
    weights = lax.all_gather(woven, "sp", axis=0, tiled=True)

    steps = (2, 1, -1)
    line = [kv]
    for d in steps:
        line.append(crossed(kv, d, False))
    line, *halves = lined_up(*line)
    near = []
    for d in (1, -1):
        near.append(crossed(line, d, True))
    far = []
    for n in range(2):
        far.append(crossed(halves[n], 2, True))

    sent = [payload]
    for r in range(1, parts):
        sent.append(shifted(payload, -r))

    state = flash(q, [line, other_core(line)], None, tok, False)
    state, near = lax.optimization_barrier((state, near))
    near_swapped = [other_core(v) for v in near]
    state = flash(q, near, state, tok, False)
    state = flash(q, near_swapped, state, tok, False)
    state, far[0] = lax.optimization_barrier((state, far[0]))
    far_swapped = [other_core(far[0])]
    state = flash(q, [far[0], far_swapped[0]], state, tok, False)
    state, far[1], sent = lax.optimization_barrier((state, far[1], sent))
    far_swapped.append(other_core(far[1]))
    swapped = [kept]
    for r in range(1, parts):
        swapped.append(other_core(sent[r]))
    attended = flash(q, [far[1], far_swapped[1]], state, tok, True)

    att_parts = [attended] + [shifted(attended, -r) for r in range(1, parts)]
    own_rows, part_1, part_2, hidden = layer(place, att_parts, sent, swapped, mix_gain, weights, units)
    part_0, part_3 = rest(hidden, weights)
    unit_sum = part_0.astype(f32)
    for r, part in ((1, part_1), (2, part_2), (3, part_3)):
        unit_sum = unit_sum + shifted(part, r).astype(f32)
    return (own_rows.astype(f32) + 0.5 * unit_sum).astype(bf16)


def solution(mesh):
    placed = (
        P("sp", "tp"),
        P("sp", "tp"),
        P("sp", "tp"),
        P(),
        P(),
        P(("sp", "tp"), None),
        P("tp", None),
        P(),
        P("sp", "tp"),
        P("sp", "tp"),
        P("tp", "sp"),
    )
    return jax.shard_map(on_device, mesh=mesh, in_specs=placed, out_specs=P(("sp", "tp"), None), check_vma=False)
```

```python
import functools

import jax
import jax.numpy as jnp
from jax import lax
from jax.experimental import pallas as pl
from jax.experimental.pallas import tpu as pltpu
from jax.sharding import PartitionSpec as P

GRID = 64
norm_eps = 1e-06
theta_base = 10000.0
LOG2E = 1.4426950408889634
f32 = jnp.float32
bf16 = jnp.bfloat16


def angle_tables(first_row, rows, head_dim):
    quarter = head_dim // 4
    frequency = jnp.power(theta_base, -2.0 * jnp.arange(quarter, dtype=f32) / (head_dim // 2))
    places = jnp.concatenate([first_row + jnp.arange(rows, dtype=jnp.int32), jnp.arange(GRID, dtype=jnp.int32)])
    angles = places.astype(f32)[:, None] * frequency
    cosine, sine = lax.optimization_barrier((jnp.cos(angles), jnp.sin(angles)))
    is_row = (jnp.arange(rows + GRID) < rows)[:, None]
    zero = jnp.zeros_like(cosine)

    def placed(lead, trail):
        return jnp.concatenate(
            [
                jnp.where(is_row, lead, zero),
                jnp.where(is_row, trail, zero),
                jnp.where(is_row, zero, lead),
                jnp.where(is_row, zero, trail),
            ],
            axis=1,
        )

    return placed(cosine, cosine), placed(-sine, sine)


def prepare_kernel(
    core, q_hbm, k_hbm, v_hbm, w_hbm, r_hbm, qg_ref, kg_ref, cos_ref, sin_ref,
    q_out, kv_out, sent, kept,
    q_ref, k_ref, v_ref, w_ref, r_ref, sems, *, rows, head_dim, heads,
):
    tok = rows * GRID
    half = kept.shape[0]
    first_half = pl.ds(pl.multiple_of(core[0] * half, half), half)
    other_half = pl.ds(pl.multiple_of((1 - core[0]) * half, half), half)
    moves = [
        (k_hbm, k_ref),
        (v_hbm, v_ref),
        (q_hbm, q_ref),
        (w_hbm.at[first_half, :], w_ref.at[pl.ds(0, half), :]),
        (w_hbm.at[other_half, :], w_ref.at[pl.ds(half, half), :]),
        (r_hbm, r_ref),
        (w_ref.at[pl.ds(0, half), :], sent.at[pl.ds(0, half), :]),
        (w_ref.at[pl.ds(half, half), :], kept),
        (r_ref, sent.at[pl.ds(half, r_hbm.shape[0]), :]),
    ]
    copies = [pltpu.make_async_copy(x, y, sems.at[n]) for n, (x, y) in enumerate(moves)]
    for c in copies[:6]:
        c.start()

    def spread(ref):
        both = ref[0:rows, :][:, None, :] + ref[rows : rows + GRID, :][None, :, :]
        return both.reshape(tok, head_dim)

    cosine = spread(cos_ref)
    sine = spread(sin_ref)
    lane = lax.broadcasted_iota(jnp.int32, (tok, head_dim), 1)
    first = (lane % (head_dim // 2)) < head_dim // 4
    quarter = head_dim // 4

    def prepared(raw, gain):
        x = raw.astype(f32)
        x = x * lax.rsqrt(jnp.mean(x * x, axis=-1, keepdims=True) + norm_eps) * gain
        partner = jnp.where(first, pltpu.roll(x, head_dim - quarter, 1), pltpu.roll(x, quarter, 1))
        return (x * cosine + partner * sine).astype(bf16)

    copies[0].wait()
    copies[1].wait()
    kv_out[:, 0:head_dim] = prepared(k_ref[...], kg_ref[...])
    kv_out[:, head_dim:] = v_ref[...]
    for n in (3, 4, 5):
        copies[n].wait()
        copies[n + 3].start()
    copies[2].wait()
    for h in range(heads):
        q_out[h * tok : (h + 1) * tok, :] = prepared(q_ref[:, h * head_dim : (h + 1) * head_dim], qg_ref[...])
    for n in (6, 7, 8):
        copies[n].wait()


def weave_kernel(g_hbm, u_hbm, d_hbm, woven, g_ref, u_ref, d_ref, sems, *, tile):
    moves = ((g_hbm, g_ref), (u_hbm, u_ref), (d_hbm, d_ref))
    copies = [pltpu.make_async_copy(x, y, sems.at[n]) for n, (x, y) in enumerate(moves)]
    for c in copies:
        c.start()
    for c in copies:
        c.wait()
    units = g_ref.shape[1]
    for n in range(units // tile):
        part = slice(n * tile, (n + 1) * tile)
        woven[:, 2 * n * tile : (2 * n + 1) * tile] = g_ref[:, part]
        woven[:, (2 * n + 1) * tile : (2 * n + 2) * tile] = u_ref[:, part]
    woven[:, 2 * units :] = d_ref[...]


def interleaved(gate, up, down, tile=128):
    big = (gate, up, down.T)
    return pl.pallas_call(
        functools.partial(weave_kernel, tile=tile),
        in_specs=[pl.BlockSpec(memory_space=pltpu.HBM)] * 3,
        out_shape=jax.ShapeDtypeStruct((gate.shape[0], 3 * gate.shape[1]), bf16),
        scratch_shapes=[pltpu.VMEM(x.shape, bf16) for x in big] + [pltpu.SemaphoreType.DMA((3,))],
        compiler_params=pltpu.CompilerParams(vmem_limit_bytes=60 * 1024 * 1024),
        name="weave",
    )(*big)


def prepare(query_rows, key_rows, value_rows, query_gain, key_gain, out_weight, residual):
    tok, width = query_rows.shape
    head_dim = query_gain.shape[0]
    rows = tok // GRID
    cosine, sine = angle_tables(lax.axis_index("sp") * rows, rows, head_dim)
    hbm = pl.BlockSpec(memory_space=pltpu.HBM)
    vmem = pl.BlockSpec(memory_space=pltpu.VMEM)
    big = (query_rows, key_rows, value_rows, out_weight, residual)
    half = out_weight.shape[0] // 2
    return pl.pallas_call(
        functools.partial(prepare_kernel, rows=rows, head_dim=head_dim, heads=width // head_dim),
        in_specs=[pl.BlockSpec(memory_space=pltpu.SMEM)] + [hbm] * 5 + [vmem] * 4,
        out_specs=[vmem] * 2 + [hbm] * 2,
        out_shape=(
            jax.ShapeDtypeStruct((tok * (width // head_dim), head_dim), bf16),
            jax.ShapeDtypeStruct((tok, 2 * head_dim), bf16),
            jax.ShapeDtypeStruct((half + residual.shape[0], residual.shape[1]), bf16),
            jax.ShapeDtypeStruct((half, residual.shape[1]), bf16),
        ),
        scratch_shapes=[pltpu.VMEM(x.shape, bf16) for x in big] + [pltpu.SemaphoreType.DMA((9,))],
        compiler_params=pltpu.CompilerParams(vmem_limit_bytes=60 * 1024 * 1024),
        name="prepare",
    )(
        (lax.axis_index("sp") % 2)[None], *big, query_gain[None, :], key_gain[None, :], cosine, sine
    )


def flash_kernel(*refs, pieces, scale, first, last, block=1024):
    q_ref = refs[0]
    kv_refs = refs[1 : 1 + pieces]
    refs = refs[1 + pieces :]
    if not first:
        m_in, acc_in = refs[0:2]
        refs = refs[2:]
    if last:
        o_ref = refs[0]
        refs = refs[1:]
    else:
        m_out, acc_out = refs[0:2]
        refs = refs[2:]
    head_dim = q_ref.shape[1]
    q = q_ref[...]
    if first:
        m = jnp.full((q.shape[0], 128), -jnp.inf, f32)
        acc = jnp.zeros((q.shape[0], 2 * head_dim), f32)
    else:
        m = m_in[...]
        acc = acc_in[...]

    parts = [(ref, slice(r, r + block)) for ref in kv_refs for r in range(0, ref.shape[0], block)]

    def scores(n):
        ref, rows = parts[n]
        return lax.dot_general(q, ref[rows, 0:head_dim], (((1,), (1,)), ((), ())), preferred_element_type=f32)

    following = scores(0)
    for n, (ref, rows) in enumerate(parts):
        values = ref[rows, head_dim:]
        values = jnp.concatenate([values, jnp.ones_like(values)], axis=1)
        s = following * scale
        if n + 1 < len(parts):
            following = scores(n + 1)
        new = jnp.maximum(m, jnp.max(s, axis=1, keepdims=True))
        w = jnp.exp2(s - new[:, 0:1]).astype(bf16)
        factor = jnp.exp2(m - new)
        acc = acc * factor[:, 0:1] + jnp.dot(w, values, preferred_element_type=f32)
        m = new
    if last:
        o_ref[...] = (acc[:, 0:head_dim] / acc[:, head_dim:]).astype(bf16)
    else:
        m_out[...] = m
        acc_out[...] = acc


def flash(q, kv, state, tok, last, tile=256):
    rows, head_dim = q.shape
    heads = rows // tok
    pieces = len(kv)
    piece = kv[0].shape
    tiles = tok // tile
    held = [pl.BlockSpec((tile, 128), lambda i: (i, 0)), pl.BlockSpec((tile, 2 * head_dim), lambda i: (i, 0))]
    held_shape = (jax.ShapeDtypeStruct((rows, 128), f32), jax.ShapeDtypeStruct((rows, 2 * head_dim), f32))
    first = state is None
    return pl.pallas_call(
        functools.partial(flash_kernel, pieces=pieces, scale=head_dim**-0.5 * LOG2E, first=first, last=last),
        grid=(rows // tile,),
        in_specs=[pl.BlockSpec((tile, head_dim), lambda i: (i, 0))]
        + [pl.BlockSpec(piece, lambda i: (0, 0))] * pieces
        + ([] if first else held),
        out_specs=pl.BlockSpec((tile, head_dim), lambda i: (i % tiles, i // tiles)) if last else tuple(held),
        out_shape=jax.ShapeDtypeStruct((tok, heads * head_dim), bf16) if last else held_shape,
        compiler_params=pltpu.CompilerParams(dimension_semantics=("arbitrary",), vmem_limit_bytes=12 << 20),
        cost_estimate=pl.CostEstimate(
            flops=4 * rows * piece[0] * pieces * head_dim,
            bytes_accessed=4 * piece[0] * pieces * head_dim,
            transcendentals=rows * piece[0] * pieces,
        ),
    )(q, *kv, *([] if first else state))


def layer_kernel(place, *refs, parts, tile, sub, units, unit_tile):
    att = refs[0:parts]
    sent = refs[parts : 2 * parts]
    swapped = refs[2 * parts : 3 * parts]
    gain_ref, w_hbm, own_ref = refs[3 * parts : 3 * parts + 3]
    out_1, out_2, rest_ref = refs[3 * parts + 3 : -5]
    x_ref, pair_ref, down_ref, h_ref, sems = refs[-5:]
    step = pl.program_id(0)
    half = sent[0].shape[0] - sub
    count = units // unit_tile
    blocks, rows, _ = down_ref.shape

    def copies():
        found = []
        for n in range(count):
            source = w_hbm.at[:, pl.ds(2 * n * unit_tile, 2 * unit_tile)]
            found.append(pltpu.make_async_copy(source, pair_ref.at[n], sems.at[n]))
        for n in range(blocks):
            source = w_hbm.at[pl.ds(n * rows, rows), pl.ds(2 * units, units)]
            found.append(pltpu.make_async_copy(source, down_ref.at[n], sems.at[count + n]))
        return found

    @pl.when(step == 0)
    def _():
        for c in copies():
            c.start()

    cols = pl.ds(pl.multiple_of(step * tile, tile), tile)
    total = None
    for a, w, o in zip(att, sent, swapped):
        rolled = []
        for r in range(parts):
            some = pl.ds(pl.multiple_of(((place[0] + r) % parts) * sub, sub), sub)
            halves = [a[some, pl.ds(pl.multiple_of(c * half, half), half)] for c in (place[1], 1 - place[1])]
            rolled.append(jnp.concatenate(halves, axis=1))
        weight = jnp.concatenate([w[0:half, :], o[0:half, :]], axis=0)
        part = jnp.dot(jnp.concatenate(rolled, axis=0), weight, preferred_element_type=f32).astype(bf16).astype(f32)
        total = part if total is None else total + part
    for r in range(parts):
        updated = (sent[r][half:, :].astype(f32) + total[r * sub : (r + 1) * sub, :]).astype(bf16)
        x_ref[r * sub : (r + 1) * sub, cols] = updated

    @pl.when(step == pl.num_programs(0) - 1)
    def _():
        own_ref[...] = x_ref[0:sub, :]
        for r in range(2 * parts):
            some = slice(r * sub // 2, (r + 1) * sub // 2)
            x = x_ref[some, :].astype(f32)
            x = x * lax.rsqrt(jnp.mean(x * x, axis=-1, keepdims=True) + norm_eps)
            x_ref[some, :] = (x * gain_ref[...]).astype(bf16)
        for c in copies():
            c.wait()

        def product(n):
            return jnp.dot(x_ref[...], pair_ref[n], preferred_element_type=f32)

        following = product(0)
        for n in range(count):
            r = following
            if n + 1 < count:
                following = product(n + 1)
            gate = r[:, 0:unit_tile]
            hidden = gate / (1.0 + jnp.exp(-gate)) * r[:, unit_tile:]
            h_ref[:, n * unit_tile : (n + 1) * unit_tile] = hidden.astype(bf16)
        rest_ref[0:sub, :] = h_ref[0:sub, :]
        rest_ref[sub:, :] = h_ref[3 * sub :, :]
        down_products(h_ref[sub : 3 * sub, :], down_ref, (out_1, out_2))


def down_products(hidden, down_ref, outs):
    blocks, rows, _ = down_ref.shape
    sub = outs[0].shape[0]
    for n in range(blocks):
        y = lax.dot_general(hidden, down_ref[n], (((1,), (1,)), ((), ())), preferred_element_type=f32).astype(bf16)
        for p, out in enumerate(outs):
            out[:, n * rows : (n + 1) * rows] = y[p * sub : (p + 1) * sub, :]


def rest_kernel(h_ref, w_hbm, out_0, out_3, down_ref, sems):
    blocks, rows, units = down_ref.shape
    copies = []
    for n in range(blocks):
        source = w_hbm.at[pl.ds(n * rows, rows), pl.ds(2 * units, units)]
        copies.append(pltpu.make_async_copy(source, down_ref.at[n], sems.at[n]))
    for c in copies:
        c.start()
    for c in copies:
        c.wait()
    down_products(h_ref[...], down_ref, (out_0, out_3))


def rest(hidden, weights, rows=512):
    tok, units = hidden.shape
    width = weights.shape[0]
    return pl.pallas_call(
        rest_kernel,
        in_specs=[pl.BlockSpec(memory_space=pltpu.VMEM), pl.BlockSpec(memory_space=pltpu.HBM)],
        out_shape=[jax.ShapeDtypeStruct((tok // 2, width), bf16)] * 2,
        scratch_shapes=[pltpu.VMEM((width // rows, rows, units), bf16), pltpu.SemaphoreType.DMA((width // rows,))],
        compiler_params=pltpu.CompilerParams(vmem_limit_bytes=50 << 20),
        name="rest",
    )(hidden, weights)


def layer(place, att, sent, swapped, gain, weights, units, tile=512, unit_tile=128, rows=512):
    parts = len(att)
    tok, part_width = att[0].shape
    both, width = sent[0].shape
    sub = tok // parts
    count = units // unit_tile
    blocks = width // rows
    return pl.pallas_call(
        functools.partial(layer_kernel, parts=parts, tile=tile, sub=sub, units=units, unit_tile=unit_tile),
        grid_spec=pltpu.PrefetchScalarGridSpec(
            num_scalar_prefetch=1,
            grid=(width // tile,),
            in_specs=[pl.BlockSpec((tok, part_width), lambda i, p: (0, 0))] * parts
            + [pl.BlockSpec((both, tile), lambda i, p: (0, i))] * parts
            + [pl.BlockSpec((s.shape[0], tile), lambda i, p: (0, i)) for s in swapped]
            + [pl.BlockSpec((1, width), lambda i, p: (0, 0)), pl.BlockSpec(memory_space=pltpu.HBM)],
            out_specs=[pl.BlockSpec((sub, width), lambda i, p: (0, 0))] * 3
            + [pl.BlockSpec((2 * sub, units), lambda i, p: (0, 0))],
            scratch_shapes=[
                pltpu.VMEM((tok, width), bf16),
                pltpu.VMEM((count, width, 2 * unit_tile), bf16),
                pltpu.VMEM((blocks, rows, units), bf16),
                pltpu.VMEM((tok, units), bf16),
                pltpu.SemaphoreType.DMA((count + blocks,)),
            ],
        ),
        out_shape=[jax.ShapeDtypeStruct((sub, width), bf16)] * 3 + [jax.ShapeDtypeStruct((2 * sub, units), bf16)],
        compiler_params=pltpu.CompilerParams(dimension_semantics=("arbitrary",), vmem_limit_bytes=50 << 20),
        name="layer",
    )(place, *att, *sent, *swapped, gain[None, :], weights)


def line_kernel(*refs):
    pieces, (whole, *halves) = refs[:-3], refs[-3:]
    rows = pieces[0].shape[0]
    each = len(pieces) // 2
    for n, piece in enumerate(pieces):
        whole[n * rows : (n + 1) * rows, :] = piece[...]
        halves[n // each][n % each * rows : (n % each + 1) * rows, :] = piece[...]


def lined_up(*pieces):
    rows, width = pieces[0].shape
    count = rows * len(pieces)
    return pl.pallas_call(
        line_kernel,
        out_shape=[jax.ShapeDtypeStruct((n, width), bf16) for n in (count, count // 2, count // 2)],
        compiler_params=pltpu.CompilerParams(vmem_limit_bytes=10 << 20),
        name="lines",
    )(*pieces)


def shifted(value, by):
    count = lax.axis_size("tp")
    return lax.ppermute(value, "tp", [(i, (i + by) % count) for i in range(count)])


SIDE = 4


def sp_index(z, y, core):
    return (z % SIDE * SIDE + y % SIDE) * 2 + core


def crossed(value, by, turned):
    pairs = []
    for z in range(SIDE):
        for y in range(SIDE):
            for core in range(2):
                along_y = (core == 0) != turned
                goal = sp_index(z, y + by, core) if along_y else sp_index(z + by, y, core)
                pairs.append((sp_index(z, y, core), goal))
    return lax.ppermute(value, "sp", pairs)


def other_core(value):
    count = 2 * SIDE * SIDE
    return lax.ppermute(value, "sp", [(n, n ^ 1) for n in range(count)])


def on_device(
    query_rows,
    key_rows,
    value_rows,
    query_gain,
    key_gain,
    residual,
    out_weight,
    mix_gain,
    gate_weight,
    up_weight,
    down_weight,
):
    tok = query_rows.shape[0]
    parts = lax.axis_size("tp")
    units = gate_weight.shape[1]
    core = lax.axis_index("sp") % 2
    place = jnp.stack([lax.axis_index("tp"), core])
    woven = interleaved(gate_weight, up_weight, down_weight)
    weights = lax.all_gather(woven, "sp", axis=0, tiled=True)
    key_rows, woven = lax.optimization_barrier((key_rows, woven))
    q, kv, payload, kept = prepare(query_rows, key_rows, value_rows, query_gain, key_gain, out_weight, residual)

    steps = (2, 1, -1)
    line = [kv]
    for d in steps:
        line.append(crossed(kv, d, False))
    line, *halves = lined_up(*line)
    near = []
    for d in (1, -1):
        near.append(crossed(line, d, True))
    far = []
    for n in range(2):
        far.append(crossed(halves[n], 2, True))

    sent = [payload]
    for r in range(1, parts):
        sent.append(shifted(payload, -r))

    state = flash(q, [line, other_core(line)], None, tok, False)
    state, near = lax.optimization_barrier((state, near))
    near_swapped = [other_core(v) for v in near]
    state = flash(q, near, state, tok, False)
    state = flash(q, near_swapped, state, tok, False)
    state, far[0] = lax.optimization_barrier((state, far[0]))
    far_swapped = [other_core(far[0])]
    state = flash(q, [far[0], far_swapped[0]], state, tok, False)
    state, far[1], sent = lax.optimization_barrier((state, far[1], sent))
    far_swapped.append(other_core(far[1]))
    swapped = [kept]
    for r in range(1, parts):
        swapped.append(other_core(sent[r]))
    attended = flash(q, [far[1], far_swapped[1]], state, tok, True)

    att_parts = [attended] + [shifted(attended, -r) for r in range(1, parts)]
    own_rows, part_1, part_2, hidden = layer(place, att_parts, sent, swapped, mix_gain, weights, units)
    part_0, part_3 = rest(hidden, weights)
    unit_sum = part_0.astype(f32)
    for r, part in ((1, part_1), (2, part_2), (3, part_3)):
        unit_sum = unit_sum + shifted(part, r).astype(f32)
    return (own_rows.astype(f32) + 0.5 * unit_sum).astype(bf16)


def solution(mesh):
    placed = (
        P("sp", "tp"),
        P("sp", "tp"),
        P("sp", "tp"),
        P(),
        P(),
        P(("sp", "tp"), None),
        P("tp", None),
        P(),
        P("sp", "tp"),
        P("sp", "tp"),
        P("tp", "sp"),
    )
    return jax.shard_map(on_device, mesh=mesh, in_specs=placed, out_specs=P(("sp", "tp"), None), check_vma=False)
```

```python
import functools

import jax
import jax.numpy as jnp
from jax import lax
from jax.experimental import pallas as pl
from jax.experimental.pallas import tpu as pltpu
from jax.sharding import PartitionSpec as P

GRID = 64
norm_eps = 1e-06
theta_base = 10000.0
LOG2E = 1.4426950408889634
f32 = jnp.float32
bf16 = jnp.bfloat16


def angle_tables(first_row, rows, head_dim):
    quarter = head_dim // 4
    frequency = jnp.power(theta_base, -2.0 * jnp.arange(quarter, dtype=f32) / (head_dim // 2))
    places = jnp.concatenate([first_row + jnp.arange(rows, dtype=jnp.int32), jnp.arange(GRID, dtype=jnp.int32)])
    angles = places.astype(f32)[:, None] * frequency
    cosine, sine = lax.optimization_barrier((jnp.cos(angles), jnp.sin(angles)))
    is_row = (jnp.arange(rows + GRID) < rows)[:, None]
    zero = jnp.zeros_like(cosine)

    def placed(lead, trail):
        return jnp.concatenate(
            [
                jnp.where(is_row, lead, zero),
                jnp.where(is_row, trail, zero),
                jnp.where(is_row, zero, lead),
                jnp.where(is_row, zero, trail),
            ],
            axis=1,
        )

    return placed(cosine, cosine), placed(-sine, sine)


def prepare_kernel(
    core, q_hbm, k_hbm, v_hbm, w_hbm, r_hbm, qg_ref, kg_ref, cos_ref, sin_ref,
    q_out, kv_out, sent, kept,
    q_ref, k_ref, v_ref, w_ref, r_ref, sems, *, rows, head_dim, heads,
):
    tok = rows * GRID
    half = kept.shape[0]
    first_half = pl.ds(pl.multiple_of(core[0] * half, half), half)
    other_half = pl.ds(pl.multiple_of((1 - core[0]) * half, half), half)
    moves = [
        (k_hbm, k_ref),
        (v_hbm, v_ref),
        (q_hbm, q_ref),
        (w_hbm.at[first_half, :], w_ref.at[pl.ds(0, half), :]),
        (w_hbm.at[other_half, :], w_ref.at[pl.ds(half, half), :]),
        (r_hbm, r_ref),
        (w_ref.at[pl.ds(0, half), :], sent.at[pl.ds(0, half), :]),
        (w_ref.at[pl.ds(half, half), :], kept),
        (r_ref, sent.at[pl.ds(half, r_hbm.shape[0]), :]),
    ]
    copies = [pltpu.make_async_copy(x, y, sems.at[n]) for n, (x, y) in enumerate(moves)]
    for c in copies[:6]:
        c.start()

    def spread(ref):
        both = ref[0:rows, :][:, None, :] + ref[rows : rows + GRID, :][None, :, :]
        return both.reshape(tok, head_dim)

    cosine = spread(cos_ref)
    sine = spread(sin_ref)
    lane = lax.broadcasted_iota(jnp.int32, (tok, head_dim), 1)
    first = (lane % (head_dim // 2)) < head_dim // 4
    quarter = head_dim // 4

    def prepared(raw, gain):
        x = raw.astype(f32)
        x = x * lax.rsqrt(jnp.mean(x * x, axis=-1, keepdims=True) + norm_eps) * gain
        partner = jnp.where(first, pltpu.roll(x, head_dim - quarter, 1), pltpu.roll(x, quarter, 1))
        return (x * cosine + partner * sine).astype(bf16)

    copies[0].wait()
    copies[1].wait()
    kv_out[:, 0:head_dim] = prepared(k_ref[...], kg_ref[...])
    kv_out[:, head_dim:] = v_ref[...]
    for n in (3, 4, 5):
        copies[n].wait()
        copies[n + 3].start()
    copies[2].wait()
    for h in range(heads):
        q_out[h * tok : (h + 1) * tok, :] = prepared(q_ref[:, h * head_dim : (h + 1) * head_dim], qg_ref[...])
    for n in (6, 7, 8):
        copies[n].wait()


def weave_kernel(g_hbm, u_hbm, d_hbm, woven, g_ref, u_ref, d_ref, sems, *, tile):
    moves = ((g_hbm, g_ref), (u_hbm, u_ref), (d_hbm, d_ref))
    copies = [pltpu.make_async_copy(x, y, sems.at[n]) for n, (x, y) in enumerate(moves)]
    for c in copies:
        c.start()
    for c in copies:
        c.wait()
    units = g_ref.shape[1]
    for n in range(units // tile):
        part = slice(n * tile, (n + 1) * tile)
        woven[:, 2 * n * tile : (2 * n + 1) * tile] = g_ref[:, part]
        woven[:, (2 * n + 1) * tile : (2 * n + 2) * tile] = u_ref[:, part]
    woven[:, 2 * units :] = d_ref[...]


def interleaved(gate, up, down, tile=128):
    big = (gate, up, down.T)
    return pl.pallas_call(
        functools.partial(weave_kernel, tile=tile),
        in_specs=[pl.BlockSpec(memory_space=pltpu.HBM)] * 3,
        out_shape=jax.ShapeDtypeStruct((gate.shape[0], 3 * gate.shape[1]), bf16),
        scratch_shapes=[pltpu.VMEM(x.shape, bf16) for x in big] + [pltpu.SemaphoreType.DMA((3,))],
        compiler_params=pltpu.CompilerParams(vmem_limit_bytes=60 * 1024 * 1024),
        name="weave",
    )(*big)


def prepare(query_rows, key_rows, value_rows, query_gain, key_gain, out_weight, residual):
    tok, width = query_rows.shape
    head_dim = query_gain.shape[0]
    rows = tok // GRID
    cosine, sine = angle_tables(lax.axis_index("sp") * rows, rows, head_dim)
    hbm = pl.BlockSpec(memory_space=pltpu.HBM)
    vmem = pl.BlockSpec(memory_space=pltpu.VMEM)
    big = (query_rows, key_rows, value_rows, out_weight, residual)
    half = out_weight.shape[0] // 2
    return pl.pallas_call(
        functools.partial(prepare_kernel, rows=rows, head_dim=head_dim, heads=width // head_dim),
        in_specs=[pl.BlockSpec(memory_space=pltpu.SMEM)] + [hbm] * 5 + [vmem] * 4,
        out_specs=[vmem] * 2 + [hbm] * 2,
        out_shape=(
            jax.ShapeDtypeStruct((tok * (width // head_dim), head_dim), bf16),
            jax.ShapeDtypeStruct((tok, 2 * head_dim), bf16),
            jax.ShapeDtypeStruct((half + residual.shape[0], residual.shape[1]), bf16),
            jax.ShapeDtypeStruct((half, residual.shape[1]), bf16),
        ),
        scratch_shapes=[pltpu.VMEM(x.shape, bf16) for x in big] + [pltpu.SemaphoreType.DMA((9,))],
        compiler_params=pltpu.CompilerParams(vmem_limit_bytes=60 * 1024 * 1024),
        name="prepare",
    )(
        (lax.axis_index("sp") % 2)[None], *big, query_gain[None, :], key_gain[None, :], cosine, sine
    )


def flash_kernel(*refs, pieces, scale, first, last, block=1024):
    q_ref = refs[0]
    kv_refs = refs[1 : 1 + pieces]
    refs = refs[1 + pieces :]
    if not first:
        m_in, acc_in = refs[0:2]
        refs = refs[2:]
    if last:
        o_ref = refs[0]
        refs = refs[1:]
    else:
        m_out, acc_out = refs[0:2]
        refs = refs[2:]
    head_dim = q_ref.shape[1]
    q = q_ref[...]
    if first:
        m = jnp.full((q.shape[0], 128), -jnp.inf, f32)
        acc = jnp.zeros((q.shape[0], 2 * head_dim), f32)
    else:
        m = m_in[...]
        acc = acc_in[...]

    parts = [(ref, slice(r, r + block)) for ref in kv_refs for r in range(0, ref.shape[0], block)]

    def scores(n):
        ref, rows = parts[n]
        return lax.dot_general(q, ref[rows, 0:head_dim], (((1,), (1,)), ((), ())), preferred_element_type=f32)

    following = scores(0)
    for n, (ref, rows) in enumerate(parts):
        values = ref[rows, head_dim:]
        values = jnp.concatenate([values, jnp.ones_like(values)], axis=1)
        s = following * scale
        if n + 1 < len(parts):
            following = scores(n + 1)
        new = jnp.maximum(m, jnp.max(s, axis=1, keepdims=True))
        w = jnp.exp2(s - new[:, 0:1]).astype(bf16)
        factor = jnp.exp2(m - new)
        acc = acc * factor[:, 0:1] + jnp.dot(w, values, preferred_element_type=f32)
        m = new
    if last:
        o_ref[...] = (acc[:, 0:head_dim] / acc[:, head_dim:]).astype(bf16)
    else:
        m_out[...] = m
        acc_out[...] = acc


def flash(q, kv, state, tok, last, tile=256):
    rows, head_dim = q.shape
    heads = rows // tok
    pieces = len(kv)
    piece = kv[0].shape
    tiles = tok // tile
    held = [pl.BlockSpec((tile, 128), lambda i: (i, 0)), pl.BlockSpec((tile, 2 * head_dim), lambda i: (i, 0))]
    held_shape = (jax.ShapeDtypeStruct((rows, 128), f32), jax.ShapeDtypeStruct((rows, 2 * head_dim), f32))
    first = state is None
    return pl.pallas_call(
        functools.partial(flash_kernel, pieces=pieces, scale=head_dim**-0.5 * LOG2E, first=first, last=last),
        grid=(rows // tile,),
        in_specs=[pl.BlockSpec((tile, head_dim), lambda i: (i, 0))]
        + [pl.BlockSpec(piece, lambda i: (0, 0))] * pieces
        + ([] if first else held),
        out_specs=pl.BlockSpec((tile, head_dim), lambda i: (i % tiles, i // tiles)) if last else tuple(held),
        out_shape=jax.ShapeDtypeStruct((tok, heads * head_dim), bf16) if last else held_shape,
        compiler_params=pltpu.CompilerParams(dimension_semantics=("arbitrary",), vmem_limit_bytes=12 << 20),
        cost_estimate=pl.CostEstimate(
            flops=4 * rows * piece[0] * pieces * head_dim,
            bytes_accessed=4 * piece[0] * pieces * head_dim,
            transcendentals=rows * piece[0] * pieces,
        ),
    )(q, *kv, *([] if first else state))


def project_kernel(place, *refs, parts, tile, sub):
    att = refs[0:parts]
    sent = refs[parts : 2 * parts]
    swapped = refs[2 * parts : 3 * parts]
    gain_ref, own_ref, norm_ref, x_ref = refs[3 * parts :]
    step = pl.program_id(0)
    half = sent[0].shape[0] - sub
    cols = pl.ds(pl.multiple_of(step * tile, tile), tile)
    total = None
    for a, w, o in zip(att, sent, swapped):
        rolled = []
        for r in range(parts):
            some = pl.ds(pl.multiple_of(((place[0] + r) % parts) * sub, sub), sub)
            halves = [a[some, pl.ds(pl.multiple_of(c * half, half), half)] for c in (place[1], 1 - place[1])]
            rolled.append(jnp.concatenate(halves, axis=1))
        weight = jnp.concatenate([w[0:half, :], o[0:half, :]], axis=0)
        part = jnp.dot(jnp.concatenate(rolled, axis=0), weight, preferred_element_type=f32).astype(bf16).astype(f32)
        total = part if total is None else total + part
    for r in range(parts):
        updated = (sent[r][half:, :].astype(f32) + total[r * sub : (r + 1) * sub, :]).astype(bf16)
        x_ref[r * sub : (r + 1) * sub, cols] = updated

    @pl.when(step == pl.num_programs(0) - 1)
    def _():
        own_ref[...] = x_ref[0:sub, :]
        for r in range(2 * parts):
            some = slice(r * sub // 2, (r + 1) * sub // 2)
            x = x_ref[some, :].astype(f32)
            x = x * lax.rsqrt(jnp.mean(x * x, axis=-1, keepdims=True) + norm_eps)
            norm_ref[some, :] = (x * gain_ref[...]).astype(bf16)


def project(place, att, sent, swapped, gain, tile=512):
    parts = len(att)
    tok, part_width = att[0].shape
    both, width = sent[0].shape
    sub = tok // parts
    return pl.pallas_call(
        functools.partial(project_kernel, parts=parts, tile=tile, sub=sub),
        grid_spec=pltpu.PrefetchScalarGridSpec(
            num_scalar_prefetch=1,
            grid=(width // tile,),
            in_specs=[pl.BlockSpec((tok, part_width), lambda i, p: (0, 0))] * parts
            + [pl.BlockSpec((both, tile), lambda i, p: (0, i))] * parts
            + [pl.BlockSpec((s.shape[0], tile), lambda i, p: (0, i)) for s in swapped]
            + [pl.BlockSpec((1, width), lambda i, p: (0, 0))],
            out_specs=[pl.BlockSpec((sub, width), lambda i, p: (0, 0)), pl.BlockSpec((tok, width), lambda i, p: (0, 0))],
            scratch_shapes=[pltpu.VMEM((tok, width), bf16)],
        ),
        out_shape=[jax.ShapeDtypeStruct((sub, width), bf16), jax.ShapeDtypeStruct((tok, width), bf16)],
        compiler_params=pltpu.CompilerParams(dimension_semantics=("arbitrary",), vmem_limit_bytes=54 << 20),
        name="project",
    )(place, *att, *sent, *swapped, gain[None, :])


def unit_kernel(x_ref, w_hbm, out_1, out_2, rest_ref, pair_ref, down_ref, h_ref, sems, *, units, unit_tile, groups, split):
    sub = out_1.shape[0]
    width = x_ref.shape[1]
    count = units // unit_tile
    blocks, rows, _ = down_ref.shape

    def copies(n):
        found = []
        for m in range(split):
            if n < count:
                part = pl.ds(m * width // split, width // split)
                source = w_hbm.at[part, pl.ds(2 * n * unit_tile, 2 * unit_tile)]
                target = pair_ref.at[n, part, :]
            else:
                b = n - count
                source = w_hbm.at[pl.ds(b * rows + m * rows // split, rows // split), pl.ds(2 * units, units)]
                target = down_ref.at[b, pl.ds(m * rows // split, rows // split), :]
            found.append(pltpu.make_async_copy(source, target, sems.at[n * split + m]))
        return found

    bounds = [sum(groups[:g]) for g in range(len(groups) + 1)] + [count + blocks]
    waves = [[c for n in range(bounds[g], bounds[g + 1]) for c in copies(n)] for g in range(len(groups) + 1)]

    def arrive(g):
        for c in waves[g]:
            c.wait()
        if g + 1 < len(waves):
            for c in waves[g + 1]:
                c.start()

    def product(n):
        return jnp.dot(x_ref[...], pair_ref[n], preferred_element_type=f32)

    for c in waves[0]:
        c.start()
    for g in range(len(groups)):
        arrive(g)
        following = product(bounds[g])
        for n in range(bounds[g], bounds[g + 1]):
            r = following
            if n + 1 < bounds[g + 1]:
                following = product(n + 1)
            gate = r[:, 0:unit_tile]
            hidden = gate / (1.0 + jnp.exp(-gate)) * r[:, unit_tile:]
            h_ref[:, n * unit_tile : (n + 1) * unit_tile] = hidden.astype(bf16)
    arrive(len(groups))
    rest_ref[0:sub, :] = h_ref[0:sub, :]
    rest_ref[sub:, :] = h_ref[3 * sub :, :]
    down_products(h_ref[sub : 3 * sub, :], down_ref, (out_1, out_2))


def feed_forward(x, weights, units, sub, unit_tile=128, rows=512, groups=(3, 4, 4), split=2):
    tok, width = x.shape
    count = units // unit_tile
    blocks = width // rows
    return pl.pallas_call(
        functools.partial(unit_kernel, units=units, unit_tile=unit_tile, groups=groups, split=split),
        in_specs=[pl.BlockSpec(memory_space=pltpu.VMEM), pl.BlockSpec(memory_space=pltpu.HBM)],
        out_shape=[jax.ShapeDtypeStruct((sub, width), bf16)] * 2 + [jax.ShapeDtypeStruct((2 * sub, units), bf16)],
        scratch_shapes=[
            pltpu.VMEM((count, width, 2 * unit_tile), bf16),
            pltpu.VMEM((blocks, rows, units), bf16),
            pltpu.VMEM((tok, units), bf16),
            pltpu.SemaphoreType.DMA(((count + blocks) * split,)),
        ],
        compiler_params=pltpu.CompilerParams(vmem_limit_bytes=50 << 20),
        name="units",
    )(x, weights)


def down_products(hidden, down_ref, outs):
    blocks, rows, _ = down_ref.shape
    sub = outs[0].shape[0]
    for n in range(blocks):
        y = lax.dot_general(hidden, down_ref[n], (((1,), (1,)), ((), ())), preferred_element_type=f32).astype(bf16)
        for p, out in enumerate(outs):
            out[:, n * rows : (n + 1) * rows] = y[p * sub : (p + 1) * sub, :]


def rest_kernel(h_ref, w_hbm, out_0, out_3, down_ref, sems):
    blocks, rows, units = down_ref.shape
    copies = []
    for n in range(blocks):
        source = w_hbm.at[pl.ds(n * rows, rows), pl.ds(2 * units, units)]
        copies.append(pltpu.make_async_copy(source, down_ref.at[n], sems.at[n]))
    for c in copies:
        c.start()
    for c in copies:
        c.wait()
    down_products(h_ref[...], down_ref, (out_0, out_3))


def rest(hidden, weights, rows=512):
    tok, units = hidden.shape
    width = weights.shape[0]
    return pl.pallas_call(
        rest_kernel,
        in_specs=[pl.BlockSpec(memory_space=pltpu.VMEM), pl.BlockSpec(memory_space=pltpu.HBM)],
        out_shape=[jax.ShapeDtypeStruct((tok // 2, width), bf16)] * 2,
        scratch_shapes=[pltpu.VMEM((width // rows, rows, units), bf16), pltpu.SemaphoreType.DMA((width // rows,))],
        compiler_params=pltpu.CompilerParams(vmem_limit_bytes=50 << 20),
        name="rest",
    )(hidden, weights)


def line_kernel(*refs):
    rows = refs[0].shape[0]
    for n, piece in enumerate(refs[:-1]):
        refs[-1][n * rows : (n + 1) * rows, :] = piece[...]


def lined_up(*pieces):
    rows, width = pieces[0].shape
    return pl.pallas_call(
        line_kernel,
        out_shape=jax.ShapeDtypeStruct((rows * len(pieces), width), bf16),
        compiler_params=pltpu.CompilerParams(vmem_limit_bytes=8 << 20),
        name="lines",
    )(*pieces)


def shifted(value, by):
    count = lax.axis_size("tp")
    return lax.ppermute(value, "tp", [(i, (i + by) % count) for i in range(count)])


SIDE = 4


def sp_index(z, y, core):
    return (z % SIDE * SIDE + y % SIDE) * 2 + core


def crossed(value, by, turned):
    pairs = []
    for z in range(SIDE):
        for y in range(SIDE):
            for core in range(2):
                along_y = (core == 0) != turned
                goal = sp_index(z, y + by, core) if along_y else sp_index(z + by, y, core)
                pairs.append((sp_index(z, y, core), goal))
    return lax.ppermute(value, "sp", pairs)


def other_core(value):
    count = 2 * SIDE * SIDE
    return lax.ppermute(value, "sp", [(n, n ^ 1) for n in range(count)])


def on_device(
    query_rows,
    key_rows,
    value_rows,
    query_gain,
    key_gain,
    residual,
    out_weight,
    mix_gain,
    gate_weight,
    up_weight,
    down_weight,
):
    tok = query_rows.shape[0]
    parts = lax.axis_size("tp")
    units = gate_weight.shape[1]
    core = lax.axis_index("sp") % 2
    place = jnp.stack([lax.axis_index("tp"), core])
    weights = lax.all_gather(interleaved(gate_weight, up_weight, down_weight), "sp", axis=0, tiled=True)
    q, kv, payload, kept = prepare(query_rows, key_rows, value_rows, query_gain, key_gain, out_weight, residual)

    steps = (2, 1, -1)
    line = [kv]
    for d in steps:
        line.append(crossed(kv, d, False))
    line = lined_up(*line)
    near = []
    for d in (1, -1):
        near.append(crossed(line, d, True))
    far = crossed(line, 2, True)

    sent = [payload]
    for r in range(1, parts):
        sent.append(shifted(payload, -r))

    state = flash(q, [line, other_core(line)], None, tok, False)
    state, near = lax.optimization_barrier((state, near))
    near_swapped = [other_core(v) for v in near]
    state = flash(q, near, state, tok, False)
    state = flash(q, near_swapped, state, tok, False)
    state, far, sent = lax.optimization_barrier((state, far, sent))
    far_swapped = other_core(far)
    swapped = [kept]
    for r in range(1, parts):
        swapped.append(other_core(sent[r]))
    state = flash(q, [far], state, tok, False)
    attended = flash(q, [far_swapped], state, tok, True)

    att_parts = [attended] + [shifted(attended, -r) for r in range(1, parts)]
    own_rows, normed = project(place, att_parts, sent, swapped, mix_gain)
    part_1, part_2, hidden = feed_forward(normed, weights, units, own_rows.shape[0])
    part_0, part_3 = rest(hidden, weights)
    unit_sum = part_0.astype(f32)
    for r, part in ((1, part_1), (2, part_2), (3, part_3)):
        unit_sum = unit_sum + shifted(part, r).astype(f32)
    return (own_rows.astype(f32) + 0.5 * unit_sum).astype(bf16)


def solution(mesh):
    placed = (
        P("sp", "tp"),
        P("sp", "tp"),
        P("sp", "tp"),
        P(),
        P(),
        P(("sp", "tp"), None),
        P("tp", None),
        P(),
        P("sp", "tp"),
        P("sp", "tp"),
        P("tp", "sp"),
    )
    return jax.shard_map(on_device, mesh=mesh, in_specs=placed, out_specs=P(("sp", "tp"), None), check_vma=False)
```

```python
import functools

import jax
import jax.numpy as jnp
from jax import lax
from jax.experimental import pallas as pl
from jax.experimental.pallas import tpu as pltpu
from jax.sharding import PartitionSpec as P

GRID = 64
norm_eps = 1e-06
theta_base = 10000.0
LOG2E = 1.4426950408889634
f32 = jnp.float32
bf16 = jnp.bfloat16


def angle_tables(first_row, rows, head_dim):
    quarter = head_dim // 4
    frequency = jnp.power(theta_base, -2.0 * jnp.arange(quarter, dtype=f32) / (head_dim // 2))
    places = jnp.concatenate([first_row + jnp.arange(rows, dtype=jnp.int32), jnp.arange(GRID, dtype=jnp.int32)])
    angles = places.astype(f32)[:, None] * frequency
    cosine, sine = lax.optimization_barrier((jnp.cos(angles), jnp.sin(angles)))
    is_row = (jnp.arange(rows + GRID) < rows)[:, None]
    zero = jnp.zeros_like(cosine)

    def placed(lead, trail):
        return jnp.concatenate(
            [
                jnp.where(is_row, lead, zero),
                jnp.where(is_row, trail, zero),
                jnp.where(is_row, zero, lead),
                jnp.where(is_row, zero, trail),
            ],
            axis=1,
        )

    return placed(cosine, cosine), placed(-sine, sine)


def prepare_kernel(
    core, q_hbm, k_hbm, v_hbm, w_hbm, r_hbm, qg_ref, kg_ref, cos_ref, sin_ref,
    q_out, kv_out, sent, kept,
    q_ref, k_ref, v_ref, w_ref, r_ref, sems, *, rows, head_dim, heads,
):
    tok = rows * GRID
    half = kept.shape[0]
    first_half = pl.ds(pl.multiple_of(core[0] * half, half), half)
    other_half = pl.ds(pl.multiple_of((1 - core[0]) * half, half), half)
    moves = [
        (k_hbm, k_ref),
        (v_hbm, v_ref),
        (q_hbm, q_ref),
        (w_hbm.at[first_half, :], w_ref.at[pl.ds(0, half), :]),
        (w_hbm.at[other_half, :], w_ref.at[pl.ds(half, half), :]),
        (r_hbm, r_ref),
        (w_ref.at[pl.ds(0, half), :], sent.at[pl.ds(0, half), :]),
        (w_ref.at[pl.ds(half, half), :], kept),
        (r_ref, sent.at[pl.ds(half, r_hbm.shape[0]), :]),
    ]
    copies = [pltpu.make_async_copy(x, y, sems.at[n]) for n, (x, y) in enumerate(moves)]
    for c in copies[:6]:
        c.start()

    def spread(ref):
        both = ref[0:rows, :][:, None, :] + ref[rows : rows + GRID, :][None, :, :]
        return both.reshape(tok, head_dim)

    cosine = spread(cos_ref)
    sine = spread(sin_ref)
    lane = lax.broadcasted_iota(jnp.int32, (tok, head_dim), 1)
    first = (lane % (head_dim // 2)) < head_dim // 4
    quarter = head_dim // 4

    def prepared(raw, gain):
        x = raw.astype(f32)
        x = x * lax.rsqrt(jnp.mean(x * x, axis=-1, keepdims=True) + norm_eps) * gain
        partner = jnp.where(first, pltpu.roll(x, head_dim - quarter, 1), pltpu.roll(x, quarter, 1))
        return (x * cosine + partner * sine).astype(bf16)

    copies[0].wait()
    copies[1].wait()
    kv_out[:, 0:head_dim] = prepared(k_ref[...], kg_ref[...])
    kv_out[:, head_dim:] = v_ref[...]
    for n in (3, 4, 5):
        copies[n].wait()
        copies[n + 3].start()
    copies[2].wait()
    for h in range(heads):
        q_out[h * tok : (h + 1) * tok, :] = prepared(q_ref[:, h * head_dim : (h + 1) * head_dim], qg_ref[...])
    for n in (6, 7, 8):
        copies[n].wait()


def weave_kernel(g_hbm, u_hbm, d_hbm, woven, g_ref, u_ref, d_ref, sems, *, tile):
    moves = ((g_hbm, g_ref), (u_hbm, u_ref), (d_hbm, d_ref))
    copies = [pltpu.make_async_copy(x, y, sems.at[n]) for n, (x, y) in enumerate(moves)]
    for c in copies:
        c.start()
    for c in copies:
        c.wait()
    units = g_ref.shape[1]
    for n in range(units // tile):
        part = slice(n * tile, (n + 1) * tile)
        woven[:, 2 * n * tile : (2 * n + 1) * tile] = g_ref[:, part]
        woven[:, (2 * n + 1) * tile : (2 * n + 2) * tile] = u_ref[:, part]
    woven[:, 2 * units :] = d_ref[...]


def interleaved(gate, up, down, tile=128):
    big = (gate, up, down.T)
    return pl.pallas_call(
        functools.partial(weave_kernel, tile=tile),
        in_specs=[pl.BlockSpec(memory_space=pltpu.HBM)] * 3,
        out_shape=jax.ShapeDtypeStruct((gate.shape[0], 3 * gate.shape[1]), bf16),
        scratch_shapes=[pltpu.VMEM(x.shape, bf16) for x in big] + [pltpu.SemaphoreType.DMA((3,))],
        compiler_params=pltpu.CompilerParams(vmem_limit_bytes=60 * 1024 * 1024),
        name="weave",
    )(*big)


def prepare(query_rows, key_rows, value_rows, query_gain, key_gain, out_weight, residual):
    tok, width = query_rows.shape
    head_dim = query_gain.shape[0]
    rows = tok // GRID
    cosine, sine = angle_tables(lax.axis_index("sp") * rows, rows, head_dim)
    hbm = pl.BlockSpec(memory_space=pltpu.HBM)
    vmem = pl.BlockSpec(memory_space=pltpu.VMEM)
    big = (query_rows, key_rows, value_rows, out_weight, residual)
    half = out_weight.shape[0] // 2
    return pl.pallas_call(
        functools.partial(prepare_kernel, rows=rows, head_dim=head_dim, heads=width // head_dim),
        in_specs=[pl.BlockSpec(memory_space=pltpu.SMEM)] + [hbm] * 5 + [vmem] * 4,
        out_specs=[vmem] * 2 + [hbm] * 2,
        out_shape=(
            jax.ShapeDtypeStruct((tok * (width // head_dim), head_dim), bf16),
            jax.ShapeDtypeStruct((tok, 2 * head_dim), bf16),
            jax.ShapeDtypeStruct((half + residual.shape[0], residual.shape[1]), bf16),
            jax.ShapeDtypeStruct((half, residual.shape[1]), bf16),
        ),
        scratch_shapes=[pltpu.VMEM(x.shape, bf16) for x in big] + [pltpu.SemaphoreType.DMA((9,))],
        compiler_params=pltpu.CompilerParams(vmem_limit_bytes=60 * 1024 * 1024),
        name="prepare",
    )(
        (lax.axis_index("sp") % 2)[None], *big, query_gain[None, :], key_gain[None, :], cosine, sine
    )


def flash_kernel(*refs, pieces, scale, first, last, block=1024):
    q_ref = refs[0]
    kv_refs = refs[1 : 1 + pieces]
    refs = refs[1 + pieces :]
    if not first:
        m_in, acc_in = refs[0:2]
        refs = refs[2:]
    if last:
        o_ref = refs[0]
        refs = refs[1:]
    else:
        m_out, acc_out = refs[0:2]
        refs = refs[2:]
    head_dim = q_ref.shape[1]
    q = q_ref[...]
    if first:
        m = jnp.full((q.shape[0], 128), -jnp.inf, f32)
        acc = jnp.zeros((q.shape[0], 2 * head_dim), f32)
    else:
        m = m_in[...]
        acc = acc_in[...]

    parts = [(ref, slice(r, r + block)) for ref in kv_refs for r in range(0, ref.shape[0], block)]

    def scores(n):
        ref, rows = parts[n]
        return lax.dot_general(q, ref[rows, 0:head_dim], (((1,), (1,)), ((), ())), preferred_element_type=f32)

    following = scores(0)
    for n, (ref, rows) in enumerate(parts):
        values = ref[rows, head_dim:]
        values = jnp.concatenate([values, jnp.ones_like(values)], axis=1)
        s = following * scale
        if n + 1 < len(parts):
            following = scores(n + 1)
        new = jnp.maximum(m, jnp.max(s, axis=1, keepdims=True))
        w = jnp.exp2(s - new[:, 0:1]).astype(bf16)
        factor = jnp.exp2(m - new)
        acc = acc * factor[:, 0:1] + jnp.dot(w, values, preferred_element_type=f32)
        m = new
    if last:
        o_ref[...] = (acc[:, 0:head_dim] / acc[:, head_dim:]).astype(bf16)
    else:
        m_out[...] = m
        acc_out[...] = acc


def flash(q, kv, state, tok, last, tile=256):
    rows, head_dim = q.shape
    heads = rows // tok
    pieces = len(kv)
    piece = kv[0].shape
    tiles = tok // tile
    held = [pl.BlockSpec((tile, 128), lambda i: (i, 0)), pl.BlockSpec((tile, 2 * head_dim), lambda i: (i, 0))]
    held_shape = (jax.ShapeDtypeStruct((rows, 128), f32), jax.ShapeDtypeStruct((rows, 2 * head_dim), f32))
    first = state is None
    return pl.pallas_call(
        functools.partial(flash_kernel, pieces=pieces, scale=head_dim**-0.5 * LOG2E, first=first, last=last),
        grid=(rows // tile,),
        in_specs=[pl.BlockSpec((tile, head_dim), lambda i: (i, 0))]
        + [pl.BlockSpec(piece, lambda i: (0, 0))] * pieces
        + ([] if first else held),
        out_specs=pl.BlockSpec((tile, head_dim), lambda i: (i % tiles, i // tiles)) if last else tuple(held),
        out_shape=jax.ShapeDtypeStruct((tok, heads * head_dim), bf16) if last else held_shape,
        compiler_params=pltpu.CompilerParams(dimension_semantics=("arbitrary",), vmem_limit_bytes=12 << 20),
        cost_estimate=pl.CostEstimate(
            flops=4 * rows * piece[0] * pieces * head_dim,
            bytes_accessed=4 * piece[0] * pieces * head_dim,
            transcendentals=rows * piece[0] * pieces,
        ),
    )(q, *kv, *([] if first else state))


def layer_kernel(place, *refs, parts, tile, sub, units, unit_tile):
    att = refs[0:parts]
    sent = refs[parts : 2 * parts]
    swapped = refs[2 * parts : 3 * parts]
    gain_ref, w_hbm, own_ref = refs[3 * parts : 3 * parts + 3]
    out_1, out_2, rest_ref = refs[3 * parts + 3 : -6]
    x_ref, att_ref, pair_ref, down_ref, h_ref, sems = refs[-6:]
    step = pl.program_id(0)
    half = sent[0].shape[0] - sub
    count = units // unit_tile
    blocks, rows, _ = down_ref.shape

    def copies():
        found = []
        for n in range(count):
            source = w_hbm.at[:, pl.ds(2 * n * unit_tile, 2 * unit_tile)]
            found.append(pltpu.make_async_copy(source, pair_ref.at[n], sems.at[n]))
        for n in range(blocks):
            source = w_hbm.at[pl.ds(n * rows, rows), pl.ds(2 * units, units)]
            found.append(pltpu.make_async_copy(source, down_ref.at[n], sems.at[count + n]))
        return found

    @pl.when(step == 0)
    def _():
        for c in copies():
            c.start()

    @pl.when(step == 0)
    def _():
        for m, a in enumerate(att):
            for r in range(parts):
                some = pl.ds(pl.multiple_of(((place[0] + r) % parts) * sub, sub), sub)
                for k, c in enumerate((place[1], 1 - place[1])):
                    head = a[some, pl.ds(pl.multiple_of(c * half, half), half)]
                    att_ref[r * sub : (r + 1) * sub, (2 * m + k) * half : (2 * m + k + 1) * half] = head

    cols = pl.ds(pl.multiple_of(step * tile, tile), tile)
    weight = jnp.concatenate([v for w, o in zip(sent, swapped) for v in (w[0:half, :], o[0:half, :])], axis=0)
    total = jnp.dot(att_ref[...], weight, preferred_element_type=f32)
    for r in range(parts):
        updated = (sent[r][half:, :].astype(f32) + total[r * sub : (r + 1) * sub, :]).astype(bf16)
        x_ref[r * sub : (r + 1) * sub, cols] = updated

    @pl.when(step == pl.num_programs(0) - 1)
    def _():
        own_ref[...] = x_ref[0:sub, :]
        for r in range(2 * parts):
            some = slice(r * sub // 2, (r + 1) * sub // 2)
            x = x_ref[some, :].astype(f32)
            x = x * lax.rsqrt(jnp.mean(x * x, axis=-1, keepdims=True) + norm_eps)
            x_ref[some, :] = (x * gain_ref[...]).astype(bf16)
        for c in copies():
            c.wait()

        def product(n):
            return jnp.dot(x_ref[...], pair_ref[n], preferred_element_type=f32)

        following = product(0)
        for n in range(count):
            r = following
            if n + 1 < count:
                following = product(n + 1)
            gate = r[:, 0:unit_tile]
            hidden = gate / (1.0 + jnp.exp(-gate)) * r[:, unit_tile:]
            h_ref[:, n * unit_tile : (n + 1) * unit_tile] = hidden.astype(bf16)
        rest_ref[0:sub, :] = h_ref[0:sub, :]
        rest_ref[sub:, :] = h_ref[3 * sub :, :]
        down_products(h_ref[sub : 3 * sub, :], down_ref, (out_1, out_2))


def down_products(hidden, down_ref, outs):
    blocks, rows, _ = down_ref.shape
    sub = outs[0].shape[0]
    for n in range(blocks):
        y = lax.dot_general(hidden, down_ref[n], (((1,), (1,)), ((), ())), preferred_element_type=f32).astype(bf16)
        for p, out in enumerate(outs):
            out[:, n * rows : (n + 1) * rows] = y[p * sub : (p + 1) * sub, :]


def rest_kernel(h_ref, w_hbm, out_0, out_3, down_ref, sems):
    blocks, rows, units = down_ref.shape
    copies = []
    for n in range(blocks):
        source = w_hbm.at[pl.ds(n * rows, rows), pl.ds(2 * units, units)]
        copies.append(pltpu.make_async_copy(source, down_ref.at[n], sems.at[n]))
    for c in copies:
        c.start()
    for c in copies:
        c.wait()
    down_products(h_ref[...], down_ref, (out_0, out_3))


def rest(hidden, weights, rows=512):
    tok, units = hidden.shape
    width = weights.shape[0]
    return pl.pallas_call(
        rest_kernel,
        in_specs=[pl.BlockSpec(memory_space=pltpu.VMEM), pl.BlockSpec(memory_space=pltpu.HBM)],
        out_shape=[jax.ShapeDtypeStruct((tok // 2, width), bf16)] * 2,
        scratch_shapes=[pltpu.VMEM((width // rows, rows, units), bf16), pltpu.SemaphoreType.DMA((width // rows,))],
        compiler_params=pltpu.CompilerParams(vmem_limit_bytes=50 << 20),
        name="rest",
    )(hidden, weights)


def layer(place, att, sent, swapped, gain, weights, units, tile=512, unit_tile=128, rows=512):
    parts = len(att)
    tok, part_width = att[0].shape
    both, width = sent[0].shape
    sub = tok // parts
    count = units // unit_tile
    blocks = width // rows
    return pl.pallas_call(
        functools.partial(layer_kernel, parts=parts, tile=tile, sub=sub, units=units, unit_tile=unit_tile),
        grid_spec=pltpu.PrefetchScalarGridSpec(
            num_scalar_prefetch=1,
            grid=(width // tile,),
            in_specs=[pl.BlockSpec((tok, part_width), lambda i, p: (0, 0))] * parts
            + [pl.BlockSpec((both, tile), lambda i, p: (0, i))] * parts
            + [pl.BlockSpec((s.shape[0], tile), lambda i, p: (0, i)) for s in swapped]
            + [pl.BlockSpec((1, width), lambda i, p: (0, 0)), pl.BlockSpec(memory_space=pltpu.HBM)],
            out_specs=[pl.BlockSpec((sub, width), lambda i, p: (0, 0))] * 3
            + [pl.BlockSpec((2 * sub, units), lambda i, p: (0, 0))],
            scratch_shapes=[
                pltpu.VMEM((tok, width), bf16),
                pltpu.VMEM((tok, parts * part_width), bf16),
                pltpu.VMEM((count, width, 2 * unit_tile), bf16),
                pltpu.VMEM((blocks, rows, units), bf16),
                pltpu.VMEM((tok, units), bf16),
                pltpu.SemaphoreType.DMA((count + blocks,)),
            ],
        ),
        out_shape=[jax.ShapeDtypeStruct((sub, width), bf16)] * 3 + [jax.ShapeDtypeStruct((2 * sub, units), bf16)],
        compiler_params=pltpu.CompilerParams(dimension_semantics=("arbitrary",), vmem_limit_bytes=50 << 20),
        name="layer",
    )(place, *att, *sent, *swapped, gain[None, :], weights)


def line_kernel(*refs):
    rows = refs[0].shape[0]
    for n, piece in enumerate(refs[:-1]):
        refs[-1][n * rows : (n + 1) * rows, :] = piece[...]


def lined_up(*pieces):
    rows, width = pieces[0].shape
    return pl.pallas_call(
        line_kernel,
        out_shape=jax.ShapeDtypeStruct((rows * len(pieces), width), bf16),
        compiler_params=pltpu.CompilerParams(vmem_limit_bytes=8 << 20),
        name="lines",
    )(*pieces)


def shifted(value, by):
    count = lax.axis_size("tp")
    return lax.ppermute(value, "tp", [(i, (i + by) % count) for i in range(count)])


SIDE = 4


def sp_index(z, y, core):
    return (z % SIDE * SIDE + y % SIDE) * 2 + core


def crossed(value, by, turned):
    pairs = []
    for z in range(SIDE):
        for y in range(SIDE):
            for core in range(2):
                along_y = (core == 0) != turned
                goal = sp_index(z, y + by, core) if along_y else sp_index(z + by, y, core)
                pairs.append((sp_index(z, y, core), goal))
    return lax.ppermute(value, "sp", pairs)


def other_core(value):
    count = 2 * SIDE * SIDE
    return lax.ppermute(value, "sp", [(n, n ^ 1) for n in range(count)])


def on_device(
    query_rows,
    key_rows,
    value_rows,
    query_gain,
    key_gain,
    residual,
    out_weight,
    mix_gain,
    gate_weight,
    up_weight,
    down_weight,
):
    tok = query_rows.shape[0]
    parts = lax.axis_size("tp")
    units = gate_weight.shape[1]
    core = lax.axis_index("sp") % 2
    place = jnp.stack([lax.axis_index("tp"), core])
    weights = lax.all_gather(interleaved(gate_weight, up_weight, down_weight), "sp", axis=0, tiled=True)
    q, kv, payload, kept = prepare(query_rows, key_rows, value_rows, query_gain, key_gain, out_weight, residual)

    steps = (2, 1, -1)
    line = [kv]
    for d in steps:
        line.append(crossed(kv, d, False))
    line = lined_up(*line)
    near = []
    for d in (1, -1):
        near.append(crossed(line, d, True))
    far = crossed(line, 2, True)

    sent = [payload]
    for r in range(1, parts):
        sent.append(shifted(payload, -r))

    state = flash(q, [line, other_core(line)], None, tok, False)
    state, near = lax.optimization_barrier((state, near))
    near_swapped = [other_core(v) for v in near]
    state = flash(q, near, state, tok, False)
    state = flash(q, near_swapped, state, tok, False)
    state, far, sent = lax.optimization_barrier((state, far, sent))
    far_swapped = other_core(far)
    swapped = [kept]
    for r in range(1, parts):
        swapped.append(other_core(sent[r]))
    state = flash(q, [far], state, tok, False)
    attended = flash(q, [far_swapped], state, tok, True)

    att_parts = [attended] + [shifted(attended, -r) for r in range(1, parts)]
    own_rows, part_1, part_2, hidden = layer(place, att_parts, sent, swapped, mix_gain, weights, units)
    part_0, part_3 = rest(hidden, weights)
    unit_sum = part_0.astype(f32)
    for r, part in ((1, part_1), (2, part_2), (3, part_3)):
        unit_sum = unit_sum + shifted(part, r).astype(f32)
    return (own_rows.astype(f32) + 0.5 * unit_sum).astype(bf16)


def solution(mesh):
    placed = (
        P("sp", "tp"),
        P("sp", "tp"),
        P("sp", "tp"),
        P(),
        P(),
        P(("sp", "tp"), None),
        P("tp", None),
        P(),
        P("sp", "tp"),
        P("sp", "tp"),
        P("tp", "sp"),
    )
    return jax.shard_map(on_device, mesh=mesh, in_specs=placed, out_specs=P(("sp", "tp"), None), check_vma=False)
```

```python
import functools

import jax
import jax.numpy as jnp
from jax import lax
from jax.experimental import pallas as pl
from jax.experimental.pallas import tpu as pltpu
from jax.sharding import PartitionSpec as P

GRID = 64
norm_eps = 1e-06
theta_base = 10000.0
LOG2E = 1.4426950408889634
f32 = jnp.float32
bf16 = jnp.bfloat16


def angle_tables(first_row, rows, head_dim):
    quarter = head_dim // 4
    frequency = jnp.power(theta_base, -2.0 * jnp.arange(quarter, dtype=f32) / (head_dim // 2))
    places = jnp.concatenate([first_row + jnp.arange(rows, dtype=jnp.int32), jnp.arange(GRID, dtype=jnp.int32)])
    angles = places.astype(f32)[:, None] * frequency
    cosine, sine = lax.optimization_barrier((jnp.cos(angles), jnp.sin(angles)))
    is_row = (jnp.arange(rows + GRID) < rows)[:, None]
    zero = jnp.zeros_like(cosine)

    def placed(lead, trail):
        return jnp.concatenate(
            [
                jnp.where(is_row, lead, zero),
                jnp.where(is_row, trail, zero),
                jnp.where(is_row, zero, lead),
                jnp.where(is_row, zero, trail),
            ],
            axis=1,
        )

    return placed(cosine, cosine), placed(-sine, sine)


def prepare_kernel(
    core, q_hbm, k_hbm, v_hbm, w_hbm, r_hbm, qg_ref, kg_ref, cos_ref, sin_ref,
    q_out, kv_out, sent, kept,
    q_ref, k_ref, v_ref, w_ref, r_ref, sems, *, rows, head_dim, heads,
):
    tok = rows * GRID
    half = kept.shape[0]
    first_half = pl.ds(pl.multiple_of(core[0] * half, half), half)
    other_half = pl.ds(pl.multiple_of((1 - core[0]) * half, half), half)
    moves = [
        (k_hbm, k_ref),
        (v_hbm, v_ref),
        (q_hbm, q_ref),
        (w_hbm.at[first_half, :], w_ref.at[pl.ds(0, half), :]),
        (w_hbm.at[other_half, :], w_ref.at[pl.ds(half, half), :]),
        (r_hbm, r_ref),
        (w_ref.at[pl.ds(0, half), :], sent.at[pl.ds(0, half), :]),
        (w_ref.at[pl.ds(half, half), :], kept),
        (r_ref, sent.at[pl.ds(half, r_hbm.shape[0]), :]),
    ]
    copies = [pltpu.make_async_copy(x, y, sems.at[n]) for n, (x, y) in enumerate(moves)]
    for c in copies[:6]:
        c.start()

    def spread(ref):
        both = ref[0:rows, :][:, None, :] + ref[rows : rows + GRID, :][None, :, :]
        return both.reshape(tok, head_dim)

    cosine = spread(cos_ref)
    sine = spread(sin_ref)
    lane = lax.broadcasted_iota(jnp.int32, (tok, head_dim), 1)
    first = (lane % (head_dim // 2)) < head_dim // 4
    quarter = head_dim // 4

    def prepared(raw, gain):
        x = raw.astype(f32)
        x = x * lax.rsqrt(jnp.mean(x * x, axis=-1, keepdims=True) + norm_eps) * gain
        partner = jnp.where(first, pltpu.roll(x, head_dim - quarter, 1), pltpu.roll(x, quarter, 1))
        return (x * cosine + partner * sine).astype(bf16)

    copies[0].wait()
    copies[1].wait()
    kv_out[:, 0:head_dim] = prepared(k_ref[...], kg_ref[...])
    kv_out[:, head_dim:] = v_ref[...]
    for n in (3, 4, 5):
        copies[n].wait()
        copies[n + 3].start()
    copies[2].wait()
    for h in range(heads):
        q_out[h * tok : (h + 1) * tok, :] = prepared(q_ref[:, h * head_dim : (h + 1) * head_dim], qg_ref[...])
    for n in (6, 7, 8):
        copies[n].wait()


def weave_kernel(g_hbm, u_hbm, d_hbm, woven, g_ref, u_ref, d_ref, sems, *, tile):
    moves = ((g_hbm, g_ref), (u_hbm, u_ref), (d_hbm, d_ref))
    copies = [pltpu.make_async_copy(x, y, sems.at[n]) for n, (x, y) in enumerate(moves)]
    for c in copies:
        c.start()
    for c in copies:
        c.wait()
    units = g_ref.shape[1]
    for n in range(units // tile):
        part = slice(n * tile, (n + 1) * tile)
        woven[:, 2 * n * tile : (2 * n + 1) * tile] = g_ref[:, part]
        woven[:, (2 * n + 1) * tile : (2 * n + 2) * tile] = u_ref[:, part]
    woven[:, 2 * units :] = d_ref[...]


def interleaved(gate, up, down, tile=128):
    big = (gate, up, down.T)
    return pl.pallas_call(
        functools.partial(weave_kernel, tile=tile),
        in_specs=[pl.BlockSpec(memory_space=pltpu.HBM)] * 3,
        out_shape=jax.ShapeDtypeStruct((gate.shape[0], 3 * gate.shape[1]), bf16),
        scratch_shapes=[pltpu.VMEM(x.shape, bf16) for x in big] + [pltpu.SemaphoreType.DMA((3,))],
        compiler_params=pltpu.CompilerParams(vmem_limit_bytes=60 * 1024 * 1024),
        name="weave",
    )(*big)


def prepare(query_rows, key_rows, value_rows, query_gain, key_gain, out_weight, residual):
    tok, width = query_rows.shape
    head_dim = query_gain.shape[0]
    rows = tok // GRID
    cosine, sine = angle_tables(lax.axis_index("sp") * rows, rows, head_dim)
    hbm = pl.BlockSpec(memory_space=pltpu.HBM)
    vmem = pl.BlockSpec(memory_space=pltpu.VMEM)
    big = (query_rows, key_rows, value_rows, out_weight, residual)
    half = out_weight.shape[0] // 2
    return pl.pallas_call(
        functools.partial(prepare_kernel, rows=rows, head_dim=head_dim, heads=width // head_dim),
        in_specs=[pl.BlockSpec(memory_space=pltpu.SMEM)] + [hbm] * 5 + [vmem] * 4,
        out_specs=[vmem] * 2 + [hbm] * 2,
        out_shape=(
            jax.ShapeDtypeStruct((tok * (width // head_dim), head_dim), bf16),
            jax.ShapeDtypeStruct((tok, 2 * head_dim), bf16),
            jax.ShapeDtypeStruct((half + residual.shape[0], residual.shape[1]), bf16),
            jax.ShapeDtypeStruct((half, residual.shape[1]), bf16),
        ),
        scratch_shapes=[pltpu.VMEM(x.shape, bf16) for x in big] + [pltpu.SemaphoreType.DMA((9,))],
        compiler_params=pltpu.CompilerParams(vmem_limit_bytes=60 * 1024 * 1024),
        name="prepare",
    )(
        (lax.axis_index("sp") % 2)[None], *big, query_gain[None, :], key_gain[None, :], cosine, sine
    )


def flash_kernel(*refs, pieces, scale, first, last, block=1024):
    q_ref = refs[0]
    kv_refs = refs[1 : 1 + pieces]
    refs = refs[1 + pieces :]
    if not first:
        m_in, acc_in = refs[0:2]
        refs = refs[2:]
    if last:
        o_ref = refs[0]
        refs = refs[1:]
    else:
        m_out, acc_out = refs[0:2]
        refs = refs[2:]
    head_dim = q_ref.shape[1]
    q = q_ref[...]
    if first:
        m = jnp.full((q.shape[0], 128), -jnp.inf, f32)
        acc = jnp.zeros((q.shape[0], 2 * head_dim), f32)
    else:
        m = m_in[...]
        acc = acc_in[...]

    parts = [(ref, slice(r, r + block)) for ref in kv_refs for r in range(0, ref.shape[0], block)]

    def scores(n):
        ref, rows = parts[n]
        return lax.dot_general(q, ref[rows, 0:head_dim], (((1,), (1,)), ((), ())), preferred_element_type=f32)

    following = scores(0)
    for n, (ref, rows) in enumerate(parts):
        values = ref[rows, head_dim:]
        values = jnp.concatenate([values, jnp.ones_like(values)], axis=1)
        s = following * scale
        if n + 1 < len(parts):
            following = scores(n + 1)
        new = jnp.maximum(m, jnp.max(s, axis=1, keepdims=True))
        w = jnp.exp2(s - new[:, 0:1]).astype(bf16)
        factor = jnp.exp2(m - new)
        acc = acc * factor[:, 0:1] + jnp.dot(w, values, preferred_element_type=f32)
        m = new
    if last:
        o_ref[...] = (acc[:, 0:head_dim] / acc[:, head_dim:]).astype(bf16)
    else:
        m_out[...] = m
        acc_out[...] = acc


def flash(q, kv, state, tok, last, tile=256):
    rows, head_dim = q.shape
    heads = rows // tok
    pieces = len(kv)
    piece = kv[0].shape
    tiles = tok // tile
    held = [pl.BlockSpec((tile, 128), lambda i: (i, 0)), pl.BlockSpec((tile, 2 * head_dim), lambda i: (i, 0))]
    held_shape = (jax.ShapeDtypeStruct((rows, 128), f32), jax.ShapeDtypeStruct((rows, 2 * head_dim), f32))
    first = state is None
    return pl.pallas_call(
        functools.partial(flash_kernel, pieces=pieces, scale=head_dim**-0.5 * LOG2E, first=first, last=last),
        grid=(rows // tile,),
        in_specs=[pl.BlockSpec((tile, head_dim), lambda i: (i, 0))]
        + [pl.BlockSpec(piece, lambda i: (0, 0))] * pieces
        + ([] if first else held),
        out_specs=pl.BlockSpec((tile, head_dim), lambda i: (i % tiles, i // tiles)) if last else tuple(held),
        out_shape=jax.ShapeDtypeStruct((tok, heads * head_dim), bf16) if last else held_shape,
        compiler_params=pltpu.CompilerParams(dimension_semantics=("arbitrary",), vmem_limit_bytes=12 << 20),
        cost_estimate=pl.CostEstimate(
            flops=4 * rows * piece[0] * pieces * head_dim,
            bytes_accessed=4 * piece[0] * pieces * head_dim,
            transcendentals=rows * piece[0] * pieces,
        ),
    )(q, *kv, *([] if first else state))


def layer_kernel(place, *refs, parts, tile, sub, units, unit_tile):
    att = refs[0:parts]
    sent = refs[parts : 2 * parts]
    swapped = refs[2 * parts : 3 * parts]
    gain_ref, w_hbm, own_ref = refs[3 * parts : 3 * parts + 3]
    out_1, out_2, rest_ref = refs[3 * parts + 3 : -6]
    x_ref, att_ref, pair_ref, down_ref, h_ref, sems = refs[-6:]
    step = pl.program_id(0)
    half = sent[0].shape[0] - sub
    count = units // unit_tile
    blocks, rows, _ = down_ref.shape

    def copies():
        found = []
        for n in range(count):
            source = w_hbm.at[:, pl.ds(2 * n * unit_tile, 2 * unit_tile)]
            found.append(pltpu.make_async_copy(source, pair_ref.at[n], sems.at[n]))
        for n in range(blocks):
            source = w_hbm.at[pl.ds(n * rows, rows), pl.ds(2 * units, units)]
            found.append(pltpu.make_async_copy(source, down_ref.at[n], sems.at[count + n]))
        return found

    @pl.when(step == 0)
    def _():
        for c in copies():
            c.start()

    @pl.when(step == 0)
    def _():
        for m, a in enumerate(att):
            for r in range(parts):
                some = pl.ds(pl.multiple_of(((place[0] + r) % parts) * sub, sub), sub)
                for k, c in enumerate((place[1], 1 - place[1])):
                    head = a[some, pl.ds(pl.multiple_of(c * half, half), half)]
                    att_ref[r * sub : (r + 1) * sub, (2 * m + k) * half : (2 * m + k + 1) * half] = head

    cols = pl.ds(pl.multiple_of(step * tile, tile), tile)
    weight = jnp.concatenate([v for w, o in zip(sent, swapped) for v in (w[0:half, :], o[0:half, :])], axis=0)
    total = jnp.dot(att_ref[...], weight, preferred_element_type=f32)
    for r in range(parts):
        updated = (sent[r][half:, :].astype(f32) + total[r * sub : (r + 1) * sub, :]).astype(bf16)
        x_ref[r * sub : (r + 1) * sub, cols] = updated

    @pl.when(step == pl.num_programs(0) - 1)
    def _():
        own_ref[...] = x_ref[0:sub, :]
        for r in range(2 * parts):
            some = slice(r * sub // 2, (r + 1) * sub // 2)
            x = x_ref[some, :].astype(f32)
            x = x * lax.rsqrt(jnp.mean(x * x, axis=-1, keepdims=True) + norm_eps)
            x_ref[some, :] = (x * gain_ref[...]).astype(bf16)
        for c in copies():
            c.wait()

        def product(n):
            return jnp.dot(x_ref[...], pair_ref[n], preferred_element_type=f32)

        following = product(0)
        for n in range(count):
            r = following
            if n + 1 < count:
                following = product(n + 1)
            gate = r[:, 0:unit_tile]
            hidden = gate / (1.0 + jnp.exp(-gate)) * r[:, unit_tile:]
            h_ref[:, n * unit_tile : (n + 1) * unit_tile] = hidden.astype(bf16)
        rest_ref[0:sub, :] = h_ref[0:sub, :]
        rest_ref[sub:, :] = h_ref[3 * sub :, :]
        down_products(h_ref[sub : 3 * sub, :], down_ref, (out_1, out_2))


def down_products(hidden, down_ref, outs):
    blocks, rows, _ = down_ref.shape
    sub = outs[0].shape[0]
    for n in range(blocks):
        y = lax.dot_general(hidden, down_ref[n], (((1,), (1,)), ((), ())), preferred_element_type=f32).astype(bf16)
        for p, out in enumerate(outs):
            out[:, n * rows : (n + 1) * rows] = y[p * sub : (p + 1) * sub, :]


def rest_kernel(h_ref, w_hbm, out_0, out_3, down_ref, sems):
    blocks, rows, units = down_ref.shape
    copies = []
    for n in range(blocks):
        source = w_hbm.at[pl.ds(n * rows, rows), pl.ds(2 * units, units)]
        copies.append(pltpu.make_async_copy(source, down_ref.at[n], sems.at[n]))
    for c in copies:
        c.start()
    for c in copies:
        c.wait()
    down_products(h_ref[...], down_ref, (out_0, out_3))


def rest(hidden, weights, rows=512):
    tok, units = hidden.shape
    width = weights.shape[0]
    return pl.pallas_call(
        rest_kernel,
        in_specs=[pl.BlockSpec(memory_space=pltpu.VMEM), pl.BlockSpec(memory_space=pltpu.HBM)],
        out_shape=[jax.ShapeDtypeStruct((tok // 2, width), bf16)] * 2,
        scratch_shapes=[pltpu.VMEM((width // rows, rows, units), bf16), pltpu.SemaphoreType.DMA((width // rows,))],
        compiler_params=pltpu.CompilerParams(vmem_limit_bytes=50 << 20),
        name="rest",
    )(hidden, weights)


def layer(place, att, sent, swapped, gain, weights, units, tile=512, unit_tile=128, rows=512):
    parts = len(att)
    tok, part_width = att[0].shape
    both, width = sent[0].shape
    sub = tok // parts
    count = units // unit_tile
    blocks = width // rows
    return pl.pallas_call(
        functools.partial(layer_kernel, parts=parts, tile=tile, sub=sub, units=units, unit_tile=unit_tile),
        grid_spec=pltpu.PrefetchScalarGridSpec(
            num_scalar_prefetch=1,
            grid=(width // tile,),
            in_specs=[pl.BlockSpec((tok, part_width), lambda i, p: (0, 0))] * parts
            + [pl.BlockSpec((both, tile), lambda i, p: (0, i))] * parts
            + [pl.BlockSpec((s.shape[0], tile), lambda i, p: (0, i)) for s in swapped]
            + [pl.BlockSpec((1, width), lambda i, p: (0, 0)), pl.BlockSpec(memory_space=pltpu.HBM)],
            out_specs=[pl.BlockSpec((sub, width), lambda i, p: (0, 0))] * 3
            + [pl.BlockSpec((2 * sub, units), lambda i, p: (0, 0))],
            scratch_shapes=[
                pltpu.VMEM((tok, width), bf16),
                pltpu.VMEM((tok, parts * part_width), bf16),
                pltpu.VMEM((count, width, 2 * unit_tile), bf16),
                pltpu.VMEM((blocks, rows, units), bf16),
                pltpu.VMEM((tok, units), bf16),
                pltpu.SemaphoreType.DMA((count + blocks,)),
            ],
        ),
        out_shape=[jax.ShapeDtypeStruct((sub, width), bf16)] * 3 + [jax.ShapeDtypeStruct((2 * sub, units), bf16)],
        compiler_params=pltpu.CompilerParams(dimension_semantics=("arbitrary",), vmem_limit_bytes=50 << 20),
        name="layer",
    )(place, *att, *sent, *swapped, gain[None, :], weights)


def line_kernel(*refs):
    rows = refs[0].shape[0]
    for n, piece in enumerate(refs[:-1]):
        refs[-1][n * rows : (n + 1) * rows, :] = piece[...]


def lined_up(*pieces):
    rows, width = pieces[0].shape
    return pl.pallas_call(
        line_kernel,
        out_shape=jax.ShapeDtypeStruct((rows * len(pieces), width), bf16),
        compiler_params=pltpu.CompilerParams(vmem_limit_bytes=8 << 20),
        name="lines",
    )(*pieces)


def shifted(value, by):
    count = lax.axis_size("tp")
    return lax.ppermute(value, "tp", [(i, (i + by) % count) for i in range(count)])


SIDE = 4


def sp_index(z, y, core):
    return (z % SIDE * SIDE + y % SIDE) * 2 + core


def crossed(value, by, turned):
    pairs = []
    for z in range(SIDE):
        for y in range(SIDE):
            for core in range(2):
                along_y = (core == 0) != turned
                goal = sp_index(z, y + by, core) if along_y else sp_index(z + by, y, core)
                pairs.append((sp_index(z, y, core), goal))
    return lax.ppermute(value, "sp", pairs)


def other_core(value):
    count = 2 * SIDE * SIDE
    return lax.ppermute(value, "sp", [(n, n ^ 1) for n in range(count)])


def on_device(
    query_rows,
    key_rows,
    value_rows,
    query_gain,
    key_gain,
    residual,
    out_weight,
    mix_gain,
    gate_weight,
    up_weight,
    down_weight,
):
    tok = query_rows.shape[0]
    parts = lax.axis_size("tp")
    units = gate_weight.shape[1]
    core = lax.axis_index("sp") % 2
    place = jnp.stack([lax.axis_index("tp"), core])
    weights = lax.all_gather(interleaved(gate_weight, up_weight, down_weight), "sp", axis=0, tiled=True)
    q, kv, payload, kept = prepare(query_rows, key_rows, value_rows, query_gain, key_gain, out_weight, residual)

    steps = (2, 1, -1)
    line = [kv]
    for d in steps:
        line.append(crossed(kv, d, False))
    line = lined_up(*line)
    near = []
    for d in (1, -1):
        near.append(crossed(line, d, True))

    sent = [payload]
    for r in range(1, parts):
        sent.append(shifted(payload, -r))

    state = flash(q, [line, other_core(line)], None, tok, False)
    state, near = lax.optimization_barrier((state, near))
    middle = line.shape[0] // 2
    far = []
    for v, d in ((near[0][:middle], 1), (near[1][middle:], -1)):
        far.append(crossed(v, d, True))
    near_swapped = []
    for n in range(2):
        near_swapped.append(other_core(near[n]))
    state = flash(q, near, state, tok, False)
    state = flash(q, near_swapped, state, tok, False)
    state, far = lax.optimization_barrier((state, far))
    far_swapped = [other_core(v) for v in far]
    state = flash(q, far, state, tok, False)
    attended = flash(q, far_swapped, state, tok, True)

    att_parts = [attended]
    for r in range(1, parts):
        att_parts.append(shifted(attended, -r))
    att_parts[0], sent = lax.optimization_barrier((attended, sent))
    swapped = [kept]
    for r in range(1, parts):
        swapped.append(other_core(sent[r]))
    own_rows, part_1, part_2, hidden = layer(place, att_parts, sent, swapped, mix_gain, weights, units)
    part_0, part_3 = rest(hidden, weights)
    unit_sum = part_0.astype(f32)
    for r, part in ((1, part_1), (2, part_2), (3, part_3)):
        unit_sum = unit_sum + shifted(part, r).astype(f32)
    return (own_rows.astype(f32) + 0.5 * unit_sum).astype(bf16)


def solution(mesh):
    placed = (
        P("sp", "tp"),
        P("sp", "tp"),
        P("sp", "tp"),
        P(),
        P(),
        P(("sp", "tp"), None),
        P("tp", None),
        P(),
        P("sp", "tp"),
        P("sp", "tp"),
        P("tp", "sp"),
    )
    return jax.shard_map(on_device, mesh=mesh, in_specs=placed, out_specs=P(("sp", "tp"), None), check_vma=False)
```

```python
import functools

import jax
import jax.numpy as jnp
from jax import lax
from jax.experimental import pallas as pl
from jax.experimental.pallas import tpu as pltpu
from jax.sharding import PartitionSpec as P

GRID = 64
norm_eps = 1e-06
theta_base = 10000.0
LOG2E = 1.4426950408889634
f32 = jnp.float32
bf16 = jnp.bfloat16


def angle_tables(first_row, rows, head_dim):
    quarter = head_dim // 4
    frequency = jnp.power(theta_base, -2.0 * jnp.arange(quarter, dtype=f32) / (head_dim // 2))
    places = jnp.concatenate([first_row + jnp.arange(rows, dtype=jnp.int32), jnp.arange(GRID, dtype=jnp.int32)])
    angles = places.astype(f32)[:, None] * frequency
    cosine, sine = lax.optimization_barrier((jnp.cos(angles), jnp.sin(angles)))
    is_row = (jnp.arange(rows + GRID) < rows)[:, None]
    zero = jnp.zeros_like(cosine)

    def placed(lead, trail):
        return jnp.concatenate(
            [
                jnp.where(is_row, lead, zero),
                jnp.where(is_row, trail, zero),
                jnp.where(is_row, zero, lead),
                jnp.where(is_row, zero, trail),
            ],
            axis=1,
        )

    return placed(cosine, cosine), placed(-sine, sine)


def rotated(ref_x, gain_ref, cos_ref, sin_ref, rows, head_dim, columns):
    tok = rows * GRID

    def spread(ref):
        both = ref[0:rows, :][:, None, :] + ref[rows : rows + GRID, :][None, :, :]
        return both.reshape(tok, head_dim)

    cosine = spread(cos_ref)
    sine = spread(sin_ref)
    lane = lax.broadcasted_iota(jnp.int32, (tok, head_dim), 1)
    first = (lane % (head_dim // 2)) < head_dim // 4
    quarter = head_dim // 4
    found = []
    for part in columns:
        x = ref_x[:, part].astype(f32)
        x = x * lax.rsqrt(jnp.mean(x * x, axis=-1, keepdims=True) + norm_eps) * gain_ref[...]
        partner = jnp.where(first, pltpu.roll(x, head_dim - quarter, 1), pltpu.roll(x, quarter, 1))
        found.append((x * cosine + partner * sine).astype(bf16))
    return found


def keys_kernel(k_hbm, v_hbm, gain_ref, cos_ref, sin_ref, kv_out, k_ref, v_ref, sems, *, rows, head_dim):
    copies = [
        pltpu.make_async_copy(x, y, sems.at[n]) for n, (x, y) in enumerate(((k_hbm, k_ref), (v_hbm, v_ref)))
    ]
    for c in copies:
        c.start()
    for c in copies:
        c.wait()
    kv_out[:, 0:head_dim] = rotated(k_ref, gain_ref, cos_ref, sin_ref, rows, head_dim, [slice(0, head_dim)])[0]
    kv_out[:, head_dim:] = v_ref[...]


def prepare_keys(key_rows, value_rows, gain, cosine, sine):
    tok, head_dim = key_rows.shape
    hbm = pl.BlockSpec(memory_space=pltpu.HBM)
    vmem = pl.BlockSpec(memory_space=pltpu.VMEM)
    return pl.pallas_call(
        functools.partial(keys_kernel, rows=tok // GRID, head_dim=head_dim),
        in_specs=[hbm] * 2 + [vmem] * 3,
        out_shape=jax.ShapeDtypeStruct((tok, 2 * head_dim), bf16),
        scratch_shapes=[pltpu.VMEM((tok, head_dim), bf16)] * 2 + [pltpu.SemaphoreType.DMA((2,))],
        compiler_params=pltpu.CompilerParams(vmem_limit_bytes=60 * 1024 * 1024),
        name="keys",
    )(key_rows, value_rows, gain[None, :], cosine, sine)


def queries_kernel(q_ref, gain_ref, cos_ref, sin_ref, q_out, *, rows, head_dim, heads):
    tok = rows * GRID
    columns = [slice(h * head_dim, (h + 1) * head_dim) for h in range(heads)]
    for h, x in enumerate(rotated(q_ref, gain_ref, cos_ref, sin_ref, rows, head_dim, columns)):
        q_out[h * tok : (h + 1) * tok, :] = x


def prepare_queries(query_rows, gain, cosine, sine):
    tok, width = query_rows.shape
    head_dim = gain.shape[0]
    heads = width // head_dim
    return pl.pallas_call(
        functools.partial(queries_kernel, rows=tok // GRID, head_dim=head_dim, heads=heads),
        out_shape=jax.ShapeDtypeStruct((tok * heads, head_dim), bf16),
        compiler_params=pltpu.CompilerParams(vmem_limit_bytes=8 << 20),
        name="queries",
    )(query_rows, gain[None, :], cosine, sine)


def weave_kernel(
    core, g_hbm, u_hbm, d_hbm, w_hbm, r_hbm, woven, sent, kept, g_ref, u_ref, d_ref, w_ref, r_ref, sems, *, tile
):
    half = kept.shape[0]
    first_half = pl.ds(pl.multiple_of(core[0] * half, half), half)
    other_half = pl.ds(pl.multiple_of((1 - core[0]) * half, half), half)
    moves = [
        (g_hbm, g_ref),
        (u_hbm, u_ref),
        (d_hbm, d_ref),
        (w_hbm.at[first_half, :], w_ref.at[pl.ds(0, half), :]),
        (w_hbm.at[other_half, :], w_ref.at[pl.ds(half, half), :]),
        (r_hbm, r_ref),
        (w_ref.at[pl.ds(0, half), :], sent.at[pl.ds(0, half), :]),
        (w_ref.at[pl.ds(half, half), :], kept),
        (r_ref, sent.at[pl.ds(half, r_hbm.shape[0]), :]),
    ]
    copies = [pltpu.make_async_copy(x, y, sems.at[n]) for n, (x, y) in enumerate(moves)]
    for c in copies[:6]:
        c.start()
    for c in copies[:3]:
        c.wait()
    units = g_ref.shape[1]
    for n in range(units // tile):
        part = slice(n * tile, (n + 1) * tile)
        woven[:, 2 * n * tile : (2 * n + 1) * tile] = g_ref[:, part]
        woven[:, (2 * n + 1) * tile : (2 * n + 2) * tile] = u_ref[:, part]
    woven[:, 2 * units :] = d_ref[...]
    for n in (3, 4, 5):
        copies[n].wait()
        copies[n + 3].start()
    for n in (6, 7, 8):
        copies[n].wait()


def weave(core, gate, up, down, out_weight, residual, tile=128):
    big = (gate, up, down.T, out_weight, residual)
    half = out_weight.shape[0] // 2
    width = residual.shape[1]
    hbm = pl.BlockSpec(memory_space=pltpu.HBM)
    return pl.pallas_call(
        functools.partial(weave_kernel, tile=tile),
        in_specs=[pl.BlockSpec(memory_space=pltpu.SMEM)] + [hbm] * 5,
        out_specs=[pl.BlockSpec(memory_space=pltpu.VMEM), hbm, hbm],
        out_shape=[
            jax.ShapeDtypeStruct((gate.shape[0], 3 * gate.shape[1]), bf16),
            jax.ShapeDtypeStruct((half + residual.shape[0], width), bf16),
            jax.ShapeDtypeStruct((half, width), bf16),
        ],
        scratch_shapes=[pltpu.VMEM(x.shape, bf16) for x in big] + [pltpu.SemaphoreType.DMA((9,))],
        compiler_params=pltpu.CompilerParams(vmem_limit_bytes=60 * 1024 * 1024),
        name="weave",
    )(core[None], *big)


def flash_kernel(*refs, pieces, scale, first, last, block=1024):
    q_ref = refs[0]
    kv_refs = refs[1 : 1 + pieces]
    refs = refs[1 + pieces :]
    if not first:
        m_in, acc_in = refs[0:2]
        refs = refs[2:]
    if last:
        o_ref = refs[0]
        refs = refs[1:]
    else:
        m_out, acc_out = refs[0:2]
        refs = refs[2:]
    head_dim = q_ref.shape[1]
    q = q_ref[...]
    if first:
        m = jnp.full((q.shape[0], 128), -jnp.inf, f32)
        acc = jnp.zeros((q.shape[0], 2 * head_dim), f32)
    else:
        m = m_in[...]
        acc = acc_in[...]

    parts = [(ref, slice(r, r + block)) for ref in kv_refs for r in range(0, ref.shape[0], block)]

    def scores(n):
        ref, rows = parts[n]
        return lax.dot_general(q, ref[rows, 0:head_dim], (((1,), (1,)), ((), ())), preferred_element_type=f32)

    following = scores(0)
    for n, (ref, rows) in enumerate(parts):
        values = ref[rows, head_dim:]
        values = jnp.concatenate([values, jnp.ones_like(values)], axis=1)
        s = following * scale
        if n + 1 < len(parts):
            following = scores(n + 1)
        new = jnp.maximum(m, jnp.max(s, axis=1, keepdims=True))
        w = jnp.exp2(s - new[:, 0:1]).astype(bf16)
        factor = jnp.exp2(m - new)
        acc = acc * factor[:, 0:1] + jnp.dot(w, values, preferred_element_type=f32)
        m = new
    if last:
        o_ref[...] = (acc[:, 0:head_dim] / acc[:, head_dim:]).astype(bf16)
    else:
        m_out[...] = m
        acc_out[...] = acc


def flash(q, kv, state, tok, last, tile=256):
    rows, head_dim = q.shape
    heads = rows // tok
    pieces = len(kv)
    piece = kv[0].shape
    tiles = tok // tile
    held = [pl.BlockSpec((tile, 128), lambda i: (i, 0)), pl.BlockSpec((tile, 2 * head_dim), lambda i: (i, 0))]
    held_shape = (jax.ShapeDtypeStruct((rows, 128), f32), jax.ShapeDtypeStruct((rows, 2 * head_dim), f32))
    first = state is None
    return pl.pallas_call(
        functools.partial(flash_kernel, pieces=pieces, scale=head_dim**-0.5 * LOG2E, first=first, last=last),
        grid=(rows // tile,),
        in_specs=[pl.BlockSpec((tile, head_dim), lambda i: (i, 0))]
        + [pl.BlockSpec(piece, lambda i: (0, 0))] * pieces
        + ([] if first else held),
        out_specs=pl.BlockSpec((tile, head_dim), lambda i: (i % tiles, i // tiles)) if last else tuple(held),
        out_shape=jax.ShapeDtypeStruct((tok, heads * head_dim), bf16) if last else held_shape,
        compiler_params=pltpu.CompilerParams(dimension_semantics=("arbitrary",), vmem_limit_bytes=12 << 20),
        cost_estimate=pl.CostEstimate(
            flops=4 * rows * piece[0] * pieces * head_dim,
            bytes_accessed=4 * piece[0] * pieces * head_dim,
            transcendentals=rows * piece[0] * pieces,
        ),
    )(q, *kv, *([] if first else state))


def layer_kernel(place, *refs, parts, tile, sub, units, unit_tile):
    att = refs[0:parts]
    sent = refs[parts : 2 * parts]
    swapped = refs[2 * parts : 3 * parts]
    gain_ref, w_hbm, own_ref = refs[3 * parts : 3 * parts + 3]
    out_1, out_2, rest_ref = refs[3 * parts + 3 : -6]
    x_ref, att_ref, pair_ref, down_ref, h_ref, sems = refs[-6:]
    step = pl.program_id(0)
    half = sent[0].shape[0] - sub
    count = units // unit_tile
    blocks, rows, _ = down_ref.shape

    def copies():
        found = []
        for n in range(count):
            source = w_hbm.at[:, pl.ds(2 * n * unit_tile, 2 * unit_tile)]
            found.append(pltpu.make_async_copy(source, pair_ref.at[n], sems.at[n]))
        for n in range(blocks):
            source = w_hbm.at[pl.ds(n * rows, rows), pl.ds(2 * units, units)]
            found.append(pltpu.make_async_copy(source, down_ref.at[n], sems.at[count + n]))
        return found

    early = count * 2 // 3

    @pl.when(step == 0)
    def _():
        for c in copies()[:early]:
            c.start()

    @pl.when(step == 1)
    def _():
        for c in copies()[early:]:
            c.start()

    @pl.when(step == 0)
    def _():
        for m, a in enumerate(att):
            for r in range(parts):
                some = pl.ds(pl.multiple_of(((place[0] + r) % parts) * sub, sub), sub)
                for k, c in enumerate((place[1], 1 - place[1])):
                    head = a[some, pl.ds(pl.multiple_of(c * half, half), half)]
                    att_ref[r * sub : (r + 1) * sub, (2 * m + k) * half : (2 * m + k + 1) * half] = head

    cols = pl.ds(pl.multiple_of(step * tile, tile), tile)
    weight = jnp.concatenate([v for w, o in zip(sent, swapped) for v in (w[0:half, :], o[0:half, :])], axis=0)
    total = jnp.dot(att_ref[...], weight, preferred_element_type=f32)
    for r in range(parts):
        updated = (sent[r][half:, :].astype(f32) + total[r * sub : (r + 1) * sub, :]).astype(bf16)
        x_ref[r * sub : (r + 1) * sub, cols] = updated

    @pl.when(step == pl.num_programs(0) - 1)
    def _():
        own_ref[...] = x_ref[0:sub, :]
        for r in range(2 * parts):
            some = slice(r * sub // 2, (r + 1) * sub // 2)
            x = x_ref[some, :].astype(f32)
            x = x * lax.rsqrt(jnp.mean(x * x, axis=-1, keepdims=True) + norm_eps)
            x_ref[some, :] = (x * gain_ref[...]).astype(bf16)

        def product(n):
            return jnp.dot(x_ref[...], pair_ref[n], preferred_element_type=f32)

        for begin, end, arrived in ((0, early, copies()[:early]), (early, count, copies()[early:])):
            for c in arrived:
                c.wait()
            following = product(begin)
            for n in range(begin, end):
                r = following
                if n + 1 < end:
                    following = product(n + 1)
                gate = r[:, 0:unit_tile]
                hidden = gate / (1.0 + jnp.exp(-gate)) * r[:, unit_tile:]
                h_ref[:, n * unit_tile : (n + 1) * unit_tile] = hidden.astype(bf16)
        rest_ref[0:sub, :] = h_ref[0:sub, :]
        rest_ref[sub:, :] = h_ref[3 * sub :, :]
        down_products(h_ref[sub : 3 * sub, :], down_ref, (out_1, out_2))


def down_products(hidden, down_ref, outs):
    blocks, rows, _ = down_ref.shape
    sub = outs[0].shape[0]
    for n in range(blocks):
        y = lax.dot_general(hidden, down_ref[n], (((1,), (1,)), ((), ())), preferred_element_type=f32).astype(bf16)
        for p, out in enumerate(outs):
            out[:, n * rows : (n + 1) * rows] = y[p * sub : (p + 1) * sub, :]


def rest_kernel(h_ref, w_hbm, out_0, out_3, down_ref, sems):
    blocks, rows, units = down_ref.shape
    copies = []
    for n in range(blocks):
        source = w_hbm.at[pl.ds(n * rows, rows), pl.ds(2 * units, units)]
        copies.append(pltpu.make_async_copy(source, down_ref.at[n], sems.at[n]))
    for c in copies:
        c.start()
    for c in copies:
        c.wait()
    down_products(h_ref[...], down_ref, (out_0, out_3))


def rest(hidden, weights, rows=512):
    tok, units = hidden.shape
    width = weights.shape[0]
    return pl.pallas_call(
        rest_kernel,
        in_specs=[pl.BlockSpec(memory_space=pltpu.VMEM), pl.BlockSpec(memory_space=pltpu.HBM)],
        out_shape=[jax.ShapeDtypeStruct((tok // 2, width), bf16)] * 2,
        scratch_shapes=[pltpu.VMEM((width // rows, rows, units), bf16), pltpu.SemaphoreType.DMA((width // rows,))],
        compiler_params=pltpu.CompilerParams(vmem_limit_bytes=50 << 20),
        name="rest",
    )(hidden, weights)


def layer(place, att, sent, swapped, gain, weights, units, tile=512, unit_tile=128, rows=512):
    parts = len(att)
    tok, part_width = att[0].shape
    both, width = sent[0].shape
    sub = tok // parts
    count = units // unit_tile
    blocks = width // rows
    return pl.pallas_call(
        functools.partial(layer_kernel, parts=parts, tile=tile, sub=sub, units=units, unit_tile=unit_tile),
        grid_spec=pltpu.PrefetchScalarGridSpec(
            num_scalar_prefetch=1,
            grid=(width // tile,),
            in_specs=[pl.BlockSpec((tok, part_width), lambda i, p: (0, 0))] * parts
            + [pl.BlockSpec((both, tile), lambda i, p: (0, i))] * parts
            + [pl.BlockSpec((s.shape[0], tile), lambda i, p: (0, i)) for s in swapped]
            + [pl.BlockSpec((1, width), lambda i, p: (0, 0)), pl.BlockSpec(memory_space=pltpu.HBM)],
            out_specs=[pl.BlockSpec((sub, width), lambda i, p: (0, 0))] * 3
            + [pl.BlockSpec((2 * sub, units), lambda i, p: (0, 0))],
            scratch_shapes=[
                pltpu.VMEM((tok, width), bf16),
                pltpu.VMEM((tok, parts * part_width), bf16),
                pltpu.VMEM((count, width, 2 * unit_tile), bf16),
                pltpu.VMEM((blocks, rows, units), bf16),
                pltpu.VMEM((tok, units), bf16),
                pltpu.SemaphoreType.DMA((count + blocks,)),
            ],
        ),
        out_shape=[jax.ShapeDtypeStruct((sub, width), bf16)] * 3 + [jax.ShapeDtypeStruct((2 * sub, units), bf16)],
        compiler_params=pltpu.CompilerParams(dimension_semantics=("arbitrary",), vmem_limit_bytes=50 << 20),
        name="layer",
    )(place, *att, *sent, *swapped, gain[None, :], weights)


def line_kernel(*refs):
    rows = refs[0].shape[0]
    for n, piece in enumerate(refs[:-1]):
        refs[-1][n * rows : (n + 1) * rows, :] = piece[...]


def lined_up(*pieces):
    rows, width = pieces[0].shape
    return pl.pallas_call(
        line_kernel,
        out_shape=jax.ShapeDtypeStruct((rows * len(pieces), width), bf16),
        compiler_params=pltpu.CompilerParams(vmem_limit_bytes=8 << 20),
        name="lines",
    )(*pieces)


def shifted(value, by):
    count = lax.axis_size("tp")
    return lax.ppermute(value, "tp", [(i, (i + by) % count) for i in range(count)])


SIDE = 4


def sp_index(z, y, core):
    return (z % SIDE * SIDE + y % SIDE) * 2 + core


def crossed(value, by, turned):
    pairs = []
    for z in range(SIDE):
        for y in range(SIDE):
            for core in range(2):
                along_y = (core == 0) != turned
                goal = sp_index(z, y + by, core) if along_y else sp_index(z + by, y, core)
                pairs.append((sp_index(z, y, core), goal))
    return lax.ppermute(value, "sp", pairs)


def other_core(value):
    count = 2 * SIDE * SIDE
    return lax.ppermute(value, "sp", [(n, n ^ 1) for n in range(count)])


def on_device(
    query_rows,
    key_rows,
    value_rows,
    query_gain,
    key_gain,
    residual,
    out_weight,
    mix_gain,
    gate_weight,
    up_weight,
    down_weight,
):
    tok = query_rows.shape[0]
    parts = lax.axis_size("tp")
    units = gate_weight.shape[1]
    core = lax.axis_index("sp") % 2
    place = jnp.stack([lax.axis_index("tp"), core])
    rows = tok // GRID
    tables = angle_tables(lax.axis_index("sp") * rows, rows, query_gain.shape[0])
    kv = prepare_keys(key_rows, value_rows, key_gain, *tables)
    woven, payload, kept = weave(core, gate_weight, up_weight, down_weight, out_weight, residual)
    weights = lax.all_gather(woven, "sp", axis=0, tiled=True)
    q = prepare_queries(query_rows, query_gain, *tables)

    steps = (2, 1, -1)
    line = [kv]
    for d in steps:
        line.append(crossed(kv, d, False))
    line = lined_up(*line)
    near = []
    for d in (1, -1):
        near.append(crossed(line, d, True))

    sent = [payload]
    for r in range(1, parts):
        sent.append(shifted(payload, -r))

    state = flash(q, [line, other_core(line)], None, tok, False)
    state, near = lax.optimization_barrier((state, near))
    middle = line.shape[0] // 2
    far = []
    for v, d in ((near[0][:middle], 1), (near[1][middle:], -1)):
        far.append(crossed(v, d, True))
    near_swapped = []
    for n in range(2):
        near_swapped.append(other_core(near[n]))
    state = flash(q, near, state, tok, False)
    state = flash(q, near_swapped, state, tok, False)
    state, far = lax.optimization_barrier((state, far))
    far_swapped = [other_core(v) for v in far]
    state = flash(q, far, state, tok, False)
    attended = flash(q, far_swapped, state, tok, True)

    att_parts = [attended]
    for r in range(1, parts):
        att_parts.append(shifted(attended, -r))
    att_parts[0], sent = lax.optimization_barrier((attended, sent))
    swapped = [kept]
    for r in range(1, parts):
        swapped.append(other_core(sent[r]))
    own_rows, part_1, part_2, hidden = layer(place, att_parts, sent, swapped, mix_gain, weights, units)
    part_0, part_3 = rest(hidden, weights)
    unit_sum = part_0.astype(f32)
    for r, part in ((1, part_1), (2, part_2), (3, part_3)):
        unit_sum = unit_sum + shifted(part, r).astype(f32)
    return (own_rows.astype(f32) + 0.5 * unit_sum).astype(bf16)


def solution(mesh):
    placed = (
        P("sp", "tp"),
        P("sp", "tp"),
        P("sp", "tp"),
        P(),
        P(),
        P(("sp", "tp"), None),
        P("tp", None),
        P(),
        P("sp", "tp"),
        P("sp", "tp"),
        P("tp", "sp"),
    )
    return jax.shard_map(on_device, mesh=mesh, in_specs=placed, out_specs=P(("sp", "tp"), None), check_vma=False)
```

```python
import functools

import jax
import jax.numpy as jnp
from jax import lax
from jax.experimental import pallas as pl
from jax.experimental.pallas import tpu as pltpu
from jax.sharding import PartitionSpec as P

GRID = 64
norm_eps = 1e-06
theta_base = 10000.0
LOG2E = 1.4426950408889634
f32 = jnp.float32
bf16 = jnp.bfloat16


def angle_tables(first_row, rows, head_dim):
    quarter = head_dim // 4
    frequency = jnp.power(theta_base, -2.0 * jnp.arange(quarter, dtype=f32) / (head_dim // 2))
    places = jnp.concatenate([first_row + jnp.arange(rows, dtype=jnp.int32), jnp.arange(GRID, dtype=jnp.int32)])
    angles = places.astype(f32)[:, None] * frequency
    cosine, sine = lax.optimization_barrier((jnp.cos(angles), jnp.sin(angles)))
    is_row = (jnp.arange(rows + GRID) < rows)[:, None]
    zero = jnp.zeros_like(cosine)

    def placed(lead, trail):
        return jnp.concatenate(
            [
                jnp.where(is_row, lead, zero),
                jnp.where(is_row, trail, zero),
                jnp.where(is_row, zero, lead),
                jnp.where(is_row, zero, trail),
            ],
            axis=1,
        )

    return placed(cosine, cosine), placed(-sine, sine)


def rotated(ref_x, gain_ref, cos_ref, sin_ref, rows, head_dim, columns):
    tok = rows * GRID

    def spread(ref):
        both = ref[0:rows, :][:, None, :] + ref[rows : rows + GRID, :][None, :, :]
        return both.reshape(tok, head_dim)

    cosine = spread(cos_ref)
    sine = spread(sin_ref)
    lane = lax.broadcasted_iota(jnp.int32, (tok, head_dim), 1)
    first = (lane % (head_dim // 2)) < head_dim // 4
    quarter = head_dim // 4
    found = []
    for part in columns:
        x = ref_x[:, part].astype(f32)
        x = x * lax.rsqrt(jnp.mean(x * x, axis=-1, keepdims=True) + norm_eps) * gain_ref[...]
        partner = jnp.where(first, pltpu.roll(x, head_dim - quarter, 1), pltpu.roll(x, quarter, 1))
        found.append((x * cosine + partner * sine).astype(bf16))
    return found


def keys_kernel(k_hbm, v_hbm, gain_ref, cos_ref, sin_ref, kv_out, k_ref, v_ref, sems, *, rows, head_dim):
    copies = [
        pltpu.make_async_copy(x, y, sems.at[n]) for n, (x, y) in enumerate(((k_hbm, k_ref), (v_hbm, v_ref)))
    ]
    for c in copies:
        c.start()
    for c in copies:
        c.wait()
    kv_out[:, 0:head_dim] = rotated(k_ref, gain_ref, cos_ref, sin_ref, rows, head_dim, [slice(0, head_dim)])[0]
    kv_out[:, head_dim:] = v_ref[...]


def prepare_keys(key_rows, value_rows, gain, cosine, sine):
    tok, head_dim = key_rows.shape
    hbm = pl.BlockSpec(memory_space=pltpu.HBM)
    vmem = pl.BlockSpec(memory_space=pltpu.VMEM)
    return pl.pallas_call(
        functools.partial(keys_kernel, rows=tok // GRID, head_dim=head_dim),
        in_specs=[hbm] * 2 + [vmem] * 3,
        out_shape=jax.ShapeDtypeStruct((tok, 2 * head_dim), bf16),
        scratch_shapes=[pltpu.VMEM((tok, head_dim), bf16)] * 2 + [pltpu.SemaphoreType.DMA((2,))],
        compiler_params=pltpu.CompilerParams(vmem_limit_bytes=60 * 1024 * 1024),
        name="keys",
    )(key_rows, value_rows, gain[None, :], cosine, sine)


def queries_kernel(q_ref, gain_ref, cos_ref, sin_ref, q_out, *, rows, head_dim, heads):
    tok = rows * GRID
    columns = [slice(h * head_dim, (h + 1) * head_dim) for h in range(heads)]
    for h, x in enumerate(rotated(q_ref, gain_ref, cos_ref, sin_ref, rows, head_dim, columns)):
        q_out[h * tok : (h + 1) * tok, :] = x


def prepare_queries(query_rows, gain, cosine, sine):
    tok, width = query_rows.shape
    head_dim = gain.shape[0]
    heads = width // head_dim
    return pl.pallas_call(
        functools.partial(queries_kernel, rows=tok // GRID, head_dim=head_dim, heads=heads),
        out_shape=jax.ShapeDtypeStruct((tok * heads, head_dim), bf16),
        compiler_params=pltpu.CompilerParams(vmem_limit_bytes=8 << 20),
        name="queries",
    )(query_rows, gain[None, :], cosine, sine)


def weave_kernel(g_hbm, u_hbm, d_hbm, woven, g_ref, u_ref, d_ref, sems, *, tile):
    moves = ((g_hbm, g_ref), (u_hbm, u_ref), (d_hbm, d_ref))
    copies = [pltpu.make_async_copy(x, y, sems.at[n]) for n, (x, y) in enumerate(moves)]
    for c in copies:
        c.start()
    for c in copies:
        c.wait()
    units = g_ref.shape[1]
    for n in range(units // tile):
        part = slice(n * tile, (n + 1) * tile)
        woven[:, 2 * n * tile : (2 * n + 1) * tile] = g_ref[:, part]
        woven[:, (2 * n + 1) * tile : (2 * n + 2) * tile] = u_ref[:, part]
    woven[:, 2 * units :] = d_ref[...]


def weave(gate, up, down, tile=128):
    big = (gate, up, down.T)
    return pl.pallas_call(
        functools.partial(weave_kernel, tile=tile),
        in_specs=[pl.BlockSpec(memory_space=pltpu.HBM)] * 3,
        out_shape=jax.ShapeDtypeStruct((gate.shape[0], 3 * gate.shape[1]), bf16),
        scratch_shapes=[pltpu.VMEM(x.shape, bf16) for x in big] + [pltpu.SemaphoreType.DMA((3,))],
        compiler_params=pltpu.CompilerParams(vmem_limit_bytes=60 * 1024 * 1024),
        name="weave",
    )(*big)


def stage_kernel(core, w_hbm, r_hbm, sent, kept, w_ref, r_ref, sems):
    half = kept.shape[0]
    first_half = pl.ds(pl.multiple_of(core[0] * half, half), half)
    other_half = pl.ds(pl.multiple_of((1 - core[0]) * half, half), half)
    moves = [
        (w_hbm.at[first_half, :], w_ref.at[pl.ds(0, half), :]),
        (w_hbm.at[other_half, :], w_ref.at[pl.ds(half, half), :]),
        (r_hbm, r_ref),
        (w_ref.at[pl.ds(0, half), :], sent.at[pl.ds(0, half), :]),
        (w_ref.at[pl.ds(half, half), :], kept),
        (r_ref, sent.at[pl.ds(half, r_hbm.shape[0]), :]),
    ]
    copies = [pltpu.make_async_copy(x, y, sems.at[n]) for n, (x, y) in enumerate(moves)]
    for c in copies[:3]:
        c.start()
    for n in range(3):
        copies[n].wait()
        copies[n + 3].start()
    for c in copies[3:]:
        c.wait()


def staged(core, out_weight, residual):
    half = out_weight.shape[0] // 2
    rows, width = residual.shape
    hbm = pl.BlockSpec(memory_space=pltpu.HBM)
    return pl.pallas_call(
        stage_kernel,
        in_specs=[pl.BlockSpec(memory_space=pltpu.SMEM), hbm, hbm],
        out_specs=[hbm, hbm],
        out_shape=[jax.ShapeDtypeStruct((half + rows, width), bf16), jax.ShapeDtypeStruct((half, width), bf16)],
        scratch_shapes=[pltpu.VMEM(x.shape, bf16) for x in (out_weight, residual)] + [pltpu.SemaphoreType.DMA((6,))],
        compiler_params=pltpu.CompilerParams(vmem_limit_bytes=60 * 1024 * 1024),
        name="stage",
    )(core[None], out_weight, residual)


def flash_kernel(*refs, pieces, scale, first, last, block=1024):
    q_ref = refs[0]
    kv_refs = refs[1 : 1 + pieces]
    refs = refs[1 + pieces :]
    if not first:
        m_in, acc_in = refs[0:2]
        refs = refs[2:]
    if last:
        o_ref = refs[0]
        refs = refs[1:]
    else:
        m_out, acc_out = refs[0:2]
        refs = refs[2:]
    head_dim = q_ref.shape[1]
    q = q_ref[...]
    if first:
        m = jnp.full((q.shape[0], 128), -jnp.inf, f32)
        acc = jnp.zeros((q.shape[0], 2 * head_dim), f32)
    else:
        m = m_in[...]
        acc = acc_in[...]

    parts = [(ref, slice(r, r + block)) for ref in kv_refs for r in range(0, ref.shape[0], block)]

    def scores(n):
        ref, rows = parts[n]
        return lax.dot_general(q, ref[rows, 0:head_dim], (((1,), (1,)), ((), ())), preferred_element_type=f32)

    following = scores(0)
    for n, (ref, rows) in enumerate(parts):
        values = ref[rows, head_dim:]
        values = jnp.concatenate([values, jnp.ones_like(values)], axis=1)
        s = following * scale
        if n + 1 < len(parts):
            following = scores(n + 1)
        new = jnp.maximum(m, jnp.max(s, axis=1, keepdims=True))
        w = jnp.exp2(s - new[:, 0:1]).astype(bf16)
        factor = jnp.exp2(m - new)
        acc = acc * factor[:, 0:1] + jnp.dot(w, values, preferred_element_type=f32)
        m = new
    if last:
        o_ref[...] = (acc[:, 0:head_dim] / acc[:, head_dim:]).astype(bf16)
    else:
        m_out[...] = m
        acc_out[...] = acc


def flash(q, kv, state, tok, last, tile=256):
    rows, head_dim = q.shape
    heads = rows // tok
    pieces = len(kv)
    piece = kv[0].shape
    tiles = tok // tile
    held = [pl.BlockSpec((tile, 128), lambda i: (i, 0)), pl.BlockSpec((tile, 2 * head_dim), lambda i: (i, 0))]
    held_shape = (jax.ShapeDtypeStruct((rows, 128), f32), jax.ShapeDtypeStruct((rows, 2 * head_dim), f32))
    first = state is None
    return pl.pallas_call(
        functools.partial(flash_kernel, pieces=pieces, scale=head_dim**-0.5 * LOG2E, first=first, last=last),
        grid=(rows // tile,),
        in_specs=[pl.BlockSpec((tile, head_dim), lambda i: (i, 0))]
        + [pl.BlockSpec(piece, lambda i: (0, 0))] * pieces
        + ([] if first else held),
        out_specs=pl.BlockSpec((tile, head_dim), lambda i: (i % tiles, i // tiles)) if last else tuple(held),
        out_shape=jax.ShapeDtypeStruct((tok, heads * head_dim), bf16) if last else held_shape,
        compiler_params=pltpu.CompilerParams(dimension_semantics=("arbitrary",), vmem_limit_bytes=12 << 20),
        cost_estimate=pl.CostEstimate(
            flops=4 * rows * piece[0] * pieces * head_dim,
            bytes_accessed=4 * piece[0] * pieces * head_dim,
            transcendentals=rows * piece[0] * pieces,
        ),
    )(q, *kv, *([] if first else state))


def layer_kernel(place, *refs, parts, tile, sub, units, unit_tile):
    att = refs[0:parts]
    sent = refs[parts : 2 * parts]
    swapped = refs[2 * parts : 3 * parts]
    gain_ref, w_hbm, own_ref = refs[3 * parts : 3 * parts + 3]
    out_1, out_2, rest_ref = refs[3 * parts + 3 : -6]
    x_ref, att_ref, pair_ref, down_ref, h_ref, sems = refs[-6:]
    step = pl.program_id(0)
    half = sent[0].shape[0] - sub
    count = units // unit_tile
    blocks, rows, _ = down_ref.shape

    def copies():
        found = []
        for n in range(count):
            source = w_hbm.at[:, pl.ds(2 * n * unit_tile, 2 * unit_tile)]
            found.append(pltpu.make_async_copy(source, pair_ref.at[n], sems.at[n]))
        for n in range(blocks):
            source = w_hbm.at[pl.ds(n * rows, rows), pl.ds(2 * units, units)]
            found.append(pltpu.make_async_copy(source, down_ref.at[n], sems.at[count + n]))
        return found

    early = count * 2 // 3

    @pl.when(step == 0)
    def _():
        for c in copies()[:early]:
            c.start()

    @pl.when(step == 1)
    def _():
        for c in copies()[early:]:
            c.start()

    @pl.when(step == 0)
    def _():
        for m, a in enumerate(att):
            for r in range(parts):
                some = pl.ds(pl.multiple_of(((place[0] + r) % parts) * sub, sub), sub)
                for k, c in enumerate((place[1], 1 - place[1])):
                    head = a[some, pl.ds(pl.multiple_of(c * half, half), half)]
                    att_ref[r * sub : (r + 1) * sub, (2 * m + k) * half : (2 * m + k + 1) * half] = head

    cols = pl.ds(pl.multiple_of(step * tile, tile), tile)
    weight = jnp.concatenate([v for w, o in zip(sent, swapped) for v in (w[0:half, :], o[0:half, :])], axis=0)
    total = jnp.dot(att_ref[...], weight, preferred_element_type=f32)
    for r in range(parts):
        updated = (sent[r][half:, :].astype(f32) + total[r * sub : (r + 1) * sub, :]).astype(bf16)
        x_ref[r * sub : (r + 1) * sub, cols] = updated

    @pl.when(step == pl.num_programs(0) - 1)
    def _():
        own_ref[...] = x_ref[0:sub, :]
        for r in range(2 * parts):
            some = slice(r * sub // 2, (r + 1) * sub // 2)
            x = x_ref[some, :].astype(f32)
            x = x * lax.rsqrt(jnp.mean(x * x, axis=-1, keepdims=True) + norm_eps)
            x_ref[some, :] = (x * gain_ref[...]).astype(bf16)

        def product(tiles):
            both = jnp.concatenate([pair_ref[n] for n in tiles], axis=1)
            return jnp.dot(x_ref[...], both, preferred_element_type=f32)

        for begin, end, arrived in ((0, early, copies()[:early]), (early, count, copies()[early:])):
            for c in arrived:
                c.wait()
            runs = [range(n, min(n + 2, end)) for n in range(begin, end, 2)]
            following = product(runs[0])
            for k, tiles in enumerate(runs):
                r = following
                if k + 1 < len(runs):
                    following = product(runs[k + 1])
                for m, n in enumerate(tiles):
                    gate = r[:, 2 * m * unit_tile : (2 * m + 1) * unit_tile]
                    up = r[:, (2 * m + 1) * unit_tile : (2 * m + 2) * unit_tile]
                    hidden = gate / (1.0 + jnp.exp(-gate)) * up
                    h_ref[:, n * unit_tile : (n + 1) * unit_tile] = hidden.astype(bf16)
        rest_ref[0:sub, :] = h_ref[0:sub, :]
        rest_ref[sub:, :] = h_ref[3 * sub :, :]
        down_products(h_ref[sub : 3 * sub, :], down_ref, (out_1, out_2))


def down_products(hidden, down_ref, outs):
    blocks, rows, _ = down_ref.shape
    sub = outs[0].shape[0]
    for n in range(blocks):
        y = lax.dot_general(hidden, down_ref[n], (((1,), (1,)), ((), ())), preferred_element_type=f32).astype(bf16)
        for p, out in enumerate(outs):
            out[:, n * rows : (n + 1) * rows] = y[p * sub : (p + 1) * sub, :]


def rest_kernel(h_ref, w_hbm, out_0, out_3, down_ref, sems):
    blocks, rows, units = down_ref.shape
    copies = []
    for n in range(blocks):
        source = w_hbm.at[pl.ds(n * rows, rows), pl.ds(2 * units, units)]
        copies.append(pltpu.make_async_copy(source, down_ref.at[n], sems.at[n]))
    for c in copies:
        c.start()
    for c in copies:
        c.wait()
    down_products(h_ref[...], down_ref, (out_0, out_3))


def rest(hidden, weights, rows=512):
    tok, units = hidden.shape
    width = weights.shape[0]
    return pl.pallas_call(
        rest_kernel,
        in_specs=[pl.BlockSpec(memory_space=pltpu.VMEM), pl.BlockSpec(memory_space=pltpu.HBM)],
        out_shape=[jax.ShapeDtypeStruct((tok // 2, width), bf16)] * 2,
        scratch_shapes=[pltpu.VMEM((width // rows, rows, units), bf16), pltpu.SemaphoreType.DMA((width // rows,))],
        compiler_params=pltpu.CompilerParams(vmem_limit_bytes=50 << 20),
        name="rest",
    )(hidden, weights)


def layer(place, att, sent, swapped, gain, weights, units, tile=512, unit_tile=128, rows=512):
    parts = len(att)
    tok, part_width = att[0].shape
    both, width = sent[0].shape
    sub = tok // parts
    count = units // unit_tile
    blocks = width // rows
    return pl.pallas_call(
        functools.partial(layer_kernel, parts=parts, tile=tile, sub=sub, units=units, unit_tile=unit_tile),
        grid_spec=pltpu.PrefetchScalarGridSpec(
            num_scalar_prefetch=1,
            grid=(width // tile,),
            in_specs=[pl.BlockSpec((tok, part_width), lambda i, p: (0, 0))] * parts
            + [pl.BlockSpec((both, tile), lambda i, p: (0, i))] * parts
            + [pl.BlockSpec((s.shape[0], tile), lambda i, p: (0, i)) for s in swapped]
            + [pl.BlockSpec((1, width), lambda i, p: (0, 0)), pl.BlockSpec(memory_space=pltpu.HBM)],
            out_specs=[pl.BlockSpec((sub, width), lambda i, p: (0, 0))] * 3
            + [pl.BlockSpec((2 * sub, units), lambda i, p: (0, 0))],
            scratch_shapes=[
                pltpu.VMEM((tok, width), bf16),
                pltpu.VMEM((tok, parts * part_width), bf16),
                pltpu.VMEM((count, width, 2 * unit_tile), bf16),
                pltpu.VMEM((blocks, rows, units), bf16),
                pltpu.VMEM((tok, units), bf16),
                pltpu.SemaphoreType.DMA((count + blocks,)),
            ],
        ),
        out_shape=[jax.ShapeDtypeStruct((sub, width), bf16)] * 3 + [jax.ShapeDtypeStruct((2 * sub, units), bf16)],
        compiler_params=pltpu.CompilerParams(dimension_semantics=("arbitrary",), vmem_limit_bytes=50 << 20),
        name="layer",
    )(place, *att, *sent, *swapped, gain[None, :], weights)


def line_kernel(*refs):
    rows = refs[0].shape[0]
    for n, piece in enumerate(refs[:-1]):
        refs[-1][n * rows : (n + 1) * rows, :] = piece[...]


def lined_up(*pieces):
    rows, width = pieces[0].shape
    return pl.pallas_call(
        line_kernel,
        out_shape=jax.ShapeDtypeStruct((rows * len(pieces), width), bf16),
        compiler_params=pltpu.CompilerParams(vmem_limit_bytes=8 << 20),
        name="lines",
    )(*pieces)


def shifted(value, by):
    count = lax.axis_size("tp")
    return lax.ppermute(value, "tp", [(i, (i + by) % count) for i in range(count)])


SIDE = 4


def sp_index(z, y, core):
    return (z % SIDE * SIDE + y % SIDE) * 2 + core


def crossed(value, by, turned):
    pairs = []
    for z in range(SIDE):
        for y in range(SIDE):
            for core in range(2):
                along_y = (core == 0) != turned
                goal = sp_index(z, y + by, core) if along_y else sp_index(z + by, y, core)
                pairs.append((sp_index(z, y, core), goal))
    return lax.ppermute(value, "sp", pairs)


def other_core(value):
    count = 2 * SIDE * SIDE
    return lax.ppermute(value, "sp", [(n, n ^ 1) for n in range(count)])


def on_device(
    query_rows,
    key_rows,
    value_rows,
    query_gain,
    key_gain,
    residual,
    out_weight,
    mix_gain,
    gate_weight,
    up_weight,
    down_weight,
):
    tok = query_rows.shape[0]
    parts = lax.axis_size("tp")
    units = gate_weight.shape[1]
    core = lax.axis_index("sp") % 2
    place = jnp.stack([lax.axis_index("tp"), core])
    rows = tok // GRID
    tables = angle_tables(lax.axis_index("sp") * rows, rows, query_gain.shape[0])
    kv = prepare_keys(key_rows, value_rows, key_gain, *tables)
    weights = lax.all_gather(weave(gate_weight, up_weight, down_weight), "sp", axis=0, tiled=True)
    payload, kept = staged(core, out_weight, residual)
    q = prepare_queries(query_rows, query_gain, *tables)

    steps = (2, 1, -1)
    line = [kv]
    for d in steps:
        line.append(crossed(kv, d, False))
    line = lined_up(*line)
    near = []
    for d in (1, -1):
        near.append(crossed(line, d, True))

    sent = [payload]
    for r in range(1, parts):
        sent.append(shifted(payload, -r))

    state = flash(q, [line, other_core(line)], None, tok, False)
    state, near = lax.optimization_barrier((state, near))
    middle = line.shape[0] // 2
    far = []
    for v, d in ((near[0][:middle], 1), (near[1][middle:], -1)):
        far.append(crossed(v, d, True))
    near_swapped = []
    for n in range(2):
        near_swapped.append(other_core(near[n]))
    state = flash(q, near, state, tok, False)
    state = flash(q, near_swapped, state, tok, False)
    state, far = lax.optimization_barrier((state, far))
    far_swapped = [other_core(v) for v in far]
    state = flash(q, far, state, tok, False)
    attended = flash(q, far_swapped, state, tok, True)

    att_parts = [attended]
    for r in range(1, parts):
        att_parts.append(shifted(attended, -r))
    att_parts[0], sent = lax.optimization_barrier((attended, sent))
    swapped = [kept]
    for r in range(1, parts):
        swapped.append(other_core(sent[r]))
    own_rows, part_1, part_2, hidden = layer(place, att_parts, sent, swapped, mix_gain, weights, units)
    part_0, part_3 = rest(hidden, weights)
    unit_sum = part_0.astype(f32)
    for r, part in ((1, part_1), (2, part_2), (3, part_3)):
        unit_sum = unit_sum + shifted(part, r).astype(f32)
    return (own_rows.astype(f32) + 0.5 * unit_sum).astype(bf16)


def solution(mesh):
    placed = (
        P("sp", "tp"),
        P("sp", "tp"),
        P("sp", "tp"),
        P(),
        P(),
        P(("sp", "tp"), None),
        P("tp", None),
        P(),
        P("sp", "tp"),
        P("sp", "tp"),
        P("tp", "sp"),
    )
    return jax.shard_map(on_device, mesh=mesh, in_specs=placed, out_specs=P(("sp", "tp"), None), check_vma=False)
```

```python
import functools

import jax
import jax.numpy as jnp
from jax import lax
from jax.experimental import pallas as pl
from jax.experimental.pallas import tpu as pltpu
from jax.sharding import PartitionSpec as P

GRID = 64
norm_eps = 1e-06
theta_base = 10000.0
LOG2E = 1.4426950408889634
f32 = jnp.float32
bf16 = jnp.bfloat16


def angle_tables(first_row, rows, head_dim):
    quarter = head_dim // 4
    frequency = jnp.power(theta_base, -2.0 * jnp.arange(quarter, dtype=f32) / (head_dim // 2))
    places = jnp.concatenate([first_row + jnp.arange(rows, dtype=jnp.int32), jnp.arange(GRID, dtype=jnp.int32)])
    angles = places.astype(f32)[:, None] * frequency
    cosine, sine = lax.optimization_barrier((jnp.cos(angles), jnp.sin(angles)))
    is_row = (jnp.arange(rows + GRID) < rows)[:, None]
    zero = jnp.zeros_like(cosine)

    def placed(lead, trail):
        return jnp.concatenate(
            [
                jnp.where(is_row, lead, zero),
                jnp.where(is_row, trail, zero),
                jnp.where(is_row, zero, lead),
                jnp.where(is_row, zero, trail),
            ],
            axis=1,
        )

    return placed(cosine, cosine), placed(-sine, sine)


def rotated(ref_x, gain_ref, cos_ref, sin_ref, rows, head_dim, columns):
    tok = rows * GRID

    def spread(ref):
        both = ref[0:rows, :][:, None, :] + ref[rows : rows + GRID, :][None, :, :]
        return both.reshape(tok, head_dim)

    cosine = spread(cos_ref)
    sine = spread(sin_ref)
    lane = lax.broadcasted_iota(jnp.int32, (tok, head_dim), 1)
    first = (lane % (head_dim // 2)) < head_dim // 4
    quarter = head_dim // 4
    found = []
    for part in columns:
        x = ref_x[:, part].astype(f32)
        x = x * lax.rsqrt(jnp.mean(x * x, axis=-1, keepdims=True) + norm_eps) * gain_ref[...]
        partner = jnp.where(first, pltpu.roll(x, head_dim - quarter, 1), pltpu.roll(x, quarter, 1))
        found.append((x * cosine + partner * sine).astype(bf16))
    return found


def keys_kernel(k_hbm, v_hbm, gain_ref, cos_ref, sin_ref, kv_out, k_ref, v_ref, sems, *, rows, head_dim):
    copies = [
        pltpu.make_async_copy(x, y, sems.at[n]) for n, (x, y) in enumerate(((k_hbm, k_ref), (v_hbm, v_ref)))
    ]
    for c in copies:
        c.start()
    for c in copies:
        c.wait()
    kv_out[:, 0:head_dim] = rotated(k_ref, gain_ref, cos_ref, sin_ref, rows, head_dim, [slice(0, head_dim)])[0]
    kv_out[:, head_dim:] = v_ref[...]


def prepare_keys(key_rows, value_rows, gain, cosine, sine):
    tok, head_dim = key_rows.shape
    hbm = pl.BlockSpec(memory_space=pltpu.HBM)
    vmem = pl.BlockSpec(memory_space=pltpu.VMEM)
    return pl.pallas_call(
        functools.partial(keys_kernel, rows=tok // GRID, head_dim=head_dim),
        in_specs=[hbm] * 2 + [vmem] * 3,
        out_shape=jax.ShapeDtypeStruct((tok, 2 * head_dim), bf16),
        scratch_shapes=[pltpu.VMEM((tok, head_dim), bf16)] * 2 + [pltpu.SemaphoreType.DMA((2,))],
        compiler_params=pltpu.CompilerParams(vmem_limit_bytes=60 * 1024 * 1024),
        name="keys",
    )(key_rows, value_rows, gain[None, :], cosine, sine)


def queries_kernel(q_ref, gain_ref, cos_ref, sin_ref, q_out, *, rows, head_dim, heads):
    tok = rows * GRID
    columns = [slice(h * head_dim, (h + 1) * head_dim) for h in range(heads)]
    for h, x in enumerate(rotated(q_ref, gain_ref, cos_ref, sin_ref, rows, head_dim, columns)):
        q_out[h * tok : (h + 1) * tok, :] = x


def prepare_queries(query_rows, gain, cosine, sine):
    tok, width = query_rows.shape
    head_dim = gain.shape[0]
    heads = width // head_dim
    return pl.pallas_call(
        functools.partial(queries_kernel, rows=tok // GRID, head_dim=head_dim, heads=heads),
        out_shape=jax.ShapeDtypeStruct((tok * heads, head_dim), bf16),
        compiler_params=pltpu.CompilerParams(vmem_limit_bytes=8 << 20),
        name="queries",
    )(query_rows, gain[None, :], cosine, sine)


def weave_kernel(g_hbm, u_hbm, d_hbm, woven, g_ref, u_ref, d_ref, sems, *, tile):
    moves = ((g_hbm, g_ref), (u_hbm, u_ref), (d_hbm, d_ref))
    copies = [pltpu.make_async_copy(x, y, sems.at[n]) for n, (x, y) in enumerate(moves)]
    for c in copies:
        c.start()
    for c in copies:
        c.wait()
    units = g_ref.shape[1]
    for n in range(units // tile):
        part = slice(n * tile, (n + 1) * tile)
        woven[:, 2 * n * tile : (2 * n + 1) * tile] = g_ref[:, part]
        woven[:, (2 * n + 1) * tile : (2 * n + 2) * tile] = u_ref[:, part]
    woven[:, 2 * units :] = d_ref[...]


def weave(gate, up, down, tile=128):
    big = (gate, up, down.T)
    return pl.pallas_call(
        functools.partial(weave_kernel, tile=tile),
        in_specs=[pl.BlockSpec(memory_space=pltpu.HBM)] * 3,
        out_shape=jax.ShapeDtypeStruct((gate.shape[0], 3 * gate.shape[1]), bf16),
        scratch_shapes=[pltpu.VMEM(x.shape, bf16) for x in big] + [pltpu.SemaphoreType.DMA((3,))],
        compiler_params=pltpu.CompilerParams(vmem_limit_bytes=60 * 1024 * 1024),
        name="weave",
    )(*big)


def stage_kernel(core, w_hbm, r_hbm, sent, kept, w_ref, r_ref, sems):
    half = kept.shape[0]
    first_half = pl.ds(pl.multiple_of(core[0] * half, half), half)
    other_half = pl.ds(pl.multiple_of((1 - core[0]) * half, half), half)
    moves = [
        (w_hbm.at[first_half, :], w_ref.at[pl.ds(0, half), :]),
        (w_hbm.at[other_half, :], w_ref.at[pl.ds(half, half), :]),
        (r_hbm, r_ref),
        (w_ref.at[pl.ds(0, half), :], sent.at[pl.ds(0, half), :]),
        (w_ref.at[pl.ds(half, half), :], kept),
        (r_ref, sent.at[pl.ds(half, r_hbm.shape[0]), :]),
    ]
    copies = [pltpu.make_async_copy(x, y, sems.at[n]) for n, (x, y) in enumerate(moves)]
    for c in copies[:3]:
        c.start()
    for n in range(3):
        copies[n].wait()
        copies[n + 3].start()
    for c in copies[3:]:
        c.wait()


def staged(core, out_weight, residual):
    half = out_weight.shape[0] // 2
    rows, width = residual.shape
    hbm = pl.BlockSpec(memory_space=pltpu.HBM)
    return pl.pallas_call(
        stage_kernel,
        in_specs=[pl.BlockSpec(memory_space=pltpu.SMEM), hbm, hbm],
        out_specs=[hbm, hbm],
        out_shape=[jax.ShapeDtypeStruct((half + rows, width), bf16), jax.ShapeDtypeStruct((half, width), bf16)],
        scratch_shapes=[pltpu.VMEM(x.shape, bf16) for x in (out_weight, residual)] + [pltpu.SemaphoreType.DMA((6,))],
        compiler_params=pltpu.CompilerParams(vmem_limit_bytes=60 * 1024 * 1024),
        name="stage",
    )(core[None], out_weight, residual)


def flash_kernel(*refs, pieces, scale, first, last, block=1024):
    q_ref = refs[0]
    kv_refs = refs[1 : 1 + pieces]
    refs = refs[1 + pieces :]
    if not first:
        m_in, acc_in = refs[0:2]
        refs = refs[2:]
    if last:
        o_ref = refs[0]
        refs = refs[1:]
    else:
        m_out, acc_out = refs[0:2]
        refs = refs[2:]
    head_dim = q_ref.shape[1]
    q = q_ref[...]
    if first:
        m = jnp.full((q.shape[0], 128), -jnp.inf, f32)
        acc = jnp.zeros((q.shape[0], 2 * head_dim), f32)
    else:
        m = m_in[...]
        acc = acc_in[...]

    parts = [(ref, slice(r, r + block)) for ref in kv_refs for r in range(0, ref.shape[0], block)]

    def scores(n):
        ref, rows = parts[n]
        return lax.dot_general(q, ref[rows, 0:head_dim], (((1,), (1,)), ((), ())), preferred_element_type=f32)

    following = scores(0)
    for n, (ref, rows) in enumerate(parts):
        values = ref[rows, head_dim:]
        values = jnp.concatenate([values, jnp.ones_like(values)], axis=1)
        s = following * scale
        if n + 1 < len(parts):
            following = scores(n + 1)
        new = jnp.maximum(m, jnp.max(s, axis=1, keepdims=True))
        w = jnp.exp2(s - new[:, 0:1]).astype(bf16)
        factor = jnp.exp2(m - new)
        acc = acc * factor[:, 0:1] + jnp.dot(w, values, preferred_element_type=f32)
        m = new
    if last:
        o_ref[...] = (acc[:, 0:head_dim] / acc[:, head_dim:]).astype(bf16)
    else:
        m_out[...] = m
        acc_out[...] = acc


def flash(q, kv, state, tok, last, tile=256):
    rows, head_dim = q.shape
    heads = rows // tok
    pieces = len(kv)
    piece = kv[0].shape
    tiles = tok // tile
    held = [pl.BlockSpec((tile, 128), lambda i: (i, 0)), pl.BlockSpec((tile, 2 * head_dim), lambda i: (i, 0))]
    held_shape = (jax.ShapeDtypeStruct((rows, 128), f32), jax.ShapeDtypeStruct((rows, 2 * head_dim), f32))
    first = state is None
    return pl.pallas_call(
        functools.partial(flash_kernel, pieces=pieces, scale=head_dim**-0.5 * LOG2E, first=first, last=last),
        grid=(rows // tile,),
        in_specs=[pl.BlockSpec((tile, head_dim), lambda i: (i, 0))]
        + [pl.BlockSpec(piece, lambda i: (0, 0))] * pieces
        + ([] if first else held),
        out_specs=pl.BlockSpec((tile, head_dim), lambda i: (i % tiles, i // tiles)) if last else tuple(held),
        out_shape=jax.ShapeDtypeStruct((tok, heads * head_dim), bf16) if last else held_shape,
        compiler_params=pltpu.CompilerParams(dimension_semantics=("arbitrary",), vmem_limit_bytes=20 << 20),
        cost_estimate=pl.CostEstimate(
            flops=4 * rows * piece[0] * pieces * head_dim,
            bytes_accessed=4 * piece[0] * pieces * head_dim,
            transcendentals=rows * piece[0] * pieces,
        ),
    )(q, *kv, *([] if first else state))


def layer_kernel(place, *refs, parts, tile, sub, units, unit_tile):
    att = refs[0:parts]
    sent = refs[parts : 2 * parts]
    swapped = refs[2 * parts : 3 * parts]
    gain_ref, w_hbm, own_ref = refs[3 * parts : 3 * parts + 3]
    out_1, out_2, rest_ref = refs[3 * parts + 3 : -6]
    x_ref, att_ref, pair_ref, down_ref, h_ref, sems = refs[-6:]
    step = pl.program_id(0)
    half = sent[0].shape[0] - sub
    count = units // unit_tile
    blocks, rows, _ = down_ref.shape

    def copies():
        found = []
        for n in range(count):
            source = w_hbm.at[:, pl.ds(2 * n * unit_tile, 2 * unit_tile)]
            found.append(pltpu.make_async_copy(source, pair_ref.at[n], sems.at[n]))
        for n in range(blocks):
            source = w_hbm.at[pl.ds(n * rows, rows), pl.ds(2 * units, units)]
            found.append(pltpu.make_async_copy(source, down_ref.at[n], sems.at[count + n]))
        return found

    early = count * 2 // 3

    @pl.when(step == 0)
    def _():
        for c in copies()[:early]:
            c.start()

    @pl.when(step == 1)
    def _():
        for c in copies()[early:]:
            c.start()

    @pl.when(step == 0)
    def _():
        for m, a in enumerate(att):
            for r in range(parts):
                some = pl.ds(pl.multiple_of(((place[0] + r) % parts) * sub, sub), sub)
                for k, c in enumerate((place[1], 1 - place[1])):
                    head = a[some, pl.ds(pl.multiple_of(c * half, half), half)]
                    att_ref[r * sub : (r + 1) * sub, (2 * m + k) * half : (2 * m + k + 1) * half] = head

    cols = pl.ds(pl.multiple_of(step * tile, tile), tile)
    weight = jnp.concatenate([v for w, o in zip(sent, swapped) for v in (w[0:half, :], o[0:half, :])], axis=0)
    total = jnp.dot(att_ref[...], weight, preferred_element_type=f32)
    for r in range(parts):
        updated = (sent[r][half:, :].astype(f32) + total[r * sub : (r + 1) * sub, :]).astype(bf16)
        x_ref[r * sub : (r + 1) * sub, cols] = updated

    @pl.when(step == pl.num_programs(0) - 1)
    def _():
        own_ref[...] = x_ref[0:sub, :]
        for r in range(2 * parts):
            some = slice(r * sub // 2, (r + 1) * sub // 2)
            x = x_ref[some, :].astype(f32)
            x = x * lax.rsqrt(jnp.mean(x * x, axis=-1, keepdims=True) + norm_eps)
            x_ref[some, :] = (x * gain_ref[...]).astype(bf16)

        def product(tiles):
            both = jnp.concatenate([pair_ref[n] for n in tiles], axis=1)
            return jnp.dot(x_ref[...], both, preferred_element_type=f32)

        for begin, end, arrived in ((0, early, copies()[:early]), (early, count, copies()[early:])):
            for c in arrived:
                c.wait()
            runs = [range(n, min(n + 2, end)) for n in range(begin, end, 2)]
            following = product(runs[0])
            for k, tiles in enumerate(runs):
                r = following
                if k + 1 < len(runs):
                    following = product(runs[k + 1])
                for m, n in enumerate(tiles):
                    gate = r[:, 2 * m * unit_tile : (2 * m + 1) * unit_tile]
                    up = r[:, (2 * m + 1) * unit_tile : (2 * m + 2) * unit_tile]
                    hidden = gate / (1.0 + jnp.exp(-gate)) * up
                    h_ref[:, n * unit_tile : (n + 1) * unit_tile] = hidden.astype(bf16)
        rest_ref[0:sub, :] = h_ref[0:sub, :]
        rest_ref[sub:, :] = h_ref[3 * sub :, :]
        down_products(h_ref[sub : 3 * sub, :], down_ref, (out_1, out_2))


def down_products(hidden, down_ref, outs):
    blocks, rows, _ = down_ref.shape
    sub = outs[0].shape[0]
    for n in range(blocks):
        y = lax.dot_general(hidden, down_ref[n], (((1,), (1,)), ((), ())), preferred_element_type=f32).astype(bf16)
        for p, out in enumerate(outs):
            out[:, n * rows : (n + 1) * rows] = y[p * sub : (p + 1) * sub, :]


def rest_kernel(h_ref, w_hbm, out_0, out_3, down_ref, sems):
    blocks, rows, units = down_ref.shape
    copies = []
    for n in range(blocks):
        source = w_hbm.at[pl.ds(n * rows, rows), pl.ds(2 * units, units)]
        copies.append(pltpu.make_async_copy(source, down_ref.at[n], sems.at[n]))
    for c in copies:
        c.start()
    for c in copies:
        c.wait()
    down_products(h_ref[...], down_ref, (out_0, out_3))


def rest(hidden, weights, rows=512):
    tok, units = hidden.shape
    width = weights.shape[0]
    return pl.pallas_call(
        rest_kernel,
        in_specs=[pl.BlockSpec(memory_space=pltpu.VMEM), pl.BlockSpec(memory_space=pltpu.HBM)],
        out_shape=[jax.ShapeDtypeStruct((tok // 2, width), bf16)] * 2,
        scratch_shapes=[pltpu.VMEM((width // rows, rows, units), bf16), pltpu.SemaphoreType.DMA((width // rows,))],
        compiler_params=pltpu.CompilerParams(vmem_limit_bytes=50 << 20),
        name="rest",
    )(hidden, weights)


def layer(place, att, sent, swapped, gain, weights, units, tile=512, unit_tile=128, rows=512):
    parts = len(att)
    tok, part_width = att[0].shape
    both, width = sent[0].shape
    sub = tok // parts
    count = units // unit_tile
    blocks = width // rows
    return pl.pallas_call(
        functools.partial(layer_kernel, parts=parts, tile=tile, sub=sub, units=units, unit_tile=unit_tile),
        grid_spec=pltpu.PrefetchScalarGridSpec(
            num_scalar_prefetch=1,
            grid=(width // tile,),
            in_specs=[pl.BlockSpec((tok, part_width), lambda i, p: (0, 0))] * parts
            + [pl.BlockSpec((both, tile), lambda i, p: (0, i))] * parts
            + [pl.BlockSpec((s.shape[0], tile), lambda i, p: (0, i)) for s in swapped]
            + [pl.BlockSpec((1, width), lambda i, p: (0, 0)), pl.BlockSpec(memory_space=pltpu.HBM)],
            out_specs=[pl.BlockSpec((sub, width), lambda i, p: (0, 0))] * 3
            + [pl.BlockSpec((2 * sub, units), lambda i, p: (0, 0))],
            scratch_shapes=[
                pltpu.VMEM((tok, width), bf16),
                pltpu.VMEM((tok, parts * part_width), bf16),
                pltpu.VMEM((count, width, 2 * unit_tile), bf16),
                pltpu.VMEM((blocks, rows, units), bf16),
                pltpu.VMEM((tok, units), bf16),
                pltpu.SemaphoreType.DMA((count + blocks,)),
            ],
        ),
        out_shape=[jax.ShapeDtypeStruct((sub, width), bf16)] * 3 + [jax.ShapeDtypeStruct((2 * sub, units), bf16)],
        compiler_params=pltpu.CompilerParams(dimension_semantics=("arbitrary",), vmem_limit_bytes=50 << 20),
        name="layer",
    )(place, *att, *sent, *swapped, gain[None, :], weights)


def line_kernel(*refs):
    rows = refs[0].shape[0]
    for n, piece in enumerate(refs[:-1]):
        refs[-1][n * rows : (n + 1) * rows, :] = piece[...]


def lined_up(*pieces):
    rows, width = pieces[0].shape
    return pl.pallas_call(
        line_kernel,
        out_shape=jax.ShapeDtypeStruct((rows * len(pieces), width), bf16),
        compiler_params=pltpu.CompilerParams(vmem_limit_bytes=8 << 20),
        name="lines",
    )(*pieces)


def shifted(value, by):
    count = lax.axis_size("tp")
    return lax.ppermute(value, "tp", [(i, (i + by) % count) for i in range(count)])


SIDE = 4


def sp_index(z, y, core):
    return (z % SIDE * SIDE + y % SIDE) * 2 + core


def crossed(value, by, turned):
    pairs = []
    for z in range(SIDE):
        for y in range(SIDE):
            for core in range(2):
                along_y = (core == 0) != turned
                goal = sp_index(z, y + by, core) if along_y else sp_index(z + by, y, core)
                pairs.append((sp_index(z, y, core), goal))
    return lax.ppermute(value, "sp", pairs)


def other_core(value):
    count = 2 * SIDE * SIDE
    return lax.ppermute(value, "sp", [(n, n ^ 1) for n in range(count)])


def on_device(
    query_rows,
    key_rows,
    value_rows,
    query_gain,
    key_gain,
    residual,
    out_weight,
    mix_gain,
    gate_weight,
    up_weight,
    down_weight,
):
    tok = query_rows.shape[0]
    parts = lax.axis_size("tp")
    units = gate_weight.shape[1]
    core = lax.axis_index("sp") % 2
    place = jnp.stack([lax.axis_index("tp"), core])
    rows = tok // GRID
    tables = angle_tables(lax.axis_index("sp") * rows, rows, query_gain.shape[0])
    kv = prepare_keys(key_rows, value_rows, key_gain, *tables)
    weights = lax.all_gather(weave(gate_weight, up_weight, down_weight), "sp", axis=0, tiled=True)
    payload, kept = staged(core, out_weight, residual)
    q = prepare_queries(query_rows, query_gain, *tables)

    steps = (2, 1, -1)
    line = [kv]
    for d in steps:
        line.append(crossed(kv, d, False))
    line = lined_up(*line)
    near = []
    for d in (1, -1):
        near.append(crossed(line, d, True))

    sent = [payload]
    for r in range(1, parts):
        sent.append(shifted(payload, -r))

    state = flash(q, [line, other_core(line)], None, tok, False)
    state, near = lax.optimization_barrier((state, near))
    middle = line.shape[0] // 2
    far = []
    for v, d in ((near[0][:middle], 1), (near[1][middle:], -1)):
        far.append(crossed(v, d, True))
    near_swapped = []
    for n in range(2):
        near_swapped.append(other_core(near[n]))
    state = flash(q, near, state, tok, False)
    state = flash(q, near_swapped, state, tok, False)
    state, far = lax.optimization_barrier((state, far))
    far_swapped = [other_core(v) for v in far]
    state = flash(q, far, state, tok, False, tile=512)
    attended = flash(q, far_swapped, state, tok, True, tile=512)

    att_parts = [attended]
    for r in range(1, parts):
        att_parts.append(shifted(attended, -r))
    att_parts[0], sent = lax.optimization_barrier((attended, sent))
    swapped = [kept]
    for r in range(1, parts):
        swapped.append(other_core(sent[r]))
    own_rows, part_1, part_2, hidden = layer(place, att_parts, sent, swapped, mix_gain, weights, units)
    part_0, part_3 = rest(hidden, weights)
    unit_sum = part_0.astype(f32)
    for r, part in ((1, part_1), (2, part_2), (3, part_3)):
        unit_sum = unit_sum + shifted(part, r).astype(f32)
    return (own_rows.astype(f32) + 0.5 * unit_sum).astype(bf16)


def solution(mesh):
    placed = (
        P("sp", "tp"),
        P("sp", "tp"),
        P("sp", "tp"),
        P(),
        P(),
        P(("sp", "tp"), None),
        P("tp", None),
        P(),
        P("sp", "tp"),
        P("sp", "tp"),
        P("tp", "sp"),
    )
    return jax.shard_map(on_device, mesh=mesh, in_specs=placed, out_specs=P(("sp", "tp"), None), check_vma=False)
```
